32 devices in a mesh: grp: 2 (over y), sp: 4 (over z), tp: 4 (over x, core).
Axes of the slice: x: 2, y: 2, z: 4, core: 2. Of those that a mesh axis runs over, the one named last changes fastest.
Arguments:
- hidden_in: bfloat16 [3072, 4096], P(('grp', 'sp'), 'tp'), parts along dimension 0, may hold values from -30 to 30
- in_gain: float32 [2, 4096], P(None, 'tp'), may hold values from 0.1 to 1.9
- w_value: bfloat16 [2, 4096, 2048], P(None, 'sp', 'tp'), may hold values from -0.09375 to 0.09375
- w_gate: bfloat16 [2, 4096, 2048], P(None, 'sp', 'tp'), may hold values from -0.09375 to 0.09375
- conv_taps: float32 [2, 31, 2048], P(None, None, 'tp'), may hold values from -9 to 9
- norm_gain: float32 [2, 2048], P(None, 'tp'), may hold values from 0.1 to 1.9
- norm_shift: float32 [2, 2048], P(None, 'tp'), may hold values from -3 to 3
- w_out: bfloat16 [2, 2048, 4096], P(None, 'tp', 'sp'), may hold values from -0.125 to 0.125
Outputs:
- hidden_out: bfloat16 [3072, 4096], P(('grp', 'sp'), 'tp'), parts along dimension 0
The draws below stay inside these ranges and needn't reach their ends.
There are 2 independent parts, one for each index of `grp`. The reference program is written for one: setup_inputs(seed, part) draws one part's arguments, and reference() takes and returns one part's arrays. A program takes and returns all parts, laid end to end along the dimension named above; an argument that names none is the same for every part. Nothing has to cross between parts.
All inputs are finite; a program needn't handle non-finite values.
Results may differ from the reference program's by a relative error of at most 0.013.
Values may be sent and summed in bfloat16 or wider, within the bound.
A program may use at most 64 MiB of HBM per device.

```python
import math
import jax
import jax.numpy as jnp
from jax import lax

D = 4096
C = 2048
KERNEL = 31
LAYERS = 2
TOKENS = 1536
N_TP = 4


def draw_hidden_in(key, part):
    keys = jax.random.split(key, 3)
    base = jnp.clip(jax.random.normal(keys[0], (TOKENS, D), jnp.float32), -4.0, 4.0)
    ramp = 3.0 ** (jnp.arange(D, dtype=jnp.float32) / D - 0.5)
    column = ramp * jnp.exp(jax.random.uniform(keys[1], (D,), jnp.float32, math.log(0.6), math.log(1.6)))
    row_scale = jnp.exp(jax.random.uniform(keys[2], (TOKENS,), jnp.float32, math.log(0.4), math.log(2.5)))
    return (base * row_scale[:, None] * column[None, :]).astype(jnp.bfloat16)


def draw_conv_taps(key, part):
    keys = jax.random.split(key, 2)
    base = jnp.clip(jax.random.normal(keys[0], (LAYERS, KERNEL, C), jnp.float32), -4.0, 4.0)
    ramp = 3.0 ** (jnp.arange(C, dtype=jnp.float32) / C)
    channel = ramp * jnp.exp(jax.random.uniform(keys[1], (C,), jnp.float32, 0.0, math.log(4.0)))
    return base / math.sqrt(KERNEL) * channel[None, None, :]


def block_levels(own_key, extent, pieces, smallest, largest):
    level, own = 1.0, jax.random.fold_in(own_key, 6)
    for axis_at, parts in pieces:
        heights = jnp.exp(jax.random.uniform(jax.random.fold_in(own, axis_at), (parts,), jnp.float32, smallest / len(pieces), largest / len(pieces)))
        level = level * jnp.repeat(heights, extent[axis_at] // parts).reshape([-1 if axis == axis_at else 1 for axis in range(len(extent))])
    return level


def scatter_about(own_key, shape, spread, most, cuts=(), kind=jnp.bfloat16):
    drawn = spread * jax.random.normal(own_key, shape, jnp.float32)
    if cuts:
        drawn = drawn * block_levels(own_key, shape, cuts, -0.22, 0.18)
    return jnp.clip(drawn, -most, most).astype(kind)


def setup_inputs(seed: int = 0, part: int = 0) -> dict:
    key_of = jax.random.split(jax.random.key(seed), 9)
    own_keys = jax.random.split(jax.random.fold_in(key_of[8], part), 9)
    return {
        "hidden_in": draw_hidden_in(jax.random.fold_in(jax.random.fold_in(key_of[8], part), 71), part),
        "in_gain": jnp.clip(1.0 + 0.18 * jax.random.normal(key_of[1], (LAYERS, D), jnp.float32), 0.1, 1.9),
        "w_value": scatter_about(key_of[2], (LAYERS, D, C), D ** -0.5, 0.09375, ((1, 4), (2, 4))),
        "w_gate": scatter_about(key_of[3], (LAYERS, D, C), D ** -0.5, 0.09375, ((1, 4), (2, 4))),
        "conv_taps": draw_conv_taps(jax.random.fold_in(key_of[8], 71), part),
        "norm_gain": jnp.clip(1.0 + 0.18 * jax.random.normal(key_of[5], (LAYERS, C), jnp.float32), 0.1, 1.9),
        "norm_shift": scatter_about(key_of[6], (LAYERS, C), 0.5, 3.0, ((1, 4),), jnp.float32),
        "w_out": scatter_about(key_of[7], (LAYERS, C, D), C ** -0.5, 0.125, ((1, 4), (2, 4))),
    }


epsilon = 1e-06

def block_sum(mixed_out, weight):
    block_width = C // N_TP

    def add_block(block_index, running):
        offset = block_index.astype(jnp.int32) * block_width
        block_cols = lax.dynamic_slice_in_dim(mixed_out, offset, block_width, 1)
        block_rows = lax.dynamic_slice_in_dim(weight, offset, block_width, 0)
        partial_value = jnp.dot(block_cols, block_rows, preferred_element_type=jnp.float32).astype(jnp.bfloat16)
        partial_value = lax.optimization_barrier(partial_value)
        return running + partial_value.astype(jnp.float32)
    start_sum = jnp.zeros((mixed_out.shape[0], weight.shape[1]), jnp.float32)
    return lax.fori_loop(0, N_TP, add_block, start_sum)

def causal_taps(gated_wide, taps):
    row_total = gated_wide.shape[0]
    padded = jnp.concatenate([jnp.zeros((KERNEL - 1, gated_wide.shape[1]), jnp.float32), gated_wide], axis=0)

    def add_tap(tap_index, running):
        where = tap_index.astype(jnp.int32)
        window = lax.dynamic_slice_in_dim(padded, where, row_total, 0)
        weight_row = lax.dynamic_slice_in_dim(taps, where, 1, 0)
        return running + weight_row * window
    start_sum = jnp.zeros(gated_wide.shape, jnp.float32)
    return lax.fori_loop(0, KERNEL, add_tap, start_sum)

def reference(hidden_in, in_gain, w_value, w_gate, conv_taps, norm_gain, norm_shift, w_out):
    hidden = hidden_in
    for layer_idx in range(LAYERS):
        widened = hidden.astype(jnp.float32)
        inv_rms = lax.rsqrt(lax.optimization_barrier(jnp.mean(widened * widened, axis=1, keepdims=True)) + epsilon)
        normalized = (widened * inv_rms * in_gain[layer_idx]).astype(jnp.bfloat16)
        value_part = jnp.dot(normalized, w_value[layer_idx], preferred_element_type=jnp.float32)
        gate_part = jnp.dot(normalized, w_gate[layer_idx], preferred_element_type=jnp.float32)
        gated = (value_part * jax.nn.sigmoid(gate_part)).astype(jnp.bfloat16)
        conved = causal_taps(gated.astype(jnp.float32), conv_taps[layer_idx])
        row_mean = lax.optimization_barrier(jnp.mean(conved, axis=1, keepdims=True))
        variance = lax.optimization_barrier(jnp.mean(jnp.square(conved - row_mean), axis=1, keepdims=True))
        normed = (conved - row_mean) * lax.rsqrt(variance + epsilon) * norm_gain[layer_idx] + norm_shift[layer_idx]
        mixed_out = jax.nn.silu(normed).astype(jnp.bfloat16)
        branch = block_sum(mixed_out, w_out[layer_idx])
        hidden = (hidden.astype(jnp.float32) + branch).astype(jnp.bfloat16)
    return hidden
```

```python
import functools

import jax
import jax.numpy as jnp
from jax import lax
from jax.experimental import pallas as pl
from jax.experimental.pallas import tpu as pltpu
from jax.sharding import PartitionSpec as P

epsilon = 1e-06
CHUNK = 128
PIECES = (1, 1, 2)
F32, BF16 = jnp.float32, jnp.bfloat16


def kernel(
    S, T, h_ref, gain_ref, wv_ref, wg_ref, taps_ref, ng_ref, ns_ref, wo_ref, out_ref,
    WV, WG, WO, X, XG, ACC, GACC, EXT, CONV, MIX, PART, PRECV, SUMB, RECV, STAT, GSTAT, HB,
    own_sem, zr, zs_right, zs_left, yr, ys, dr, ds, xr, xs, xf, sr, ss, gr, gs, hr, hs, br, bs,
    pr, ps, rr, rs,
):
    L = wv_ref.shape[0]
    Ds, Cn = wv_ref.shape[1], wv_ref.shape[2]
    rows, Dt = h_ref.shape
    taps = taps_ref.shape[1]
    features, channels = Dt * T, Cn * T
    chips = T // 2
    halo = EXT.shape[1] - 2 * rows
    g, me, t = lax.axis_index("grp"), lax.axis_index("sp"), lax.axis_index("tp")
    core = lax.rem(t, 2)
    chip = lax.div(t, 2)
    partner = t + 1 - 2 * core
    MESH = pl.DeviceIdType.MESH
    both, either, no = jnp.logical_and, jnp.logical_or, jnp.logical_not
    first, last = me == 0, me == S - 1
    low, high = me == 1, me == S - 2
    edge, near = either(first, last), either(low, high)
    inward = jnp.where(first, 1, -1)
    outward = jnp.where(low, -1, 1)
    own_base = jnp.where(low, rows, 0)
    guest_base = jnp.where(low, 0, rows)

    def is_edge(plane):
        return either(plane == 0, plane == S - 1)

    table = []
    groups = []
    for layer in range(L):
        of_layer = []
        for which in range(3):
            ids = []
            for piece in range(PIECES[which]):
                ids.append(len(table))
                table.append((layer, which, piece, PIECES[which]))
            of_layer.append(ids)
        groups.append(of_layer)
    items = len(table)

    def direct(item):
        layer, which, _, _ = table[item]
        return (layer, which) != (0, 2)

    def folded(item):
        layer, which, _, _ = table[item]
        return layer == 0 and which < 2

    def inside(item, plane):
        low_end, high_end = (1, S - 2) if folded(item) else (0, S - 1)
        return both(plane >= low_end, plane <= high_end)

    def skips_y(item, owner):
        if not direct(item):
            return jnp.bool_(False)
        return either(both(owner == 0, low), both(owner == S - 1, high))

    sources = [(wv_ref, WV), (wg_ref, WG), (wo_ref, WO)]

    def own(layer, which):
        source, slots = sources[which]
        return pltpu.make_async_copy(source.at[layer], slots.at[layer, me], own_sem.at[layer, which])

    for layer in range(L):
        for which in range(3):
            own(layer, which).start()

    def each_chunk(body, size=CHUNK):
        def step(index, _):
            body(pl.ds(pl.multiple_of(index * size, size), size))
            return 0

        lax.fori_loop(0, rows // size, step, 0)

    def put_stat(slot, where, left, right):
        lane = lax.broadcasted_iota(jnp.int32, (left.shape[0], 128), 1)
        wide = jnp.where(lane == 0, left, right)
        STAT[slot, t, :, where] = wide.T[:8]

    def stat_copy(slot, peer):
        return pltpu.make_async_remote_copy(
            STAT.at[slot, t], STAT.at[slot, t], ss.at[slot, peer], sr.at[slot, t],
            device_id={"tp": peer}, device_id_type=MESH,
        )

    def stat_arrival(slot, peer):
        return pltpu.make_async_remote_copy(
            STAT.at[slot, peer], STAT.at[slot, peer], ss.at[slot, peer], sr.at[slot, peer],
            device_id={"tp": peer}, device_id_type=MESH,
        )

    def send_stat(slot):
        for shift in range(1, T):
            stat_copy(slot, lax.rem(t + shift, T)).start()

    def wait_stat(slot):
        for shift in range(1, T):
            stat_arrival(slot, lax.rem(t + shift, T)).wait_recv()

    def total_stat(stat, where):
        total = stat[0, :, where]
        for peer in range(1, T):
            total = total + stat[peer, :, where]
        return jnp.concatenate([total] * 16, axis=0).T

    def part_ref(item, owner, half):
        layer, which, piece, pieces = table[item]
        slots = sources[which][1]
        size = slots.shape[2] // (2 * pieces)
        start = pl.multiple_of(half * (size * pieces) + piece * size, size)
        return slots.at[layer, owner, pl.ds(start, size)]

    def zcopy(item, owner, way):
        ref = part_ref(item, owner, g)
        sems = zs_right if way > 0 else zs_left
        return pltpu.make_async_remote_copy(
            ref, ref, sems.at[item, owner], zr.at[item, owner],
            device_id={"sp": me + way}, device_id_type=MESH,
        )

    def dcopy(item, owner):
        ref = part_ref(item, owner, 1 - g)
        return pltpu.make_async_remote_copy(
            ref, ref, ds.at[item], dr.at[item], device_id={"sp": me + inward}, device_id_type=MESH,
        )

    def ycopy(item, owner):
        ref = part_ref(item, owner, g)
        return pltpu.make_async_remote_copy(
            ref, ref, ys.at[item, owner], yr.at[item, owner],
            device_id={"grp": 1 - g}, device_id_type=MESH,
        )

    def yarrival(item, owner):
        ref = part_ref(item, owner, 1 - g)
        return pltpu.make_async_remote_copy(
            ref, ref, ys.at[item, owner], yr.at[item, owner],
            device_id={"grp": 1 - g}, device_id_type=MESH,
        )

    def outgoing(way):
        return low if way < 0 else high

    def send_out(ids):
        for item in ids:
            for way in (1, -1):

                @pl.when(outgoing(way))
                def _(item=item, way=way):
                    zcopy(item, me, way).start()

    def send_own(ids):
        for item in ids:
            for way in (1, -1):
                allowed = inside(item, me + way)
                if not folded(item):
                    allowed = both(allowed, no(outgoing(way)))

                @pl.when(allowed)
                def _(item=item, way=way):
                    zcopy(item, me, way).start()

    def send_direct(ids):
        for item in ids:
            if direct(item):
                dcopy(item, me).start()

    def take(ids, k, select=None):
        for item in ids:
            for way in (1, -1):
                owner = me - way * k
                ok = both(both(owner >= 0, owner < S), inside(item, me))
                if select is not None:
                    ok = both(ok, select(owner))

                @pl.when(ok)
                def _(item=item, way=way, owner=owner):
                    zcopy(item, owner, way).wait_recv()

                    @pl.when(inside(item, me + way))
                    def _():
                        zcopy(item, owner, way).start()

                    @pl.when(no(skips_y(item, owner)))
                    def _():
                        ycopy(item, owner).start()

    def arrive(ids, owner):
        for item in ids:
            skip = skips_y(item, owner)

            @pl.when(no(skip))
            def _(item=item):
                yarrival(item, owner).wait_recv()

            @pl.when(skip)
            def _(item=item):
                dcopy(item, owner).wait_recv()

    def x_ref(slot, source):
        return XG.at[source] if slot == L else X.at[slot, source]

    def xcopy(slot, source, peer, sem):
        return pltpu.make_async_remote_copy(
            x_ref(slot, source), x_ref(slot, source), sem, xr.at[slot, source],
            device_id={"tp": peer}, device_id_type=MESH,
        )

    def make_x(layer):
        source = h_ref if layer == 0 else HB

        def body(where):
            wide = source[where, :].astype(F32)
            X[layer, t, where, :] = (wide * gain_ref[layer : layer + 1, :]).astype(BF16)
            squares = jnp.sum(wide * wide, axis=1, keepdims=True)
            put_stat(2 * layer, where, squares, squares)

        each_chunk(body)

    def send_x(slot):
        for shift in range(1, chips):
            peer = lax.rem(chip + shift, chips) * 2 + core
            xcopy(slot, t, peer, xs.at[slot, shift]).start()
        xcopy(slot, t, partner, xs.at[slot, 0]).start()

    def relay_x(slot):
        for shift in range(1, chips):
            source = lax.rem(chip + shift, chips) * 2 + core
            xcopy(slot, source, partner, xf.at[slot, shift]).wait_recv()
            xcopy(slot, source, partner, xf.at[slot, shift]).start()

    def wait_x(slot):
        for shift in range(chips):
            source = lax.rem(chip + shift, chips) * 2 + 1 - core
            xcopy(slot, source, partner, xf.at[slot, 0]).wait_recv()

    def guest_x_copy():
        return pltpu.make_async_remote_copy(
            X.at[0, t], XG.at[t], xs.at[L, 0], xr.at[L, t],
            device_id={"sp": me + inward}, device_id_type=MESH,
        )

    def guest_stat_copy():
        return pltpu.make_async_remote_copy(
            STAT.at[0, t], GSTAT.at[t], gs.at[t], gr.at[t],
            device_id={"sp": me + inward}, device_id_type=MESH,
        )

    def guest_stat_pass(source, peer):
        return pltpu.make_async_remote_copy(
            GSTAT.at[source], GSTAT.at[source], gs.at[peer], gr.at[source],
            device_id={"tp": peer}, device_id_type=MESH,
        )

    def guest_back(index):
        start = pl.multiple_of(index * CHUNK + halo, 16)
        return pltpu.make_async_remote_copy(
            EXT.at[0, pl.ds(pl.multiple_of(guest_base + start, 16), CHUNK)],
            EXT.at[0, pl.ds(start, CHUNK)],
            bs.at[index], br.at[index],
            device_id={"sp": me + outward}, device_id_type=MESH,
        )

    def at_distance(k, body, select=None):
        if k == 0:
            body(me)
            return

        def step(index, _):
            owner = me + k - 2 * k * index
            ok = both(owner >= 0, owner < S)
            if select is not None:
                ok = both(ok, select(owner))

            @pl.when(ok)
            def _():
                body(owner)

            return 0

        lax.fori_loop(0, 2, step, 0)

    def multiply(total, x, layer, owner, start):
        at = lax.div(owner * Ds, Dt)
        columns = pl.ds(pl.multiple_of(lax.rem(owner * Ds, Dt), 128), Ds)
        xs_block = x[at, :, columns]
        for which, slots in ((0, WV), (1, WG)):
            part = jnp.dot(xs_block, slots[layer, owner], preferred_element_type=F32)
            if start:
                total[which] = part
            else:
                total[which] += part

    def project(layer, k, select=None):
        def block(owner):
            if k > 0:
                arrive(groups[layer][0] + groups[layer][1], owner)
            multiply(ACC, X.at[layer], layer, owner, k == 0)

        at_distance(k, block, select)

    def halo_copy(layer):
        end = halo + rows + (own_base if layer == 0 else 0)
        return pltpu.make_async_remote_copy(
            EXT.at[layer, pl.ds(pl.multiple_of(end - halo, 16), halo)],
            EXT.at[layer, pl.ds(0, halo)],
            hs.at[layer], hr.at[layer],
            device_id={"sp": me + 1}, device_id_type=MESH,
        )

    def sends_halo(layer):
        return both(no(last), no(first)) if layer == 0 else no(last)

    def takes_halo(layer):
        return both(no(first), no(low)) if layer == 0 else no(first)

    def gate_rows(layer, total, stat, base, where):
        mean = total_stat(stat, where)[:, :1] / features
        inv = lax.rsqrt(mean + epsilon)
        value, gating = total[0, where, :] * inv, total[1, where, :] * inv
        gated = (value / (1.0 + jnp.exp(-gating))).astype(BF16)
        EXT[layer, pl.ds(pl.multiple_of(base + where.start + halo, 16), where.size), :] = gated

    def gate(layer):
        base = own_base if layer == 0 else 0
        each_chunk(functools.partial(gate_rows, layer, ACC, STAT.at[2 * layer], base))

        @pl.when(sends_halo(layer))
        def _():
            halo_copy(layer).start()

    def convolve(layer):
        @pl.when(first)
        def _():
            EXT[layer, pl.ds(0, halo), :] = jnp.zeros((halo, Cn), BF16)

        @pl.when(takes_halo(layer))
        def _():
            halo_copy(layer).wait_recv()

        tall = CHUNK + halo + 8
        offset = halo - (taps - 1)
        base = own_base if layer == 0 else 0

        def body(where):
            if layer == 0:

                @pl.when(edge)
                def _():
                    guest_back(lax.div(where.start, CHUNK)).wait_recv()

            for column in range(0, Cn, 128):
                at = pl.ds(column, 128)
                window = EXT[layer, pl.ds(pl.multiple_of(base + where.start, 16), CHUNK + halo), at]
                tile = jnp.concatenate([window.astype(F32), jnp.zeros((8, 128), F32)], axis=0)
                total = jnp.zeros((CHUNK, 128), F32)
                for residue in range(8):
                    ks = [k for k in range(taps) if (k + offset) % 8 == residue]
                    if not ks:
                        continue
                    turned = pltpu.roll(tile, tall - residue, 0) if residue else tile
                    for k in ks:
                        low_row = k + offset - residue
                        total = total + taps_ref[layer, k : k + 1, at] * turned[low_row : low_row + CHUNK]
                CONV[where, at] = total
            conved = CONV[where, :]
            put_stat(
                2 * layer + 1, where,
                jnp.sum(conved, axis=1, keepdims=True),
                jnp.sum(conved * conved, axis=1, keepdims=True),
            )

        each_chunk(body)
        send_stat(2 * layer + 1)

    def mix(layer):
        wait_stat(2 * layer + 1)

        def body(where):
            stat = total_stat(STAT.at[2 * layer + 1], where)
            mean = stat[:, 0:1] / channels
            spread = stat[:, 1:2] / channels - mean * mean
            normed = (CONV[where, :] - mean) * lax.rsqrt(spread + epsilon) * ng_ref[
                layer : layer + 1, :
            ] + ns_ref[layer : layer + 1, :]
            MIX[where, :] = (normed / (1.0 + jnp.exp(-normed))).astype(BF16)

        each_chunk(body)

    def pair_copy(layer, at):
        return pltpu.make_async_remote_copy(
            PART.at[layer, 2 * at + 1 - core], PRECV.at[layer, at], ps.at[layer, at], pr.at[layer, at],
            device_id={"tp": partner}, device_id_type=MESH,
        )

    def sum_copy(layer, at):
        return pltpu.make_async_remote_copy(
            SUMB.at[layer, at], RECV.at[layer, chip], rs.at[layer, at], rr.at[layer, chip],
            device_id={"tp": at * 2 + core}, device_id_type=MESH,
        )

    def sum_arrival(layer, at):
        return pltpu.make_async_remote_copy(
            SUMB.at[layer, at], RECV.at[layer, at], rs.at[layer, at], rr.at[layer, at],
            device_id={"tp": at * 2 + core}, device_id_type=MESH,
        )

    def sum_pair(layer, at):
        pair_copy(layer, at).wait_recv()

        def body(where):
            SUMB[layer, at, where, :] = (
                PART[layer, at * 2 + core, where, :].astype(F32) + PRECV[layer, at, where, :].astype(F32)
            ).astype(BF16)

        each_chunk(body)
        sum_copy(layer, at).start()

    def branch(layer, k):
        def block(owner):
            if k > 0:
                arrive(groups[layer][2], owner)
            target = lax.div(owner * Ds, Dt)
            columns = pl.ds(pl.multiple_of(lax.rem(owner * Ds, Dt), 128), Ds)
            PART[layer, target, :, columns] = jnp.dot(
                MIX[...], WO[layer, owner], preferred_element_type=F32
            ).astype(BF16)
            if S == T:
                at = lax.div(target, 2)

                @pl.when(lax.rem(target, 2) != core)
                def _():
                    pair_copy(layer, at).start()

                @pl.when(both(lax.rem(target, 2) == core, at != chip))
                def _():
                    sum_pair(layer, at)

        at_distance(k, block)
        if S != T and k == S - 1:
            for shift in list(range(1, chips)) + [0]:
                pair_copy(layer, lax.rem(chip + shift, chips)).start()
            for shift in range(1, chips):
                sum_pair(layer, lax.rem(chip + shift, chips))

    def finish(layer):
        pair_copy(layer, chip).wait_recv()
        for shift in range(1, chips):
            sum_arrival(layer, lax.rem(chip + shift, chips)).wait_recv()
        source = h_ref if layer == 0 else HB
        target = out_ref if layer == L - 1 else HB

        def body(where):
            total = PART[layer, t, where, :].astype(F32) + PRECV[layer, chip, where, :].astype(F32)
            for shift in range(1, chips):
                total = total + RECV[layer, lax.rem(chip + shift, chips), where, :].astype(F32)
            target[where, :] = (source[where, :].astype(F32) + total).astype(BF16)

        each_chunk(body)

    barrier = pltpu.get_barrier_semaphore()
    for shift in range(1, T):
        pl.semaphore_signal(barrier, inc=1, device_id={"tp": lax.rem(t + shift, T)}, device_id_type=MESH)
    pl.semaphore_signal(barrier, inc=1, device_id={"grp": 1 - g}, device_id_type=MESH)

    @pl.when(no(first))
    def _():
        pl.semaphore_signal(barrier, inc=1, device_id={"sp": me - 1}, device_id_type=MESH)

    @pl.when(no(last))
    def _():
        pl.semaphore_signal(barrier, inc=1, device_id={"sp": me + 1}, device_id_type=MESH)

    inner = jnp.where(first, 0, 1) + jnp.where(last, 0, 1)
    pl.semaphore_wait(barrier, T + inner)

    value0, gating0, out0 = groups[0]
    later = [item for of_layer in groups[1:] for ids in of_layer for item in ids]
    for which in range(2):
        own(0, which).wait()
        send_own(groups[0][which])
    own(0, 2).wait()
    send_out(out0)
    for layer in range(1, L):
        for which in range(3):
            own(layer, which).wait()
            send_out(groups[layer][which])
    make_x(0)

    @pl.when(edge)
    def _():
        guest_x_copy().start()
        guest_stat_copy().start()
        send_direct(value0 + gating0)
        send_own(out0)
        send_direct(out0)
        for layer in range(1, L):
            send_own(groups[layer][0] + groups[layer][1])
            send_direct(groups[layer][0] + groups[layer][1])
            send_own(groups[layer][2])
        take(out0 + later, 1)

    def owned_inside(owner):
        return no(is_edge(owner))

    @pl.when(no(edge))
    def _():
        send_x(0)
        send_stat(0)
        take(value0 + gating0, 1)
        send_own(out0)
        relay_x(0)
        wait_x(0)
        project(0, 0)
        for k in range(2, S - 1):
            take(value0, k)
            if k == 2:

                @pl.when(near)
                def _():
                    xcopy(L, t, partner, xf.at[L, 0]).wait_recv()
                    guest_stat_pass(t, partner).wait_recv()
                    send_x(L)
                    for shift in range(1, T):
                        guest_stat_pass(t, lax.rem(t + shift, T)).start()

            take(gating0, k)
            project(0, k - 1, lambda owner: no(skips_y(value0[0], owner)))
        take(out0, 1, owned_inside)

        @pl.when(near)
        def _():
            relay_x(L)
            wait_x(L)
            for shift in range(1, T):
                guest_stat_pass(lax.rem(t + shift, T), partner).wait_recv()

        project(0, S - 2)
        wait_stat(0)

        @pl.when(near)
        def _():
            corner = jnp.where(low, 0, S - 1)
            arrive(value0 + gating0, corner)
            multiply(ACC, X.at[0], 0, corner, False)
            multiply(GACC, XG, 0, me, True)

            def add(index, _):
                owner = lax.rem(me + index, S)
                multiply(GACC, XG, 0, owner, False)
                return 0

            lax.fori_loop(1, S, add, 0)

            def back(where):
                gate_rows(0, GACC, GSTAT, guest_base, where)
                guest_back(lax.div(where.start, CHUNK)).start()

            each_chunk(back)

        gate(0)
        if L > 1:
            send_own(groups[1][0] + groups[1][1])

    for layer in range(L):
        value, gating, out = groups[layer]
        convolve(layer)
        if layer == 0:

            @pl.when(no(edge))
            def _():
                take(out0, 1, is_edge)

        else:

            @pl.when(no(edge))
            def _(out=out):
                take(out, 1)

        mix(layer)
        ahead = groups[layer + 1] if layer + 1 < L else None
        if ahead:

            @pl.when(no(edge))
            def _(ahead=ahead):
                take(ahead[0], 1)

        branch(layer, 0)
        take(out, 2)
        if ahead:

            @pl.when(no(edge))
            def _(ahead=ahead):
                take(ahead[1], 1)
                send_own(ahead[2])

        branch(layer, 1)
        for k in range(3, S):
            take(out, k)
            branch(layer, k - 1)
        branch(layer, S - 1)
        finish(layer)
        if ahead:
            make_x(layer + 1)
            send_x(layer + 1)
            send_stat(2 * layer + 2)
            take(ahead[0], 2)
            relay_x(layer + 1)
            take(ahead[1], 2)
            wait_x(layer + 1)
            project(layer + 1, 0)
            project(layer + 1, 1)
            for k in range(3, S):
                take(ahead[0] + ahead[1], k)
                project(layer + 1, k - 1)
            project(layer + 1, S - 1)
            wait_stat(2 * layer + 2)
            gate(layer + 1)

            @pl.when(edge)
            def _(ahead=ahead):
                send_direct(ahead[2])

            if layer + 2 < L:

                @pl.when(no(edge))
                def _(layer=layer):
                    send_own(groups[layer + 2][0] + groups[layer + 2][1])

    for item in range(items):

        def drain(owner, _, item=item):
            mine = owner == me
            had = either(mine, inside(item, me))

            @pl.when(both(both(owner <= me, inside(item, me + 1)), had))
            def _():
                zcopy(item, owner, 1).wait_send()

            @pl.when(both(both(owner >= me, inside(item, me - 1)), had))
            def _():
                zcopy(item, owner, -1).wait_send()

            @pl.when(both(no(mine), both(inside(item, me), no(skips_y(item, owner)))))
            def _():
                ycopy(item, owner).wait_send()

            return 0

        lax.fori_loop(0, S, drain, 0)
        if direct(item):

            @pl.when(edge)
            def _(item=item):
                dcopy(item, me).wait_send()

    def drain_x(slot):
        for shift in range(chips):
            xcopy(slot, t, partner, xs.at[slot, shift]).wait_send()
        for shift in range(1, chips):
            xcopy(slot, t, partner, xf.at[slot, shift]).wait_send()

    def drain_stat(slot):
        for shift in range(1, T):
            stat_copy(slot, lax.rem(t + shift, T)).wait_send()

    @pl.when(edge)
    def _():
        guest_x_copy().wait_send()
        guest_stat_copy().wait_send()

    @pl.when(no(edge))
    def _():
        drain_x(0)
        drain_stat(0)

    @pl.when(near)
    def _():
        drain_x(L)
        for shift in range(1, T):
            guest_stat_pass(t, lax.rem(t + shift, T)).wait_send()
        for index in range(rows // CHUNK):
            guest_back(index).wait_send()

    for layer in range(L):
        if layer > 0:
            drain_x(layer)
            drain_stat(2 * layer)
        drain_stat(2 * layer + 1)
        for shift in range(chips):
            pair_copy(layer, lax.rem(chip + shift, chips)).wait_send()
        for shift in range(1, chips):
            sum_copy(layer, lax.rem(chip + shift, chips)).wait_send()

        @pl.when(sends_halo(layer))
        def _(layer=layer):
            halo_copy(layer).wait_send()


def shards(hidden_in, in_gain, w_value, w_gate, conv_taps, norm_gain, norm_shift, w_out):
    S, T = lax.axis_size("sp"), lax.axis_size("tp")
    L, Ds, Cn = w_value.shape
    rows, Dt = hidden_in.shape
    chips = T // 2
    halo = (conv_taps.shape[1] - 1 + 15) // 16 * 16
    items = L * sum(PIECES)
    vmem = pl.BlockSpec(memory_space=pltpu.VMEM)
    hbm = pl.BlockSpec(memory_space=pl.ANY)
    dma = pltpu.SemaphoreType.DMA
    return pl.pallas_call(
        functools.partial(kernel, S, T),
        out_shape=jax.ShapeDtypeStruct((rows, Dt), BF16),
        in_specs=[vmem, vmem, hbm, hbm, vmem, vmem, vmem, hbm],
        out_specs=vmem,
        scratch_shapes=[
            pltpu.VMEM((L, S, Ds, Cn), BF16),
            pltpu.VMEM((L, S, Ds, Cn), BF16),
            pltpu.VMEM((L, S, Cn, Ds), BF16),
            pltpu.VMEM((L, T, rows, Dt), BF16),
            pltpu.VMEM((T, rows, Dt), BF16),
            pltpu.VMEM((2, rows, Cn), F32),
            pltpu.VMEM((2, rows, Cn), F32),
            pltpu.VMEM((L, halo + 2 * rows, Cn), BF16),
            pltpu.VMEM((rows, Cn), F32),
            pltpu.VMEM((rows, Cn), BF16),
            pltpu.VMEM((L, T, rows, Dt), BF16),
            pltpu.VMEM((L, chips, rows, Dt), BF16),
            pltpu.VMEM((L, chips, rows, Dt), BF16),
            pltpu.VMEM((L, chips, rows, Dt), BF16),
            pltpu.VMEM((2 * L, T, 8, rows), F32),
            pltpu.VMEM((T, 8, rows), F32),
            pltpu.VMEM((rows, Dt), BF16),
            dma((L, 3)),
            dma((items, S)), dma((items, S)), dma((items, S)), dma((items, S)), dma((items, S)),
            dma((items,)), dma((items,)),
            dma((L + 1, T)), dma((L + 1, chips)), dma((L + 1, chips)),
            dma((2 * L, T)), dma((2 * L, T)),
            dma((T,)), dma((T,)),
            dma((L,)), dma((L,)),
            dma((rows // CHUNK,)), dma((rows // CHUNK,)),
            dma((L, chips)), dma((L, chips)),
            dma((L, chips)), dma((L, chips)),
        ],
        compiler_params=pltpu.CompilerParams(
            collective_id=0, has_side_effects=True, vmem_limit_bytes=64_000_000
        ),
    )(hidden_in, in_gain, w_value, w_gate, conv_taps, norm_gain, norm_shift, w_out)


def solution(mesh):
    placed = (
        P(("grp", "sp"), "tp"),
        P(None, "tp"),
        P(None, "sp", "tp"),
        P(None, "sp", "tp"),
        P(None, None, "tp"),
        P(None, "tp"),
        P(None, "tp"),
        P(None, "tp", "sp"),
    )
    return jax.shard_map(
        shards, mesh=mesh, in_specs=placed, out_specs=P(("grp", "sp"), "tp"), check_vma=False
    )
```

```python
import functools

import jax
import jax.numpy as jnp
from jax import lax
from jax.experimental import pallas as pl
from jax.experimental.pallas import tpu as pltpu
from jax.sharding import PartitionSpec as P

epsilon = 1e-06
CHUNK = 128
F32, BF16 = jnp.float32, jnp.bfloat16


def cuts(Ds):
    return (2, 2, 2) if Ds >= 512 else (1, 1, 1)


def kernel(
    S, T, h_ref, gain_ref, wv_ref, wg_ref, taps_ref, ng_ref, ns_ref, wo_ref, out_ref,
    WV, WG, WO, X, XG, ACC, GACC, EXT, CONV, MIX, PART, PRECV, SUMB, RECV, STAT, GSTAT, HB,
    own_sem, zr, zs_right, zs_left, yr, ys, dr, ds, xr, xs, xf, sr, ss, gr, gs, hr, hs, br, bs,
    pr, ps, rr, rs,
):
    L = wv_ref.shape[0]
    Ds, Cn = wv_ref.shape[1], wv_ref.shape[2]
    rows, Dt = h_ref.shape
    taps = taps_ref.shape[1]
    features, channels = Dt * T, Cn * T
    chips = T // 2
    pieces_of = cuts(Ds)
    Q, Dq = WO.shape[2], WO.shape[4]
    halo = EXT.shape[1] - 2 * rows
    g, me, t = lax.axis_index("grp"), lax.axis_index("sp"), lax.axis_index("tp")
    core = lax.rem(t, 2)
    chip = lax.div(t, 2)
    partner = t + 1 - 2 * core
    MESH = pl.DeviceIdType.MESH
    both, either, no = jnp.logical_and, jnp.logical_or, jnp.logical_not
    first, last = me == 0, me == S - 1
    low, high = me == 1, me == S - 2
    edge, near = either(first, last), either(low, high)
    inward = jnp.where(first, 1, -1)
    outward = jnp.where(low, -1, 1)
    own_base = jnp.where(low, rows, 0)
    guest_base = jnp.where(low, 0, rows)

    def is_edge(plane):
        return either(plane == 0, plane == S - 1)

    table = []
    groups = []
    for layer in range(L):
        of_layer = []
        for which in range(3):
            ids = []
            for piece in range(pieces_of[which]):
                ids.append(len(table))
                table.append((layer, which, piece, pieces_of[which]))
            of_layer.append(ids)
        groups.append(of_layer)
    items = len(table)

    def direct(item):
        layer, which, piece, _ = table[item]
        return (layer, which) != (0, 1) or piece == 0

    def folded(item):
        layer, which, _, _ = table[item]
        return layer == 0 and which < 2

    def inside(item, plane):
        low_end, high_end = (1, S - 2) if folded(item) else (0, S - 1)
        return both(plane >= low_end, plane <= high_end)

    def skips_y(item, owner):
        if not direct(item):
            return jnp.bool_(False)
        return either(both(owner == 0, low), both(owner == S - 1, high))

    sources = [(wv_ref, WV), (wg_ref, WG), (wo_ref, WO)]

    def own(layer, which):
        source, slots = sources[which]
        if which < 2:
            return [pltpu.make_async_copy(source.at[layer], slots.at[layer, me], own_sem.at[layer, which])]
        return [
            pltpu.make_async_copy(
                source.at[layer, :, pl.ds(q * Dq, Dq)], slots.at[layer, me, q], own_sem.at[layer, 2 + q]
            )
            for q in range(Q)
        ]

    for layer in range(L):
        for which in range(3):
            for copy in own(layer, which):
                copy.start()

    def own_wait(layer, which):
        for copy in own(layer, which):
            copy.wait()

    def each_chunk(body, size=CHUNK):
        def step(index, _):
            body(pl.ds(pl.multiple_of(index * size, size), size))
            return 0

        lax.fori_loop(0, rows // size, step, 0)

    def put_stat(slot, where, left, right):
        lane = lax.broadcasted_iota(jnp.int32, (left.shape[0], 128), 1)
        wide = jnp.where(lane == 0, left, right)
        STAT[slot, t, :, where] = wide.T[:8]

    def stat_copy(slot, peer):
        return pltpu.make_async_remote_copy(
            STAT.at[slot, t], STAT.at[slot, t], ss.at[slot, peer], sr.at[slot, t],
            device_id={"tp": peer}, device_id_type=MESH,
        )

    def stat_arrival(slot, peer):
        return pltpu.make_async_remote_copy(
            STAT.at[slot, peer], STAT.at[slot, peer], ss.at[slot, peer], sr.at[slot, peer],
            device_id={"tp": peer}, device_id_type=MESH,
        )

    def send_stat(slot):
        for shift in range(1, T):
            stat_copy(slot, lax.rem(t + shift, T)).start()

    def wait_stat(slot):
        for shift in range(1, T):
            stat_arrival(slot, lax.rem(t + shift, T)).wait_recv()

    def total_stat(stat, where):
        total = stat[0, :, where]
        for peer in range(1, T):
            total = total + stat[peer, :, where]
        return jnp.concatenate([total] * 16, axis=0).T

    def part_ref(item, owner, half):
        layer, which, piece, pieces = table[item]
        slots = sources[which][1]
        if which == 2:
            return slots.at[layer, owner, half * pieces + piece]
        size = slots.shape[2] // (2 * pieces)
        start = pl.multiple_of(half * (size * pieces) + piece * size, size)
        return slots.at[layer, owner, pl.ds(start, size)]

    def zcopy(item, owner, way):
        ref = part_ref(item, owner, g)
        sems = zs_right if way > 0 else zs_left
        return pltpu.make_async_remote_copy(
            ref, ref, sems.at[item, owner], zr.at[item, owner],
            device_id={"sp": me + way}, device_id_type=MESH,
        )

    def dcopy(item, owner):
        ref = part_ref(item, owner, 1 - g)
        return pltpu.make_async_remote_copy(
            ref, ref, ds.at[item], dr.at[item], device_id={"sp": me + inward}, device_id_type=MESH,
        )

    def ycopy(item, owner):
        ref = part_ref(item, owner, g)
        return pltpu.make_async_remote_copy(
            ref, ref, ys.at[item, owner], yr.at[item, owner],
            device_id={"grp": 1 - g}, device_id_type=MESH,
        )

    def yarrival(item, owner):
        ref = part_ref(item, owner, 1 - g)
        return pltpu.make_async_remote_copy(
            ref, ref, ys.at[item, owner], yr.at[item, owner],
            device_id={"grp": 1 - g}, device_id_type=MESH,
        )

    def outgoing(way):
        return low if way < 0 else high

    def send_out(ids):
        for item in ids:
            for way in (1, -1):

                @pl.when(outgoing(way))
                def _(item=item, way=way):
                    zcopy(item, me, way).start()

    def send_own(ids):
        for item in ids:
            for way in (1, -1):
                allowed = inside(item, me + way)
                if not folded(item):
                    allowed = both(allowed, no(outgoing(way)))

                @pl.when(allowed)
                def _(item=item, way=way):
                    zcopy(item, me, way).start()

    def send_direct(ids):
        for item in ids:
            if direct(item):
                dcopy(item, me).start()

    def take(ids, k, select=None):
        for item in ids:
            for way in (1, -1):
                owner = me - way * k
                ok = both(both(owner >= 0, owner < S), inside(item, me))
                if select is not None:
                    ok = both(ok, select(owner))

                @pl.when(ok)
                def _(item=item, way=way, owner=owner):
                    zcopy(item, owner, way).wait_recv()

                    @pl.when(inside(item, me + way))
                    def _():
                        zcopy(item, owner, way).start()

                    @pl.when(no(skips_y(item, owner)))
                    def _():
                        ycopy(item, owner).start()

    def arrive(ids, owner):
        for item in ids:
            skip = skips_y(item, owner)

            @pl.when(no(skip))
            def _(item=item):
                yarrival(item, owner).wait_recv()

            @pl.when(skip)
            def _(item=item):
                dcopy(item, owner).wait_recv()

    def x_ref(slot, source):
        return XG.at[source] if slot == L else X.at[slot, source]

    def xcopy(slot, source, peer, sem):
        return pltpu.make_async_remote_copy(
            x_ref(slot, source), x_ref(slot, source), sem, xr.at[slot, source],
            device_id={"tp": peer}, device_id_type=MESH,
        )

    def make_x(layer):
        source = h_ref if layer == 0 else HB

        def body(where):
            wide = source[where, :].astype(F32)
            X[layer, t, where, :] = (wide * gain_ref[layer : layer + 1, :]).astype(BF16)
            squares = jnp.sum(wide * wide, axis=1, keepdims=True)
            put_stat(2 * layer, where, squares, squares)

        each_chunk(body)

    def send_x(slot):
        for shift in range(1, chips):
            peer = lax.rem(chip + shift, chips) * 2 + core
            xcopy(slot, t, peer, xs.at[slot, shift]).start()
        xcopy(slot, t, partner, xs.at[slot, 0]).start()

    def relay_x(slot):
        for shift in range(1, chips):
            source = lax.rem(chip + shift, chips) * 2 + core
            xcopy(slot, source, partner, xf.at[slot, shift]).wait_recv()
            xcopy(slot, source, partner, xf.at[slot, shift]).start()

    def wait_x(slot):
        for shift in range(chips):
            source = lax.rem(chip + shift, chips) * 2 + 1 - core
            xcopy(slot, source, partner, xf.at[slot, 0]).wait_recv()

    def guest_x_copy():
        return pltpu.make_async_remote_copy(
            X.at[0, t], XG.at[t], xs.at[L, 0], xr.at[L, t],
            device_id={"sp": me + inward}, device_id_type=MESH,
        )

    def guest_stat_copy():
        return pltpu.make_async_remote_copy(
            STAT.at[0, t], GSTAT.at[t], gs.at[t], gr.at[t],
            device_id={"sp": me + inward}, device_id_type=MESH,
        )

    def guest_stat_pass(source, peer):
        return pltpu.make_async_remote_copy(
            GSTAT.at[source], GSTAT.at[source], gs.at[peer], gr.at[source],
            device_id={"tp": peer}, device_id_type=MESH,
        )

    def guest_back(index):
        start = pl.multiple_of(index * CHUNK + halo, 16)
        return pltpu.make_async_remote_copy(
            EXT.at[0, pl.ds(pl.multiple_of(guest_base + start, 16), CHUNK)],
            EXT.at[0, pl.ds(start, CHUNK)],
            bs.at[index], br.at[index],
            device_id={"sp": me + outward}, device_id_type=MESH,
        )

    def at_distance(k, body, select=None):
        if k == 0:
            body(me)
            return

        def step(index, _):
            owner = me + k - 2 * k * index
            ok = both(owner >= 0, owner < S)
            if select is not None:
                ok = both(ok, select(owner))

            @pl.when(ok)
            def _():
                body(owner)

            return 0

        lax.fori_loop(0, 2, step, 0)

    def multiply(total, x, layer, owner, start):
        at = lax.div(owner * Ds, Dt)
        columns = pl.ds(pl.multiple_of(lax.rem(owner * Ds, Dt), 128), Ds)
        xs_block = x[at, :, columns]
        for which, slots in ((0, WV), (1, WG)):
            part = jnp.dot(xs_block, slots[layer, owner], preferred_element_type=F32)
            if start:
                total[which] = part
            else:
                total[which] += part

    def project(layer, k, select=None):
        def block(owner):
            if k > 0:
                arrive(groups[layer][0] + groups[layer][1], owner)
            multiply(ACC, X.at[layer], layer, owner, k == 0)

        at_distance(k, block, select)

    def halo_copy(layer):
        end = halo + rows + (own_base if layer == 0 else 0)
        return pltpu.make_async_remote_copy(
            EXT.at[layer, pl.ds(pl.multiple_of(end - halo, 16), halo)],
            EXT.at[layer, pl.ds(0, halo)],
            hs.at[layer], hr.at[layer],
            device_id={"sp": me + 1}, device_id_type=MESH,
        )

    def sends_halo(layer):
        return both(no(last), no(first)) if layer == 0 else no(last)

    def takes_halo(layer):
        return both(no(first), no(low)) if layer == 0 else no(first)

    def gate_rows(layer, total, stat, base, where):
        mean = total_stat(stat, where)[:, :1] / features
        inv = lax.rsqrt(mean + epsilon)
        value, gating = total[0, where, :] * inv, total[1, where, :] * inv
        gated = (value / (1.0 + jnp.exp(-gating))).astype(BF16)
        EXT[layer, pl.ds(pl.multiple_of(base + where.start + halo, 16), where.size), :] = gated

    def gate(layer):
        base = own_base if layer == 0 else 0
        each_chunk(functools.partial(gate_rows, layer, ACC, STAT.at[2 * layer], base))

        @pl.when(sends_halo(layer))
        def _():
            halo_copy(layer).start()

    def convolve(layer):
        @pl.when(first)
        def _():
            EXT[layer, pl.ds(0, halo), :] = jnp.zeros((halo, Cn), BF16)

        @pl.when(takes_halo(layer))
        def _():
            halo_copy(layer).wait_recv()

        tall = CHUNK + halo + 8
        offset = halo - (taps - 1)
        base = own_base if layer == 0 else 0

        def body(where):
            if layer == 0:

                @pl.when(edge)
                def _():
                    guest_back(lax.div(where.start, CHUNK)).wait_recv()

            for column in range(0, Cn, 128):
                at = pl.ds(column, 128)
                window = EXT[layer, pl.ds(pl.multiple_of(base + where.start, 16), CHUNK + halo), at]
                tile = jnp.concatenate([window.astype(F32), jnp.zeros((8, 128), F32)], axis=0)
                total = jnp.zeros((CHUNK, 128), F32)
                for residue in range(8):
                    ks = [k for k in range(taps) if (k + offset) % 8 == residue]
                    if not ks:
                        continue
                    turned = pltpu.roll(tile, tall - residue, 0) if residue else tile
                    for k in ks:
                        low_row = k + offset - residue
                        total = total + taps_ref[layer, k : k + 1, at] * turned[low_row : low_row + CHUNK]
                CONV[where, at] = total
            conved = CONV[where, :]
            put_stat(
                2 * layer + 1, where,
                jnp.sum(conved, axis=1, keepdims=True),
                jnp.sum(conved * conved, axis=1, keepdims=True),
            )

        each_chunk(body)
        send_stat(2 * layer + 1)

    def mix(layer):
        wait_stat(2 * layer + 1)

        def body(where):
            stat = total_stat(STAT.at[2 * layer + 1], where)
            mean = stat[:, 0:1] / channels
            spread = stat[:, 1:2] / channels - mean * mean
            normed = (CONV[where, :] - mean) * lax.rsqrt(spread + epsilon) * ng_ref[
                layer : layer + 1, :
            ] + ns_ref[layer : layer + 1, :]
            MIX[where, :] = (normed / (1.0 + jnp.exp(-normed))).astype(BF16)

        each_chunk(body)

    fine = Q if S == T else 1
    width = Dt // fine

    def cut(ref, q):
        return ref if fine == 1 else ref.at[:, pl.ds(pl.multiple_of(q * width, 128), width)]

    def pair_copy(layer, at, q):
        return pltpu.make_async_remote_copy(
            cut(PART.at[layer, 2 * at + 1 - core], q), cut(PRECV.at[layer, at], q),
            ps.at[layer, at, q], pr.at[layer, at, q], device_id={"tp": partner}, device_id_type=MESH,
        )

    def sum_copy(layer, at, q):
        return pltpu.make_async_remote_copy(
            cut(SUMB.at[layer, at], q), cut(RECV.at[layer, chip], q),
            rs.at[layer, at, q], rr.at[layer, chip, q],
            device_id={"tp": at * 2 + core}, device_id_type=MESH,
        )

    def sum_arrival(layer, at, q):
        return pltpu.make_async_remote_copy(
            cut(SUMB.at[layer, at], q), cut(RECV.at[layer, at], q),
            rs.at[layer, at, q], rr.at[layer, at, q],
            device_id={"tp": at * 2 + core}, device_id_type=MESH,
        )

    def columns_of(q):
        return pl.ds(pl.multiple_of(q * width, 128), width)

    def sum_pair(layer, at, q):
        pair_copy(layer, at, q).wait_recv()
        columns = columns_of(q)

        def body(where):
            SUMB[layer, at, where, columns] = (
                PART[layer, at * 2 + core, where, columns].astype(F32)
                + PRECV[layer, at, where, columns].astype(F32)
            ).astype(BF16)

        each_chunk(body)
        sum_copy(layer, at, q).start()

    def turn_order():
        count = Q // 2
        return [(False, g * count + piece, piece) for piece in range(count)] + [
            (True, (1 - g) * count + piece, piece) for piece in range(count)
        ]

    def branch(layer, k, select=None):
        def block(owner):
            target = lax.div(owner * Ds, Dt)
            base = lax.rem(owner * Ds, Dt)
            at = lax.div(target, 2)

            def product(q):
                columns = pl.ds(pl.multiple_of(base + q * Dq, 128), Dq)
                PART[layer, target, :, columns] = jnp.dot(
                    MIX[...], WO[layer, owner, q], preferred_element_type=F32
                ).astype(BF16)
                if S == T:

                    @pl.when(lax.rem(target, 2) != core)
                    def _():
                        pair_copy(layer, at, q).start()

            def total(q):
                if S == T:

                    @pl.when(both(lax.rem(target, 2) == core, at != chip))
                    def _():
                        sum_pair(layer, at, q)

            order = turn_order()
            early = order if k == 0 else [o for o in order if not o[0]]
            for _, q, _ in early:
                product(q)
            for _, q, _ in early:
                total(q)
            if k > 0:
                for _, q, piece in order[len(early) :]:
                    arrive([groups[layer][2][piece]], owner)
                    product(q)
                    total(q)

        at_distance(k, block, select)
        if S != T and k == S - 1:
            for shift in list(range(1, chips)) + [0]:
                pair_copy(layer, lax.rem(chip + shift, chips), 0).start()
            for shift in range(1, chips):
                sum_pair(layer, lax.rem(chip + shift, chips), 0)

    def finish(layer):
        source = h_ref if layer == 0 else HB
        target = out_ref if layer == L - 1 else HB
        for q in [q for _, q, _ in turn_order()] if fine > 1 else [0]:
            pair_copy(layer, chip, q).wait_recv()
            for shift in range(1, chips):
                sum_arrival(layer, lax.rem(chip + shift, chips), q).wait_recv()
            columns = columns_of(q)

            def body(where, columns=columns):
                total = PART[layer, t, where, columns].astype(F32) + PRECV[
                    layer, chip, where, columns
                ].astype(F32)
                for shift in range(1, chips):
                    total = total + RECV[layer, lax.rem(chip + shift, chips), where, columns].astype(F32)
                target[where, columns] = (source[where, columns].astype(F32) + total).astype(BF16)

            each_chunk(body)

    barrier = pltpu.get_barrier_semaphore()
    for shift in range(1, T):
        pl.semaphore_signal(barrier, inc=1, device_id={"tp": lax.rem(t + shift, T)}, device_id_type=MESH)
    pl.semaphore_signal(barrier, inc=1, device_id={"grp": 1 - g}, device_id_type=MESH)

    @pl.when(no(first))
    def _():
        pl.semaphore_signal(barrier, inc=1, device_id={"sp": me - 1}, device_id_type=MESH)

    @pl.when(no(last))
    def _():
        pl.semaphore_signal(barrier, inc=1, device_id={"sp": me + 1}, device_id_type=MESH)

    inner = jnp.where(first, 0, 1) + jnp.where(last, 0, 1)
    pl.semaphore_wait(barrier, T + inner)

    value0, gating0, out0 = groups[0]
    for which in range(2):
        own_wait(0, which)
        send_own(groups[0][which])
    own_wait(0, 2)
    send_out(out0)
    for layer in range(1, L):
        for which in range(3):
            own_wait(layer, which)
            send_out(groups[layer][which])
    make_x(0)

    def owned_inside(owner):
        return no(is_edge(owner))

    def inner_take(ids, k, select=None):
        @pl.when(no(edge))
        def _():
            take(ids, k, select)

    @pl.when(edge)
    def _():
        guest_x_copy().start()
        guest_stat_copy().start()
        send_direct(value0 + gating0)
        send_own(out0)
        send_direct(out0)
        for layer in range(1, L):
            send_own(groups[layer][0] + groups[layer][1])
            send_direct(groups[layer][0] + groups[layer][1])
            send_own(groups[layer][2])
            send_direct(groups[layer][2])
        take(out0, 1)
        for layer in range(1, L):
            for which in range(3):
                take(groups[layer][which], 1)
        take(out0, 2)

    @pl.when(no(edge))
    def _():
        send_x(0)
        send_stat(0)
        take(value0 + gating0, 1)
        send_own(out0)
        relay_x(0)
        wait_x(0)
        project(0, 0)
        for k in range(2, S - 1):
            take(value0, k)
            if k == 2:

                @pl.when(near)
                def _():
                    xcopy(L, t, partner, xf.at[L, 0]).wait_recv()
                    guest_stat_pass(t, partner).wait_recv()
                    send_x(L)
                    for shift in range(1, T):
                        guest_stat_pass(t, lax.rem(t + shift, T)).start()

            take(gating0, k)
            project(0, k - 1, lambda owner: no(skips_y(value0[0], owner)))
        take(out0, 1, owned_inside)

        @pl.when(near)
        def _():
            relay_x(L)
            wait_x(L)
            for shift in range(1, T):
                guest_stat_pass(lax.rem(t + shift, T), partner).wait_recv()

        project(0, S - 2)
        wait_stat(0)

        @pl.when(near)
        def _():
            corner = jnp.where(low, 0, S - 1)
            arrive(value0 + gating0, corner)
            multiply(ACC, X.at[0], 0, corner, False)
            multiply(GACC, XG, 0, me, True)

            def add(index, _):
                owner = lax.rem(me + index, S)
                multiply(GACC, XG, 0, owner, False)
                return 0

            lax.fori_loop(1, S, add, 0)

            def back(where):
                gate_rows(0, GACC, GSTAT, guest_base, where)
                guest_back(lax.div(where.start, CHUNK)).start()

            each_chunk(back)

        gate(0)
        take(out0, 1, is_edge)
        if L > 1:
            send_own(groups[1][0] + groups[1][1])
        take(out0, 2)

    for layer in range(L):
        value, gating, out = groups[layer]
        ahead = groups[layer + 1] if layer + 1 < L else None
        convolve(layer)
        mix(layer)
        branch(layer, 0)
        if ahead:
            inner_take(ahead[0], 1, owned_inside)
        branch(layer, 1)
        branch(layer, 2)
        for k in range(3, S):
            take(out, k)
            branch(layer, k)
        if ahead:
            inner_take(ahead[0], 1, is_edge)
            inner_take(ahead[1], 1, owned_inside)
        finish(layer)
        if ahead:
            after = layer + 1
            make_x(after)
            send_x(after)
            send_stat(2 * after)
            take(ahead[0], 2)
            inner_take(ahead[1], 1, is_edge)
            relay_x(after)
            take(ahead[1], 2)

            @pl.when(no(edge))
            def _(ahead=ahead):
                send_own(ahead[2])

            wait_x(after)
            project(after, 0)
            for k in range(3, S):
                take(ahead[0], k)
            inner_take(ahead[2], 1, owned_inside)
            project(after, 1)
            for k in range(3, S):
                take(ahead[1], k)
            for k in range(2, S):
                project(after, k)
            wait_stat(2 * after)
            gate(after)
            inner_take(ahead[2], 1, is_edge)
            if after + 1 < L:

                @pl.when(no(edge))
                def _(after=after):
                    send_own(groups[after + 1][0] + groups[after + 1][1])

            take(ahead[2], 2)

    for item in range(items):

        def drain(owner, _, item=item):
            mine = owner == me
            had = either(mine, inside(item, me))

            @pl.when(both(both(owner <= me, inside(item, me + 1)), had))
            def _():
                zcopy(item, owner, 1).wait_send()

            @pl.when(both(both(owner >= me, inside(item, me - 1)), had))
            def _():
                zcopy(item, owner, -1).wait_send()

            @pl.when(both(no(mine), both(inside(item, me), no(skips_y(item, owner)))))
            def _():
                ycopy(item, owner).wait_send()

            return 0

        lax.fori_loop(0, S, drain, 0)
        if direct(item):

            @pl.when(edge)
            def _(item=item):
                dcopy(item, me).wait_send()

    def drain_x(slot):
        for shift in range(chips):
            xcopy(slot, t, partner, xs.at[slot, shift]).wait_send()
        for shift in range(1, chips):
            xcopy(slot, t, partner, xf.at[slot, shift]).wait_send()

    def drain_stat(slot):
        for shift in range(1, T):
            stat_copy(slot, lax.rem(t + shift, T)).wait_send()

    @pl.when(edge)
    def _():
        guest_x_copy().wait_send()
        guest_stat_copy().wait_send()

    @pl.when(no(edge))
    def _():
        drain_x(0)
        drain_stat(0)

    @pl.when(near)
    def _():
        drain_x(L)
        for shift in range(1, T):
            guest_stat_pass(t, lax.rem(t + shift, T)).wait_send()
        for index in range(rows // CHUNK):
            guest_back(index).wait_send()

    for layer in range(L):
        if layer > 0:
            drain_x(layer)
            drain_stat(2 * layer)
        drain_stat(2 * layer + 1)
        for shift in range(chips):
            for q in range(fine):
                pair_copy(layer, lax.rem(chip + shift, chips), q).wait_send()
        for shift in range(1, chips):
            for q in range(fine):
                sum_copy(layer, lax.rem(chip + shift, chips), q).wait_send()

        @pl.when(sends_halo(layer))
        def _(layer=layer):
            halo_copy(layer).wait_send()


def shards(hidden_in, in_gain, w_value, w_gate, conv_taps, norm_gain, norm_shift, w_out):
    S, T = lax.axis_size("sp"), lax.axis_size("tp")
    L, Ds, Cn = w_value.shape
    rows, Dt = hidden_in.shape
    chips = T // 2
    halo = (conv_taps.shape[1] - 1 + 15) // 16 * 16
    items = L * sum(cuts(Ds))
    Q = 2 * cuts(Ds)[2]
    fine = Q if S == T else 1
    vmem = pl.BlockSpec(memory_space=pltpu.VMEM)
    hbm = pl.BlockSpec(memory_space=pl.ANY)
    dma = pltpu.SemaphoreType.DMA
    return pl.pallas_call(
        functools.partial(kernel, S, T),
        out_shape=jax.ShapeDtypeStruct((rows, Dt), BF16),
        in_specs=[vmem, vmem, hbm, hbm, vmem, vmem, vmem, hbm],
        out_specs=vmem,
        scratch_shapes=[
            pltpu.VMEM((L, S, Ds, Cn), BF16),
            pltpu.VMEM((L, S, Ds, Cn), BF16),
            pltpu.VMEM((L, S, Q, Cn, Ds // Q), BF16),
            pltpu.VMEM((L, T, rows, Dt), BF16),
            pltpu.VMEM((T, rows, Dt), BF16),
            pltpu.VMEM((2, rows, Cn), F32),
            pltpu.VMEM((2, rows, Cn), F32),
            pltpu.VMEM((L, halo + 2 * rows, Cn), BF16),
            pltpu.VMEM((rows, Cn), F32),
            pltpu.VMEM((rows, Cn), BF16),
            pltpu.VMEM((L, T, rows, Dt), BF16),
            pltpu.VMEM((L, chips, rows, Dt), BF16),
            pltpu.VMEM((L, chips, rows, Dt), BF16),
            pltpu.VMEM((L, chips, rows, Dt), BF16),
            pltpu.VMEM((2 * L, T, 8, rows), F32),
            pltpu.VMEM((T, 8, rows), F32),
            pltpu.VMEM((rows, Dt), BF16),
            dma((L, 2 + Q)),
            dma((items, S)), dma((items, S)), dma((items, S)), dma((items, S)), dma((items, S)),
            dma((items,)), dma((items,)),
            dma((L + 1, T)), dma((L + 1, chips)), dma((L + 1, chips)),
            dma((2 * L, T)), dma((2 * L, T)),
            dma((T,)), dma((T,)),
            dma((L,)), dma((L,)),
            dma((rows // CHUNK,)), dma((rows // CHUNK,)),
            dma((L, chips, fine)), dma((L, chips, fine)),
            dma((L, chips, fine)), dma((L, chips, fine)),
        ],
        compiler_params=pltpu.CompilerParams(
            collective_id=0, has_side_effects=True, vmem_limit_bytes=64_000_000
        ),
    )(hidden_in, in_gain, w_value, w_gate, conv_taps, norm_gain, norm_shift, w_out)


def solution(mesh):
    placed = (
        P(("grp", "sp"), "tp"),
        P(None, "tp"),
        P(None, "sp", "tp"),
        P(None, "sp", "tp"),
        P(None, None, "tp"),
        P(None, "tp"),
        P(None, "tp"),
        P(None, "tp", "sp"),
    )
    return jax.shard_map(
        shards, mesh=mesh, in_specs=placed, out_specs=P(("grp", "sp"), "tp"), check_vma=False
    )
```

```python
import functools

import jax
import jax.numpy as jnp
from jax import lax
from jax.experimental import pallas as pl
from jax.experimental.pallas import tpu as pltpu
from jax.sharding import PartitionSpec as P

epsilon = 1e-06
CHUNK = 128
F32, BF16 = jnp.float32, jnp.bfloat16


def cuts(Ds):
    return (2, 2, 2) if Ds >= 512 else (1, 1, 1)


def kernel(
    S, T, h_ref, gain_ref, wv_ref, wg_ref, taps_ref, ng_ref, ns_ref, wo_ref, out_ref,
    WV, WG, WO, X, XG, ACC, GACC, EXT, CONV, MIX, PART, PRECV, SUMB, RECV, STAT, GSTAT, HB,
    own_sem, zr, zs_right, zs_left, yr, ys, dr, ds, xr, xs, xf, sr, ss, gr, gs, hr, hs, br, bs,
    pr, ps, rr, rs,
):
    L = wv_ref.shape[0]
    Ds, Cn = wv_ref.shape[1], wv_ref.shape[2]
    rows, Dt = h_ref.shape
    taps = taps_ref.shape[1]
    features, channels = Dt * T, Cn * T
    chips = T // 2
    pieces_of = cuts(Ds)
    Q, Dq = WO.shape[2], WO.shape[4]
    halo = EXT.shape[1] - 2 * rows
    g, me, t = lax.axis_index("grp"), lax.axis_index("sp"), lax.axis_index("tp")
    core = lax.rem(t, 2)
    chip = lax.div(t, 2)
    partner = t + 1 - 2 * core
    MESH = pl.DeviceIdType.MESH
    both, either, no = jnp.logical_and, jnp.logical_or, jnp.logical_not
    first, last = me == 0, me == S - 1
    low, high = me == 1, me == S - 2
    edge, near = either(first, last), either(low, high)
    inward = jnp.where(first, 1, -1)
    outward = jnp.where(low, -1, 1)
    own_base = jnp.where(low, rows, 0)
    guest_base = jnp.where(low, 0, rows)

    def is_edge(plane):
        return either(plane == 0, plane == S - 1)

    table = []
    groups = []
    for layer in range(L):
        of_layer = []
        for which in range(3):
            ids = []
            for piece in range(pieces_of[which]):
                ids.append(len(table))
                table.append((layer, which, piece, pieces_of[which]))
            of_layer.append(ids)
        groups.append(of_layer)
    items = len(table)

    def direct(item):
        _, which, piece, _ = table[item]
        return which != 1 or piece == 0

    def folded(item):
        layer, which, _, _ = table[item]
        return layer == 0 and which < 2

    def inside(item, plane):
        low_end, high_end = (1, S - 2) if folded(item) else (0, S - 1)
        return both(plane >= low_end, plane <= high_end)

    def skips_y(item, owner):
        if not direct(item):
            return jnp.bool_(False)
        return either(both(owner == 0, low), both(owner == S - 1, high))

    sources = [(wv_ref, WV), (wg_ref, WG), (wo_ref, WO)]

    def own(layer, which):
        source, slots = sources[which]
        if which < 2:
            return [pltpu.make_async_copy(source.at[layer], slots.at[layer, me], own_sem.at[layer, which])]
        return [
            pltpu.make_async_copy(
                source.at[layer, :, pl.ds(q * Dq, Dq)], slots.at[layer, me, q], own_sem.at[layer, 2 + q]
            )
            for q in range(Q)
        ]

    def own_start(layer, which):
        for copy in own(layer, which):
            copy.start()

    own_start(0, 0)
    own_start(0, 1)

    def own_wait(layer, which):
        for copy in own(layer, which):
            copy.wait()

    def each_chunk(body, size=CHUNK):
        def step(index, _):
            body(pl.ds(pl.multiple_of(index * size, size), size))
            return 0

        lax.fori_loop(0, rows // size, step, 0)

    def put_stat(slot, where, left, right):
        lane = lax.broadcasted_iota(jnp.int32, (left.shape[0], 128), 1)
        wide = jnp.where(lane == 0, left, right)
        STAT[slot, t, :, where] = wide.T[:8]

    def stat_copy(slot, peer):
        return pltpu.make_async_remote_copy(
            STAT.at[slot, t], STAT.at[slot, t], ss.at[slot, peer], sr.at[slot, t],
            device_id={"tp": peer}, device_id_type=MESH,
        )

    def stat_arrival(slot, peer):
        return pltpu.make_async_remote_copy(
            STAT.at[slot, peer], STAT.at[slot, peer], ss.at[slot, peer], sr.at[slot, peer],
            device_id={"tp": peer}, device_id_type=MESH,
        )

    def send_stat(slot):
        for shift in range(1, T):
            stat_copy(slot, lax.rem(t + shift, T)).start()

    def wait_stat(slot):
        for shift in range(1, T):
            stat_arrival(slot, lax.rem(t + shift, T)).wait_recv()

    def total_stat(stat, where):
        total = stat[0, :, where]
        for peer in range(1, T):
            total = total + stat[peer, :, where]
        return jnp.concatenate([total] * 16, axis=0).T

    def part_ref(item, owner, half):
        layer, which, piece, pieces = table[item]
        slots = sources[which][1]
        if which == 2:
            return slots.at[layer, owner, half * pieces + piece]
        size = slots.shape[2] // (2 * pieces)
        start = pl.multiple_of(half * (size * pieces) + piece * size, size)
        return slots.at[layer, owner, pl.ds(start, size)]

    def zcopy(item, owner, way):
        ref = part_ref(item, owner, g)
        sems = zs_right if way > 0 else zs_left
        return pltpu.make_async_remote_copy(
            ref, ref, sems.at[item, owner], zr.at[item, owner],
            device_id={"sp": me + way}, device_id_type=MESH,
        )

    def dcopy(item, owner):
        ref = part_ref(item, owner, 1 - g)
        return pltpu.make_async_remote_copy(
            ref, ref, ds.at[item], dr.at[item], device_id={"sp": me + inward}, device_id_type=MESH,
        )

    def ycopy(item, owner):
        ref = part_ref(item, owner, g)
        return pltpu.make_async_remote_copy(
            ref, ref, ys.at[item, owner], yr.at[item, owner],
            device_id={"grp": 1 - g}, device_id_type=MESH,
        )

    def yarrival(item, owner):
        ref = part_ref(item, owner, 1 - g)
        return pltpu.make_async_remote_copy(
            ref, ref, ys.at[item, owner], yr.at[item, owner],
            device_id={"grp": 1 - g}, device_id_type=MESH,
        )

    def outgoing(way):
        return low if way < 0 else high

    def send_out(ids):
        for item in ids:
            for way in (1, -1):

                @pl.when(outgoing(way))
                def _(item=item, way=way):
                    zcopy(item, me, way).start()

    def send_own(ids):
        for item in ids:
            for way in (1, -1):
                allowed = inside(item, me + way)
                if not folded(item):
                    allowed = both(allowed, no(outgoing(way)))

                @pl.when(allowed)
                def _(item=item, way=way):
                    zcopy(item, me, way).start()

    def send_direct(ids):
        for item in ids:
            if direct(item):
                dcopy(item, me).start()

    def take(ids, k, select=None):
        for item in ids:
            for way in (1, -1):
                owner = me - way * k
                ok = both(both(owner >= 0, owner < S), inside(item, me))
                if select is not None:
                    ok = both(ok, select(owner))

                @pl.when(ok)
                def _(item=item, way=way, owner=owner):
                    zcopy(item, owner, way).wait_recv()

                    @pl.when(inside(item, me + way))
                    def _():
                        zcopy(item, owner, way).start()

                    @pl.when(no(skips_y(item, owner)))
                    def _():
                        ycopy(item, owner).start()

    def arrive(ids, owner):
        for item in ids:
            skip = skips_y(item, owner)

            @pl.when(no(skip))
            def _(item=item):
                yarrival(item, owner).wait_recv()

            @pl.when(skip)
            def _(item=item):
                dcopy(item, owner).wait_recv()

    def x_ref(slot, source):
        return XG.at[source] if slot == L else X.at[slot, source]

    def xcopy(slot, source, peer, sem):
        return pltpu.make_async_remote_copy(
            x_ref(slot, source), x_ref(slot, source), sem, xr.at[slot, source],
            device_id={"tp": peer}, device_id_type=MESH,
        )

    def make_x(layer):
        source = h_ref if layer == 0 else HB

        def body(where):
            wide = source[where, :].astype(F32)
            X[layer, t, where, :] = (wide * gain_ref[layer : layer + 1, :]).astype(BF16)
            squares = jnp.sum(wide * wide, axis=1, keepdims=True)
            put_stat(2 * layer, where, squares, squares)

        each_chunk(body)

    def send_x(slot):
        for shift in range(1, chips):
            peer = lax.rem(chip + shift, chips) * 2 + core
            xcopy(slot, t, peer, xs.at[slot, shift]).start()
        xcopy(slot, t, partner, xs.at[slot, 0]).start()

    def relay_x(slot):
        for shift in range(1, chips):
            source = lax.rem(chip + shift, chips) * 2 + core
            xcopy(slot, source, partner, xf.at[slot, shift]).wait_recv()
            xcopy(slot, source, partner, xf.at[slot, shift]).start()

    def wait_x(slot):
        for shift in range(chips):
            source = lax.rem(chip + shift, chips) * 2 + 1 - core
            xcopy(slot, source, partner, xf.at[slot, 0]).wait_recv()

    def guest_x_copy():
        return pltpu.make_async_remote_copy(
            X.at[0, t], XG.at[t], xs.at[L, 0], xr.at[L, t],
            device_id={"sp": me + inward}, device_id_type=MESH,
        )

    def guest_stat_copy():
        return pltpu.make_async_remote_copy(
            STAT.at[0, t], GSTAT.at[t], gs.at[t], gr.at[t],
            device_id={"sp": me + inward}, device_id_type=MESH,
        )

    def guest_stat_pass(source, peer):
        return pltpu.make_async_remote_copy(
            GSTAT.at[source], GSTAT.at[source], gs.at[peer], gr.at[source],
            device_id={"tp": peer}, device_id_type=MESH,
        )

    def guest_back(index):
        start = pl.multiple_of(index * CHUNK + halo, 16)
        return pltpu.make_async_remote_copy(
            EXT.at[0, pl.ds(pl.multiple_of(guest_base + start, 16), CHUNK)],
            EXT.at[0, pl.ds(start, CHUNK)],
            bs.at[index], br.at[index],
            device_id={"sp": me + outward}, device_id_type=MESH,
        )

    def at_distance(k, body, select=None):
        if k == 0:
            body(me)
            return

        def step(index, _):
            owner = me + k - 2 * k * index
            ok = both(owner >= 0, owner < S)
            if select is not None:
                ok = both(ok, select(owner))

            @pl.when(ok)
            def _():
                body(owner)

            return 0

        lax.fori_loop(0, 2, step, 0)

    def multiply(total, x, layer, owner, start):
        at = lax.div(owner * Ds, Dt)
        columns = pl.ds(pl.multiple_of(lax.rem(owner * Ds, Dt), 128), Ds)
        xs_block = x[at, :, columns]
        for which, slots in ((0, WV), (1, WG)):
            part = jnp.dot(xs_block, slots[layer, owner], preferred_element_type=F32)
            if start:
                total[which] = part
            else:
                total[which] += part

    def project(layer, k, select=None):
        def block(owner):
            if k > 0:
                arrive(groups[layer][0] + groups[layer][1], owner)
            multiply(ACC, X.at[layer], layer, owner, k == 0)

        at_distance(k, block, select)

    def halo_copy(layer):
        end = halo + rows + (own_base if layer == 0 else 0)
        return pltpu.make_async_remote_copy(
            EXT.at[layer, pl.ds(pl.multiple_of(end - halo, 16), halo)],
            EXT.at[layer, pl.ds(0, halo)],
            hs.at[layer], hr.at[layer],
            device_id={"sp": me + 1}, device_id_type=MESH,
        )

    def sends_halo(layer):
        return both(no(last), no(first)) if layer == 0 else no(last)

    def takes_halo(layer):
        return both(no(first), no(low)) if layer == 0 else no(first)

    def gate_rows(layer, total, stat, base, where):
        mean = total_stat(stat, where)[:, :1] / features
        inv = lax.rsqrt(mean + epsilon)
        value, gating = total[0, where, :] * inv, total[1, where, :] * inv
        gated = (value / (1.0 + jnp.exp(-gating))).astype(BF16)
        EXT[layer, pl.ds(pl.multiple_of(base + where.start + halo, 16), where.size), :] = gated

    def gate(layer):
        base = own_base if layer == 0 else 0
        each_chunk(functools.partial(gate_rows, layer, ACC, STAT.at[2 * layer], base))

        @pl.when(sends_halo(layer))
        def _():
            halo_copy(layer).start()

    def convolve(layer):
        @pl.when(first)
        def _():
            EXT[layer, pl.ds(0, halo), :] = jnp.zeros((halo, Cn), BF16)

        @pl.when(takes_halo(layer))
        def _():
            halo_copy(layer).wait_recv()

        tall = CHUNK + halo + 8
        offset = halo - (taps - 1)
        base = own_base if layer == 0 else 0

        def body(where):
            if layer == 0:

                @pl.when(edge)
                def _():
                    guest_back(lax.div(where.start, CHUNK)).wait_recv()

            for column in range(0, Cn, 128):
                at = pl.ds(column, 128)
                window = EXT[layer, pl.ds(pl.multiple_of(base + where.start, 16), CHUNK + halo), at]
                tile = jnp.concatenate([window.astype(F32), jnp.zeros((8, 128), F32)], axis=0)
                total = jnp.zeros((CHUNK, 128), F32)
                for residue in range(8):
                    ks = [k for k in range(taps) if (k + offset) % 8 == residue]
                    if not ks:
                        continue
                    turned = pltpu.roll(tile, tall - residue, 0) if residue else tile
                    for k in ks:
                        low_row = k + offset - residue
                        total = total + taps_ref[layer, k : k + 1, at] * turned[low_row : low_row + CHUNK]
                CONV[where, at] = total
            conved = CONV[where, :]
            put_stat(
                2 * layer + 1, where,
                jnp.sum(conved, axis=1, keepdims=True),
                jnp.sum(conved * conved, axis=1, keepdims=True),
            )

        each_chunk(body)
        send_stat(2 * layer + 1)

    def mix(layer):
        wait_stat(2 * layer + 1)

        def body(where):
            stat = total_stat(STAT.at[2 * layer + 1], where)
            mean = stat[:, 0:1] / channels
            spread = stat[:, 1:2] / channels - mean * mean
            normed = (CONV[where, :] - mean) * lax.rsqrt(spread + epsilon) * ng_ref[
                layer : layer + 1, :
            ] + ns_ref[layer : layer + 1, :]
            MIX[where, :] = (normed / (1.0 + jnp.exp(-normed))).astype(BF16)

        each_chunk(body)

    fine = Q if S == T else 1
    width = Dt // fine

    def cut(ref, q):
        return ref if fine == 1 else ref.at[:, pl.ds(pl.multiple_of(q * width, 128), width)]

    def pair_copy(layer, at, q):
        return pltpu.make_async_remote_copy(
            cut(PART.at[layer, 2 * at + 1 - core], q), cut(PRECV.at[layer, at], q),
            ps.at[layer, at, q], pr.at[layer, at, q], device_id={"tp": partner}, device_id_type=MESH,
        )

    def sum_copy(layer, at, q):
        return pltpu.make_async_remote_copy(
            cut(SUMB.at[layer, at], q), cut(RECV.at[layer, chip], q),
            rs.at[layer, at, q], rr.at[layer, chip, q],
            device_id={"tp": at * 2 + core}, device_id_type=MESH,
        )

    def sum_arrival(layer, at, q):
        return pltpu.make_async_remote_copy(
            cut(SUMB.at[layer, at], q), cut(RECV.at[layer, at], q),
            rs.at[layer, at, q], rr.at[layer, at, q],
            device_id={"tp": at * 2 + core}, device_id_type=MESH,
        )

    def columns_of(q):
        return pl.ds(pl.multiple_of(q * width, 128), width)

    def sum_pair(layer, at, q):
        pair_copy(layer, at, q).wait_recv()
        columns = columns_of(q)

        def body(where):
            SUMB[layer, at, where, columns] = (
                PART[layer, at * 2 + core, where, columns].astype(F32)
                + PRECV[layer, at, where, columns].astype(F32)
            ).astype(BF16)

        each_chunk(body)
        sum_copy(layer, at, q).start()

    def turn_order():
        count = Q // 2
        return [(False, g * count + piece, piece) for piece in range(count)] + [
            (True, (1 - g) * count + piece, piece) for piece in range(count)
        ]

    def branch(layer, k, select=None):
        def block(owner):
            target = lax.div(owner * Ds, Dt)
            base = lax.rem(owner * Ds, Dt)
            at = lax.div(target, 2)

            def product(q):
                columns = pl.ds(pl.multiple_of(base + q * Dq, 128), Dq)
                PART[layer, target, :, columns] = jnp.dot(
                    MIX[...], WO[layer, owner, q], preferred_element_type=F32
                ).astype(BF16)
                if S == T:

                    @pl.when(lax.rem(target, 2) != core)
                    def _():
                        pair_copy(layer, at, q).start()

            def total(q):
                if S == T:

                    @pl.when(both(lax.rem(target, 2) == core, at != chip))
                    def _():
                        sum_pair(layer, at, q)

            order = turn_order()
            early = order if k == 0 else [o for o in order if not o[0]]
            for _, q, _ in early:
                product(q)
            for _, q, _ in early:
                total(q)
            if k > 0:
                for _, q, piece in order[len(early) :]:
                    arrive([groups[layer][2][piece]], owner)
                    product(q)
                    total(q)

        at_distance(k, block, select)
        if S != T and k == S - 1:
            for shift in list(range(1, chips)) + [0]:
                pair_copy(layer, lax.rem(chip + shift, chips), 0).start()
            for shift in range(1, chips):
                sum_pair(layer, lax.rem(chip + shift, chips), 0)

    def finish(layer):
        source = h_ref if layer == 0 else HB
        target = out_ref if layer == L - 1 else HB
        for q in [q for _, q, _ in turn_order()] if fine > 1 else [0]:
            pair_copy(layer, chip, q).wait_recv()
            for shift in range(1, chips):
                sum_arrival(layer, lax.rem(chip + shift, chips), q).wait_recv()
            columns = columns_of(q)

            def body(where, columns=columns):
                total = PART[layer, t, where, columns].astype(F32) + PRECV[
                    layer, chip, where, columns
                ].astype(F32)
                for shift in range(1, chips):
                    total = total + RECV[layer, lax.rem(chip + shift, chips), where, columns].astype(F32)
                target[where, columns] = (source[where, columns].astype(F32) + total).astype(BF16)

            each_chunk(body)

    barrier = pltpu.get_barrier_semaphore()
    for shift in range(1, T):
        pl.semaphore_signal(barrier, inc=1, device_id={"tp": lax.rem(t + shift, T)}, device_id_type=MESH)
    pl.semaphore_signal(barrier, inc=1, device_id={"grp": 1 - g}, device_id_type=MESH)

    @pl.when(no(first))
    def _():
        pl.semaphore_signal(barrier, inc=1, device_id={"sp": me - 1}, device_id_type=MESH)

    @pl.when(no(last))
    def _():
        pl.semaphore_signal(barrier, inc=1, device_id={"sp": me + 1}, device_id_type=MESH)

    inner = jnp.where(first, 0, 1) + jnp.where(last, 0, 1)
    pl.semaphore_wait(barrier, T + inner)

    value0, gating0, out0 = groups[0]
    for which in range(2):
        own_wait(0, which)
        send_own(groups[0][which])
    rest = [(0, 2)] + [(layer, which) for layer in range(1, L) for which in range(3)]
    for layer, which in rest:
        own_start(layer, which)
    for layer, which in rest:
        own_wait(layer, which)
        send_out(groups[layer][which])
    make_x(0)

    def owned_inside(owner):
        return no(is_edge(owner))

    def inner_take(ids, k, select=None):
        @pl.when(no(edge))
        def _():
            take(ids, k, select)

    def edge_take(ids, k):
        @pl.when(edge)
        def _():
            take(ids, k)

    def far_take(ids):
        for k in range(3, S):
            take(ids, k)

    @pl.when(edge)
    def _():
        guest_x_copy().start()
        guest_stat_copy().start()
        send_direct(value0 + gating0)
        send_own(out0)
        send_direct(out0)
        for layer in range(1, L):
            send_own(groups[layer][0] + groups[layer][1])
            send_direct(groups[layer][0] + groups[layer][1])
            send_own(groups[layer][2])
            send_direct(groups[layer][2])
        take(out0, 1)
        for layer in range(1, L):
            for which in range(3):
                take(groups[layer][which], 1)
        take(out0, 2)
        if L > 1:
            take(groups[1][0][:1], 2)

    @pl.when(no(edge))
    def _():
        send_x(0)
        send_stat(0)
        take(value0 + gating0, 1)
        send_own(out0)
        relay_x(0)
        wait_x(0)
        project(0, 0)
        for k in range(2, S - 1):
            take(value0, k)
            if k == 2:

                @pl.when(near)
                def _():
                    xcopy(L, t, partner, xf.at[L, 0]).wait_recv()
                    guest_stat_pass(t, partner).wait_recv()
                    send_x(L)
                    for shift in range(1, T):
                        guest_stat_pass(t, lax.rem(t + shift, T)).start()

            take(gating0, k)
            if k == 2 and L > 1:
                send_own(groups[1][0])
            project(0, k - 1, lambda owner: no(skips_y(value0[0], owner)))
        take(out0, 1, owned_inside)

        @pl.when(near)
        def _():
            relay_x(L)
            wait_x(L)
            for shift in range(1, T):
                guest_stat_pass(lax.rem(t + shift, T), partner).wait_recv()

        if L > 1:
            take(groups[1][0][:1], 1, owned_inside)
        project(0, S - 2)
        wait_stat(0)

        @pl.when(near)
        def _():
            corner = jnp.where(low, 0, S - 1)
            arrive(value0 + gating0, corner)
            multiply(ACC, X.at[0], 0, corner, False)
            multiply(GACC, XG, 0, me, True)

            def add(index, _):
                owner = lax.rem(me + index, S)
                multiply(GACC, XG, 0, owner, False)
                return 0

            lax.fori_loop(1, S, add, 0)

            def back(where):
                gate_rows(0, GACC, GSTAT, guest_base, where)
                guest_back(lax.div(where.start, CHUNK)).start()

            each_chunk(back)

        gate(0)
        take(out0, 1, is_edge)
        if L > 1:
            send_own(groups[1][1])
            take(groups[1][0][1:], 1, owned_inside)

    for layer in range(L):
        out = groups[layer][2]
        ahead = groups[layer + 1] if layer + 1 < L else None
        if ahead and layer > 0:
            inner_take(ahead[0], 1, owned_inside)
            edge_take(ahead[0][:1], 2)
        convolve(layer)
        inner_take(out[1:] if layer > 0 else out[:1], 2)
        if layer > 0:
            far_take(out[:1])
        mix(layer)
        if layer == 0:
            inner_take(out[1:], 2)
        if ahead:
            edge_take(ahead[0][1:], 2)
        branch(layer, 0)
        branch(layer, 1)
        if ahead:
            inner_take(ahead[1][:1], 1, owned_inside)
        branch(layer, 2)
        far_take(out[1:] if layer > 0 else out)
        if ahead:
            inner_take(ahead[0], 1, is_edge)
            inner_take(ahead[1][1:], 1, owned_inside)
            edge_take(ahead[1][:1], 2)
        for k in range(3, S):
            branch(layer, k)
        finish(layer)
        if ahead:
            after = layer + 1
            make_x(after)
            send_x(after)
            send_stat(2 * after)
            inner_take(ahead[0], 2)
            inner_take(ahead[1], 1, is_edge)

            @pl.when(no(edge))
            def _(ahead=ahead):
                send_own(ahead[2])

            edge_take(ahead[1][1:], 2)
            far_take(ahead[0])
            inner_take(ahead[1], 2)
            relay_x(after)
            far_take(ahead[1][:1])
            wait_x(after)
            project(after, 0)
            project(after, 1)
            inner_take(ahead[2][:1], 1, owned_inside)
            far_take(ahead[1][1:])
            project(after, 2)
            inner_take(ahead[2][1:], 1, owned_inside)
            edge_take(ahead[2][:1], 2)
            for k in range(3, S):
                project(after, k)
            wait_stat(2 * after)
            gate(after)
            inner_take(ahead[2], 1, is_edge)
            edge_take(ahead[2][1:], 2)
            if after + 1 < L:

                @pl.when(no(edge))
                def _(after=after):
                    send_own(groups[after + 1][0] + groups[after + 1][1])

            inner_take(ahead[2][:1], 2)

    for item in range(items):

        def drain(owner, _, item=item):
            mine = owner == me
            had = either(mine, inside(item, me))

            @pl.when(both(both(owner <= me, inside(item, me + 1)), had))
            def _():
                zcopy(item, owner, 1).wait_send()

            @pl.when(both(both(owner >= me, inside(item, me - 1)), had))
            def _():
                zcopy(item, owner, -1).wait_send()

            @pl.when(both(no(mine), both(inside(item, me), no(skips_y(item, owner)))))
            def _():
                ycopy(item, owner).wait_send()

            return 0

        lax.fori_loop(0, S, drain, 0)
        if direct(item):

            @pl.when(edge)
            def _(item=item):
                dcopy(item, me).wait_send()

    def drain_x(slot):
        for shift in range(chips):
            xcopy(slot, t, partner, xs.at[slot, shift]).wait_send()
        for shift in range(1, chips):
            xcopy(slot, t, partner, xf.at[slot, shift]).wait_send()

    def drain_stat(slot):
        for shift in range(1, T):
            stat_copy(slot, lax.rem(t + shift, T)).wait_send()

    @pl.when(edge)
    def _():
        guest_x_copy().wait_send()
        guest_stat_copy().wait_send()

    @pl.when(no(edge))
    def _():
        drain_x(0)
        drain_stat(0)

    @pl.when(near)
    def _():
        drain_x(L)
        for shift in range(1, T):
            guest_stat_pass(t, lax.rem(t + shift, T)).wait_send()
        for index in range(rows // CHUNK):
            guest_back(index).wait_send()

    for layer in range(L):
        if layer > 0:
            drain_x(layer)
            drain_stat(2 * layer)
        drain_stat(2 * layer + 1)
        for shift in range(chips):
            for q in range(fine):
                pair_copy(layer, lax.rem(chip + shift, chips), q).wait_send()
        for shift in range(1, chips):
            for q in range(fine):
                sum_copy(layer, lax.rem(chip + shift, chips), q).wait_send()

        @pl.when(sends_halo(layer))
        def _(layer=layer):
            halo_copy(layer).wait_send()


def shards(hidden_in, in_gain, w_value, w_gate, conv_taps, norm_gain, norm_shift, w_out):
    S, T = lax.axis_size("sp"), lax.axis_size("tp")
    L, Ds, Cn = w_value.shape
    rows, Dt = hidden_in.shape
    chips = T // 2
    halo = (conv_taps.shape[1] - 1 + 15) // 16 * 16
    items = L * sum(cuts(Ds))
    Q = 2 * cuts(Ds)[2]
    fine = Q if S == T else 1
    vmem = pl.BlockSpec(memory_space=pltpu.VMEM)
    hbm = pl.BlockSpec(memory_space=pl.ANY)
    dma = pltpu.SemaphoreType.DMA
    return pl.pallas_call(
        functools.partial(kernel, S, T),
        out_shape=jax.ShapeDtypeStruct((rows, Dt), BF16),
        in_specs=[vmem, vmem, hbm, hbm, vmem, vmem, vmem, hbm],
        out_specs=vmem,
        scratch_shapes=[
            pltpu.VMEM((L, S, Ds, Cn), BF16),
            pltpu.VMEM((L, S, Ds, Cn), BF16),
            pltpu.VMEM((L, S, Q, Cn, Ds // Q), BF16),
            pltpu.VMEM((L, T, rows, Dt), BF16),
            pltpu.VMEM((T, rows, Dt), BF16),
            pltpu.VMEM((2, rows, Cn), F32),
            pltpu.VMEM((2, rows, Cn), F32),
            pltpu.VMEM((L, halo + 2 * rows, Cn), BF16),
            pltpu.VMEM((rows, Cn), F32),
            pltpu.VMEM((rows, Cn), BF16),
            pltpu.VMEM((L, T, rows, Dt), BF16),
            pltpu.VMEM((L, chips, rows, Dt), BF16),
            pltpu.VMEM((L, chips, rows, Dt), BF16),
            pltpu.VMEM((L, chips, rows, Dt), BF16),
            pltpu.VMEM((2 * L, T, 8, rows), F32),
            pltpu.VMEM((T, 8, rows), F32),
            pltpu.VMEM((rows, Dt), BF16),
            dma((L, 2 + Q)),
            dma((items, S)), dma((items, S)), dma((items, S)), dma((items, S)), dma((items, S)),
            dma((items,)), dma((items,)),
            dma((L + 1, T)), dma((L + 1, chips)), dma((L + 1, chips)),
            dma((2 * L, T)), dma((2 * L, T)),
            dma((T,)), dma((T,)),
            dma((L,)), dma((L,)),
            dma((rows // CHUNK,)), dma((rows // CHUNK,)),
            dma((L, chips, fine)), dma((L, chips, fine)),
            dma((L, chips, fine)), dma((L, chips, fine)),
        ],
        compiler_params=pltpu.CompilerParams(
            collective_id=0, has_side_effects=True, vmem_limit_bytes=64_000_000
        ),
    )(hidden_in, in_gain, w_value, w_gate, conv_taps, norm_gain, norm_shift, w_out)


def solution(mesh):
    placed = (
        P(("grp", "sp"), "tp"),
        P(None, "tp"),
        P(None, "sp", "tp"),
        P(None, "sp", "tp"),
        P(None, None, "tp"),
        P(None, "tp"),
        P(None, "tp"),
        P(None, "tp", "sp"),
    )
    return jax.shard_map(
        shards, mesh=mesh, in_specs=placed, out_specs=P(("grp", "sp"), "tp"), check_vma=False
    )
```

```python
import functools

import jax
import jax.numpy as jnp
from jax import lax
from jax.experimental import pallas as pl
from jax.experimental.pallas import tpu as pltpu
from jax.sharding import PartitionSpec as P

epsilon = 1e-06
CHUNK = 128
F32, BF16 = jnp.float32, jnp.bfloat16


def cuts(Ds):
    return (2, 2, 2) if Ds >= 512 else (1, 1, 1)


def kernel(
    S, T, h_ref, gain_ref, wv_ref, wg_ref, taps_ref, ng_ref, ns_ref, wo_ref, out_ref,
    WV, WG, WO, X, XG, ACC, GACC, EXT, CONV, MIX, PART, PRECV, SUMB, RECV, STAT, GSTAT, HB,
    own_sem, zr, zs, zo, yr, ys, xr, xs, xf, sr, ss, gr, gs, hr, hs, br, bs,
    pr, ps, rr, rs,
):
    L = wv_ref.shape[0]
    Ds, Cn = wv_ref.shape[1], wv_ref.shape[2]
    rows, Dt = h_ref.shape
    taps = taps_ref.shape[0]
    features, channels = Dt * T, Cn * T
    chips = T // 2
    pieces_of = cuts(Ds)
    Q, Dq = WO.shape[2], WO.shape[4]
    halo = EXT.shape[1] - 2 * rows
    g, me, t = lax.axis_index("grp"), lax.axis_index("sp"), lax.axis_index("tp")
    core = lax.rem(t, 2)
    chip = lax.div(t, 2)
    partner = t + 1 - 2 * core
    MESH = pl.DeviceIdType.MESH
    both, either, no = jnp.logical_and, jnp.logical_or, jnp.logical_not
    first, last = me == 0, me == S - 1
    low, high = me == 1, me == S - 2
    edge, near = either(first, last), either(low, high)
    inward = jnp.where(first, 1, -1)
    outward = jnp.where(low, -1, 1)
    own_base = jnp.where(low, rows, 0)
    guest_base = jnp.where(low, 0, rows)

    def is_edge(plane):
        return either(plane == 0, plane == S - 1)

    table = []
    groups = []
    for layer in range(L):
        of_layer = []
        for which in range(3):
            ids = []
            for piece in range(pieces_of[which]):
                ids.append(len(table))
                table.append((layer, which, piece, pieces_of[which]))
            of_layer.append(ids)
        groups.append(of_layer)
    items = len(table)

    def direct(item):
        _, which, piece, _ = table[item]
        return which != 1 or piece == 0

    def folded(item):
        layer, which, _, _ = table[item]
        return layer == 0 and which < 2

    def inside(item, plane):
        low_end, high_end = (1, S - 2) if folded(item) else (0, S - 1)
        return both(plane >= low_end, plane <= high_end)

    def skips_y(item, owner):
        if not direct(item):
            return jnp.bool_(False)
        return either(both(owner == 0, low), both(owner == S - 1, high))

    sources = [(wv_ref, WV), (wg_ref, WG), (wo_ref, WO)]

    def own(layer, which):
        source, slots = sources[which]
        if which < 2:
            return [pltpu.make_async_copy(source.at[layer], slots.at[layer, me], own_sem.at[layer, which])]
        return [
            pltpu.make_async_copy(
                source.at[layer, :, pl.ds(q * Dq, Dq)], slots.at[layer, me, q], own_sem.at[layer, 2]
            )
            for q in range(Q)
        ]

    def own_start(layer, which):
        for copy in own(layer, which):
            copy.start()

    own_start(0, 0)
    own_start(0, 1)

    def own_wait(layer, which):
        slot = sources[which][1].at[layer, me]
        pltpu.make_async_copy(slot, slot, own_sem.at[layer, which]).wait()

    def each_chunk(body, size=CHUNK):
        def step(index, _):
            body(pl.ds(pl.multiple_of(index * size, size), size))
            return 0

        lax.fori_loop(0, rows // size, step, 0)

    def put_stat(slot, where, left, right):
        lane = lax.broadcasted_iota(jnp.int32, (left.shape[0], 128), 1)
        wide = jnp.where(lane == 0, left, right)
        STAT[slot, t, :, where] = wide.T[:8]

    def stat_copy(slot, peer):
        return pltpu.make_async_remote_copy(
            STAT.at[slot, t], STAT.at[slot, t], ss.at[slot], sr.at[slot, t],
            device_id={"tp": peer}, device_id_type=MESH,
        )

    def stat_arrival(slot, peer):
        return pltpu.make_async_remote_copy(
            STAT.at[slot, peer], STAT.at[slot, peer], ss.at[slot], sr.at[slot, peer],
            device_id={"tp": peer}, device_id_type=MESH,
        )

    def send_stat(slot):
        for shift in range(1, T):
            stat_copy(slot, lax.rem(t + shift, T)).start()

    def wait_stat(slot):
        for shift in range(1, T):
            stat_arrival(slot, lax.rem(t + shift, T)).wait_recv()

    def total_stat(stat, where):
        total = stat[0, :, where]
        for peer in range(1, T):
            total = total + stat[peer, :, where]
        return jnp.concatenate([total] * 16, axis=0).T

    def part_ref(item, owner, half):
        layer, which, piece, pieces = table[item]
        slots = sources[which][1]
        if which == 2:
            return slots.at[layer, owner, half * pieces + piece]
        size = slots.shape[2] // (2 * pieces)
        start = pl.multiple_of(half * (size * pieces) + piece * size, size)
        return slots.at[layer, owner, pl.ds(start, size)]

    def zcopy(item, owner, way):
        ref = part_ref(item, owner, g)
        layer, which, _, _ = table[item]
        return pltpu.make_async_remote_copy(
            ref, ref, zs.at[layer, which, owner], zr.at[item, owner],
            device_id={"sp": me + way}, device_id_type=MESH,
        )

    def zown(item, way):
        ref = part_ref(item, me, g)
        layer, which, _, _ = table[item]
        return pltpu.make_async_remote_copy(
            ref, ref, zo.at[layer, which, (way + 1) // 2], zr.at[item, me],
            device_id={"sp": me + way}, device_id_type=MESH,
        )

    def dcopy(item, owner):
        ref = part_ref(item, owner, 1 - g)
        layer, which, _, _ = table[item]
        return pltpu.make_async_remote_copy(
            ref, ref, ys.at[layer, which, owner], yr.at[item, owner],
            device_id={"sp": me + inward}, device_id_type=MESH,
        )

    def ycopy(item, owner):
        ref = part_ref(item, owner, g)
        return pltpu.make_async_remote_copy(
            ref, ref, ys.at[table[item][0], table[item][1], owner], yr.at[item, owner],
            device_id={"grp": 1 - g}, device_id_type=MESH,
        )

    def yarrival(item, owner):
        ref = part_ref(item, owner, 1 - g)
        return pltpu.make_async_remote_copy(
            ref, ref, ys.at[table[item][0], table[item][1], owner], yr.at[item, owner],
            device_id={"grp": 1 - g}, device_id_type=MESH,
        )

    def outgoing(way):
        return low if way < 0 else high

    def send_out(ids):
        for item in ids:
            for way in (1, -1):

                @pl.when(outgoing(way))
                def _(item=item, way=way):
                    zown(item, way).start()

    def send_own(ids):
        for item in ids:
            for way in (1, -1):
                allowed = inside(item, me + way)
                if not folded(item):
                    allowed = both(allowed, no(outgoing(way)))

                @pl.when(allowed)
                def _(item=item, way=way):
                    zown(item, way).start()

    def send_direct(ids):
        for item in ids:
            if direct(item):
                dcopy(item, me).start()

    def take(ids, k, select=None):
        for item in ids:
            for way in (1, -1):
                owner = me - way * k
                ok = both(both(owner >= 0, owner < S), inside(item, me))
                if select is not None:
                    ok = both(ok, select(owner))

                @pl.when(ok)
                def _(item=item, way=way, owner=owner):
                    zcopy(item, owner, way).wait_recv()

                    @pl.when(inside(item, me + way))
                    def _():
                        zcopy(item, owner, way).start()

                    @pl.when(no(skips_y(item, owner)))
                    def _():
                        ycopy(item, owner).start()

    def arrive(ids, owner):
        for item in ids:
            yarrival(item, owner).wait_recv()

    def x_ref(slot, source):
        return XG.at[source] if slot == L else X.at[slot, source]

    def xcopy(slot, source, peer, sem):
        return pltpu.make_async_remote_copy(
            x_ref(slot, source), x_ref(slot, source), sem, xr.at[slot, source],
            device_id={"tp": peer}, device_id_type=MESH,
        )

    def make_x(layer):
        source = h_ref if layer == 0 else HB

        def body(where):
            wide = source[where, :].astype(F32)
            X[layer, t, where, :] = (wide * gain_ref[layer : layer + 1, :]).astype(BF16)
            squares = jnp.sum(wide * wide, axis=1, keepdims=True)
            put_stat(2 * layer, where, squares, squares)

        each_chunk(body)

    def send_x(slot):
        for shift in range(1, chips):
            peer = lax.rem(chip + shift, chips) * 2 + core
            xcopy(slot, t, peer, xs.at[slot, shift]).start()
        xcopy(slot, t, partner, xs.at[slot, 0]).start()

    def relay_x(slot):
        for shift in range(1, chips):
            source = lax.rem(chip + shift, chips) * 2 + core
            xcopy(slot, source, partner, xf.at[slot, shift]).wait_recv()
            xcopy(slot, source, partner, xf.at[slot, shift]).start()

    def wait_x(slot):
        for shift in range(chips):
            source = lax.rem(chip + shift, chips) * 2 + 1 - core
            xcopy(slot, source, partner, xf.at[slot, 0]).wait_recv()

    def guest_x_copy():
        return pltpu.make_async_remote_copy(
            X.at[0, t], XG.at[t], xs.at[L, 0], xr.at[L, t],
            device_id={"sp": me + inward}, device_id_type=MESH,
        )

    def guest_stat_copy():
        return pltpu.make_async_remote_copy(
            STAT.at[0, t], GSTAT.at[t], gs.at[0], gr.at[t],
            device_id={"sp": me + inward}, device_id_type=MESH,
        )

    def guest_stat_pass(source, peer):
        return pltpu.make_async_remote_copy(
            GSTAT.at[source], GSTAT.at[source], gs.at[0], gr.at[source],
            device_id={"tp": peer}, device_id_type=MESH,
        )

    def guest_back(index):
        start = pl.multiple_of(index * CHUNK + halo, 16)
        return pltpu.make_async_remote_copy(
            EXT.at[0, pl.ds(pl.multiple_of(guest_base + start, 16), CHUNK)],
            EXT.at[0, pl.ds(start, CHUNK)],
            bs.at[index], br.at[index],
            device_id={"sp": me + outward}, device_id_type=MESH,
        )

    def at_distance(k, body, select=None):
        if k == 0:
            body(me)
            return

        def step(index, _):
            owner = me + k - 2 * k * index
            ok = both(owner >= 0, owner < S)
            if select is not None:
                ok = both(ok, select(owner))

            @pl.when(ok)
            def _():
                body(owner)

            return 0

        lax.fori_loop(0, 2, step, 0)

    def multiply(total, x, layer, owner, start):
        at = lax.div(owner * Ds, Dt)
        columns = pl.ds(pl.multiple_of(lax.rem(owner * Ds, Dt), 128), Ds)
        xs_block = x[at, :, columns]
        for which, slots in ((0, WV), (1, WG)):
            part = jnp.dot(xs_block, slots[layer, owner], preferred_element_type=F32)
            if start:
                total[which] = part
            else:
                total[which] += part

    def project(layer, k, select=None):
        def block(owner):
            if k > 0:
                arrive(groups[layer][0] + groups[layer][1], owner)
            multiply(ACC, X.at[layer], layer, owner, k == 0)

        at_distance(k, block, select)

    def halo_copy(layer):
        end = halo + rows + (own_base if layer == 0 else 0)
        return pltpu.make_async_remote_copy(
            EXT.at[layer, pl.ds(pl.multiple_of(end - halo, 16), halo)],
            EXT.at[layer, pl.ds(0, halo)],
            hs.at[layer], hr.at[layer],
            device_id={"sp": me + 1}, device_id_type=MESH,
        )

    def sends_halo(layer):
        return both(no(last), no(first)) if layer == 0 else no(last)

    def takes_halo(layer):
        return both(no(first), no(low)) if layer == 0 else no(first)

    def gate_rows(layer, total, stat, base, where):
        mean = total_stat(stat, where)[:, :1] / features
        inv = lax.rsqrt(mean + epsilon)
        value, gating = total[0, where, :] * inv, total[1, where, :] * inv
        gated = (value / (1.0 + jnp.exp(-gating))).astype(BF16)
        EXT[layer, pl.ds(pl.multiple_of(base + where.start + halo, 16), where.size), :] = gated

    def gate(layer):
        base = own_base if layer == 0 else 0
        each_chunk(functools.partial(gate_rows, layer, ACC, STAT.at[2 * layer], base))

        @pl.when(sends_halo(layer))
        def _():
            halo_copy(layer).start()

    def convolve(layer):
        @pl.when(first)
        def _():
            EXT[layer, pl.ds(0, halo), :] = jnp.zeros((halo, Cn), BF16)

        @pl.when(takes_halo(layer))
        def _():
            halo_copy(layer).wait_recv()

        tall = CHUNK + halo + 8
        offset = halo - (taps - 1)
        base = own_base if layer == 0 else 0

        def body(where):
            if layer == 0:

                @pl.when(edge)
                def _():
                    guest_back(lax.div(where.start, CHUNK)).wait_recv()

            for column in range(0, Cn, 128):
                at = pl.ds(column, 128)
                window = EXT[layer, pl.ds(pl.multiple_of(base + where.start, 16), CHUNK + halo), at]
                tile = jnp.concatenate([window.astype(F32), jnp.zeros((8, 128), F32)], axis=0)
                total = jnp.zeros((CHUNK, 128), F32)
                for residue in range(8):
                    ks = [k for k in range(taps) if (k + offset) % 8 == residue]
                    if not ks:
                        continue
                    turned = pltpu.roll(tile, tall - residue, 0) if residue else tile
                    for k in ks:
                        low_row = k + offset - residue
                        total = total + taps_ref[k, layer : layer + 1, at] * turned[low_row : low_row + CHUNK]
                CONV[where, at] = total
            conved = CONV[where, :]
            put_stat(
                2 * layer + 1, where,
                jnp.sum(conved, axis=1, keepdims=True),
                jnp.sum(conved * conved, axis=1, keepdims=True),
            )

        each_chunk(body)
        send_stat(2 * layer + 1)

    def mix(layer):
        wait_stat(2 * layer + 1)

        def body(where):
            stat = total_stat(STAT.at[2 * layer + 1], where)
            mean = stat[:, 0:1] / channels
            spread = stat[:, 1:2] / channels - mean * mean
            normed = (CONV[where, :] - mean) * lax.rsqrt(spread + epsilon) * ng_ref[
                layer : layer + 1, :
            ] + ns_ref[layer : layer + 1, :]
            MIX[where, :] = (normed / (1.0 + jnp.exp(-normed))).astype(BF16)

        each_chunk(body)

    fine = Q if S == T else 1
    width = Dt // fine

    def cut(ref, q):
        return ref if fine == 1 else ref.at[:, pl.ds(pl.multiple_of(q * width, 128), width)]

    def pair_copy(layer, at, q):
        return pltpu.make_async_remote_copy(
            cut(PART.at[layer, 2 * at + 1 - core], q), cut(PRECV.at[layer, at], q),
            ps.at[layer, at], pr.at[layer, at, q], device_id={"tp": partner}, device_id_type=MESH,
        )

    def sum_copy(layer, at, q):
        return pltpu.make_async_remote_copy(
            cut(SUMB.at[layer, at], q), cut(RECV.at[layer, chip], q),
            rs.at[layer, at], rr.at[layer, chip, q],
            device_id={"tp": at * 2 + core}, device_id_type=MESH,
        )

    def sum_arrival(layer, at, q):
        return pltpu.make_async_remote_copy(
            cut(SUMB.at[layer, at], q), cut(RECV.at[layer, at], q),
            rs.at[layer, at], rr.at[layer, at, q],
            device_id={"tp": at * 2 + core}, device_id_type=MESH,
        )

    def columns_of(q):
        return pl.ds(pl.multiple_of(q * width, 128), width)

    def sum_pair(layer, at, q):
        pair_copy(layer, at, q).wait_recv()
        columns = columns_of(q)

        def body(where):
            SUMB[layer, at, where, columns] = (
                PART[layer, at * 2 + core, where, columns].astype(F32)
                + PRECV[layer, at, where, columns].astype(F32)
            ).astype(BF16)

        each_chunk(body)
        sum_copy(layer, at, q).start()

    def turn_order():
        count = Q // 2
        return [(False, g * count + piece, piece) for piece in range(count)] + [
            (True, (1 - g) * count + piece, piece) for piece in range(count)
        ]

    def branch(layer, k, part=None):
        def block(owner):
            target = lax.div(owner * Ds, Dt)
            base = lax.rem(owner * Ds, Dt)
            at = lax.div(target, 2)

            def product(q):
                columns = pl.ds(pl.multiple_of(base + q * Dq, 128), Dq)
                PART[layer, target, :, columns] = jnp.dot(
                    MIX[...], WO[layer, owner, q], preferred_element_type=F32
                ).astype(BF16)
                if S == T:

                    @pl.when(lax.rem(target, 2) != core)
                    def _():
                        pair_copy(layer, at, q).start()

            def total(q):
                if S == T:

                    @pl.when(both(lax.rem(target, 2) == core, at != chip))
                    def _():
                        sum_pair(layer, at, q)

            order = turn_order()
            early = order if k == 0 else [o for o in order if not o[0]]
            if part != 1:
                for _, q, _ in early:
                    product(q)
                for _, q, _ in early:
                    total(q)
            if k > 0 and part != 0:
                for _, q, piece in order[len(early) :]:
                    arrive([groups[layer][2][piece]], owner)
                    product(q)
                    total(q)

        at_distance(k, block)
        if S != T and k == S - 1 and part != 0:
            for shift in list(range(1, chips)) + [0]:
                pair_copy(layer, lax.rem(chip + shift, chips), 0).start()
            for shift in range(1, chips):
                sum_pair(layer, lax.rem(chip + shift, chips), 0)

    def finish(layer):
        source = h_ref if layer == 0 else HB
        target = out_ref if layer == L - 1 else HB
        for q in [q for _, q, _ in turn_order()] if fine > 1 else [0]:
            pair_copy(layer, chip, q).wait_recv()
            for shift in range(1, chips):
                sum_arrival(layer, lax.rem(chip + shift, chips), q).wait_recv()
            columns = columns_of(q)

            def body(where, columns=columns):
                total = PART[layer, t, where, columns].astype(F32) + PRECV[
                    layer, chip, where, columns
                ].astype(F32)
                for shift in range(1, chips):
                    total = total + RECV[layer, lax.rem(chip + shift, chips), where, columns].astype(F32)
                target[where, columns] = (source[where, columns].astype(F32) + total).astype(BF16)

            each_chunk(body)

    def sent(ref, sem):
        pltpu.make_async_remote_copy(
            ref, ref, sem, zr.at[0, 0], device_id={"tp": partner}, device_id_type=MESH
        ).wait_send()

    def half_ref(layer, which, owner, half):
        slots = sources[which][1]
        size = slots.shape[2] // 2
        return slots.at[layer, owner, pl.ds(pl.multiple_of(half * size, size), size)]

    def drain(layer, which):
        ids = groups[layer][which]
        whole = [item for item in ids if direct(item)]
        for way in (1, -1):

            @pl.when(inside(ids[0], me + way))
            def _(way=way):
                sent(half_ref(layer, which, me, g), zo.at[layer, which, (way + 1) // 2])

        @pl.when(edge)
        def _():
            if len(whole) == len(ids):
                sent(half_ref(layer, which, me, 1 - g), ys.at[layer, which, me])
            else:
                for item in whole:
                    sent(part_ref(item, me, 1 - g), ys.at[layer, which, me])

        def settle(owner, _):
            @pl.when(both(owner != me, inside(ids[0], me)))
            def _():
                @pl.when(inside(ids[0], jnp.where(owner < me, me + 1, me - 1)))
                def _():
                    sent(half_ref(layer, which, owner, g), zs.at[layer, which, owner])

                skip = skips_y(whole[0], owner)

                @pl.when(no(skip))
                def _():
                    sent(half_ref(layer, which, owner, g), ys.at[layer, which, owner])

                if len(whole) < len(ids):

                    @pl.when(skip)
                    def _():
                        for item in ids:
                            if item not in whole:
                                sent(part_ref(item, owner, g), ys.at[layer, which, owner])

            return 0

        lax.fori_loop(0, S, settle, 0)

    def drain_x(slot):
        for shift in range(chips):
            xcopy(slot, t, partner, xs.at[slot, shift]).wait_send()
        for shift in range(1, chips):
            xcopy(slot, t, partner, xf.at[slot, shift]).wait_send()

    def drain_stat(slot):
        sent(STAT.at[slot, pl.ds(0, T - 1)], ss.at[slot])

    def drain_start():
        @pl.when(edge)
        def _():
            guest_x_copy().wait_send()
            guest_stat_copy().wait_send()

        @pl.when(no(edge))
        def _():
            drain_x(0)
            drain_stat(0)

        @pl.when(near)
        def _():
            drain_x(L)
            sent(GSTAT.at[pl.ds(0, T - 1)], gs.at[0])
            for index in range(rows // CHUNK):
                guest_back(index).wait_send()

    def drain_sums(layer):
        for shift in range(chips):
            at = lax.rem(chip + shift, chips)
            sent(PRECV.at[layer, at], ps.at[layer, at])
        for shift in range(1, chips):
            at = lax.rem(chip + shift, chips)
            sent(SUMB.at[layer, at], rs.at[layer, at])

    def drain_halo(layer):
        @pl.when(sends_halo(layer))
        def _():
            halo_copy(layer).wait_send()

    barrier = pltpu.get_barrier_semaphore()
    for shift in range(1, T):
        pl.semaphore_signal(barrier, inc=1, device_id={"tp": lax.rem(t + shift, T)}, device_id_type=MESH)
    pl.semaphore_signal(barrier, inc=1, device_id={"grp": 1 - g}, device_id_type=MESH)

    @pl.when(no(first))
    def _():
        pl.semaphore_signal(barrier, inc=1, device_id={"sp": me - 1}, device_id_type=MESH)

    @pl.when(no(last))
    def _():
        pl.semaphore_signal(barrier, inc=1, device_id={"sp": me + 1}, device_id_type=MESH)

    inner = jnp.where(first, 0, 1) + jnp.where(last, 0, 1)
    pl.semaphore_wait(barrier, T + inner)

    value0, gating0, out0 = groups[0]
    for which in range(2):
        own_wait(0, which)
        send_own(groups[0][which])
    rest = [(0, 2)] + [(layer, which) for layer in range(1, L) for which in range(3)]
    for layer, which in rest:
        own_start(layer, which)
    for layer, which in rest:
        own_wait(layer, which)
        send_out(groups[layer][which])
    make_x(0)

    def owned_inside(owner):
        return no(is_edge(owner))

    def inner_take(ids, k, select=None):
        @pl.when(no(edge))
        def _():
            take(ids, k, select)

    def edge_take(ids, k):
        @pl.when(edge)
        def _():
            take(ids, k)

    def far_take(ids):
        for k in range(3, S):
            take(ids, k)

    @pl.when(edge)
    def _():
        guest_x_copy().start()
        guest_stat_copy().start()
        send_direct(value0 + gating0)
        send_own(out0)
        send_direct(out0)
        for layer in range(1, L):
            send_own(groups[layer][0] + groups[layer][1])
            send_direct(groups[layer][0] + groups[layer][1])
            send_own(groups[layer][2])
            send_direct(groups[layer][2])
        take(out0, 1)
        for layer in range(1, L):
            for which in range(3):
                take(groups[layer][which], 1)
        take(out0, 2)
        if L > 1:
            take(groups[1][0][:1], 2)

    @pl.when(no(edge))
    def _():
        send_x(0)
        send_stat(0)
        take(value0 + gating0, 1)
        send_own(out0)
        relay_x(0)
        wait_x(0)
        project(0, 0)
        for k in range(2, S - 1):
            take(value0, k)
            if k == 2:

                @pl.when(near)
                def _():
                    xcopy(L, t, partner, xf.at[L, 0]).wait_recv()
                    guest_stat_pass(t, partner).wait_recv()
                    send_x(L)
                    for shift in range(1, T):
                        guest_stat_pass(t, lax.rem(t + shift, T)).start()

            take(gating0, k)
            if k == 2 and L > 1:
                send_own(groups[1][0])
            project(0, k - 1, lambda owner: no(skips_y(value0[0], owner)))
        take(out0, 1, owned_inside)

        @pl.when(near)
        def _():
            relay_x(L)
            wait_x(L)
            for shift in range(1, T):
                guest_stat_pass(lax.rem(t + shift, T), partner).wait_recv()

        if L > 1:
            take(groups[1][0][:1], 1, owned_inside)
        take(out0[:1], 1, is_edge)
        project(0, S - 2)
        wait_stat(0)

        @pl.when(near)
        def _():
            corner = jnp.where(low, 0, S - 1)
            arrive(value0 + gating0, corner)
            multiply(ACC, X.at[0], 0, corner, False)
            multiply(GACC, XG, 0, me, True)

            def add(index, _):
                owner = lax.rem(me + index, S)
                multiply(GACC, XG, 0, owner, False)
                return 0

            lax.fori_loop(1, S, add, 0)

            def back(where):
                gate_rows(0, GACC, GSTAT, guest_base, where)
                guest_back(lax.div(where.start, CHUNK)).start()

            each_chunk(back)

        gate(0)
        take(out0[1:], 1, is_edge)
        if L > 1:
            send_own(groups[1][1])
            take(groups[1][0][1:], 1, owned_inside)

    for layer in range(L):
        out = groups[layer][2]
        ahead = groups[layer + 1] if layer + 1 < L else None
        if ahead and layer > 0:
            inner_take(ahead[0], 1, owned_inside)
            edge_take(ahead[0][:1], 2)
        convolve(layer)
        inner_take(out[1:] if layer > 0 else out[:1], 2)
        if layer > 0:
            far_take(out[:1])
        mix(layer)
        if layer == 0:
            inner_take(out[1:], 2)
        if ahead:
            edge_take(ahead[0][1:], 2)
        branch(layer, 0)
        branch(layer, 1)
        if ahead:
            inner_take(ahead[1][:1], 1, owned_inside)
        branch(layer, 2)
        if ahead is None:
            drain_stat(2 * layer + 1)
            drain_halo(layer)
            if layer > 0:
                drain_x(layer)
                drain_stat(2 * layer)
                drain(layer, 0)
                drain(layer, 1)
        far_take(out[1:] if layer > 0 else out)
        for k in range(3, S):
            branch(layer, k, 0)
        if ahead:
            inner_take(ahead[0], 1, is_edge)
            inner_take(ahead[1][1:], 1, owned_inside)
            edge_take(ahead[1][:1], 2)
        for k in range(3, S):
            branch(layer, k, 1)
        if ahead:
            inner_take(ahead[1][:1], 1, is_edge)
            inner_take(ahead[0][:1], 2)
            inner_take(ahead[1][1:], 1, is_edge)
        finish(layer)
        if ahead:
            after = layer + 1
            make_x(after)
            send_x(after)
            send_stat(2 * after)
            inner_take(ahead[0][1:], 2)

            @pl.when(no(edge))
            def _(ahead=ahead):
                send_own(ahead[2])

            edge_take(ahead[1][1:], 2)
            far_take(ahead[0])
            inner_take(ahead[1], 2)
            if layer == 0:
                drain_start()
                drain(0, 0)
                drain(0, 1)
            relay_x(after)
            far_take(ahead[1][:1])
            drain_stat(2 * layer + 1)
            drain_halo(layer)
            drain_sums(layer)
            far_take(ahead[1][1:])
            wait_x(after)
            project(after, 0)
            project(after, 1)
            inner_take(ahead[2][:1], 1, owned_inside)
            drain(layer, 2)
            if layer > 0:
                drain_x(layer)
                drain_stat(2 * layer)
                drain(layer, 0)
                drain(layer, 1)
            inner_take(ahead[2][1:], 1, owned_inside)
            inner_take(ahead[2], 1, is_edge)
            project(after, 2)
            edge_take(ahead[2][:1], 2)
            for k in range(3, S):
                project(after, k)
            wait_stat(2 * after)
            gate(after)
            edge_take(ahead[2][1:], 2)
            if after + 1 < L:

                @pl.when(no(edge))
                def _(after=after):
                    send_own(groups[after + 1][0] + groups[after + 1][1])

            inner_take(ahead[2][:1], 2)

    drain(L - 1, 2)
    drain_sums(L - 1)


def shards(hidden_in, in_gain, w_value, w_gate, conv_taps, norm_gain, norm_shift, w_out):
    S, T = lax.axis_size("sp"), lax.axis_size("tp")
    L, Ds, Cn = w_value.shape
    rows, Dt = hidden_in.shape
    chips = T // 2
    halo = (conv_taps.shape[1] - 1 + 15) // 16 * 16
    items = L * sum(cuts(Ds))
    Q = 2 * cuts(Ds)[2]
    fine = Q if S == T else 1
    vmem = pl.BlockSpec(memory_space=pltpu.VMEM)
    hbm = pl.BlockSpec(memory_space=pl.ANY)
    dma = pltpu.SemaphoreType.DMA
    return pl.pallas_call(
        functools.partial(kernel, S, T),
        out_shape=jax.ShapeDtypeStruct((rows, Dt), BF16),
        in_specs=[vmem, vmem, hbm, hbm, vmem, vmem, vmem, hbm],
        out_specs=vmem,
        scratch_shapes=[
            pltpu.VMEM((L, S, Ds, Cn), BF16),
            pltpu.VMEM((L, S, Ds, Cn), BF16),
            pltpu.VMEM((L, S, Q, Cn, Ds // Q), BF16),
            pltpu.VMEM((L, T, rows, Dt), BF16),
            pltpu.VMEM((T, rows, Dt), BF16),
            pltpu.VMEM((2, rows, Cn), F32),
            pltpu.VMEM((2, rows, Cn), F32),
            pltpu.VMEM((L, halo + 2 * rows, Cn), BF16),
            pltpu.VMEM((rows, Cn), F32),
            pltpu.VMEM((rows, Cn), BF16),
            pltpu.VMEM((L, T, rows, Dt), BF16),
            pltpu.VMEM((L, chips, rows, Dt), BF16),
            pltpu.VMEM((L, chips, rows, Dt), BF16),
            pltpu.VMEM((L, chips, rows, Dt), BF16),
            pltpu.VMEM((2 * L, T, 8, rows), F32),
            pltpu.VMEM((T, 8, rows), F32),
            pltpu.VMEM((rows, Dt), BF16),
            dma((L, 3)),
            dma((items, S)), dma((L, 3, S)), dma((L, 3, 2)), dma((items, S)), dma((L, 3, S)),
            dma((L + 1, T)), dma((L + 1, chips)), dma((L + 1, chips)),
            dma((2 * L, T)), dma((2 * L,)),
            dma((T,)), dma((1,)),
            dma((L,)), dma((L,)),
            dma((rows // CHUNK,)), dma((rows // CHUNK,)),
            dma((L, chips, fine)), dma((L, chips)),
            dma((L, chips, fine)), dma((L, chips)),
        ],
        compiler_params=pltpu.CompilerParams(
            collective_id=0, has_side_effects=True, vmem_limit_bytes=64_000_000
        ),
    )(hidden_in, in_gain, w_value, w_gate, jnp.swapaxes(conv_taps, 0, 1), norm_gain, norm_shift, w_out)


def solution(mesh):
    placed = (
        P(("grp", "sp"), "tp"),
        P(None, "tp"),
        P(None, "sp", "tp"),
        P(None, "sp", "tp"),
        P(None, None, "tp"),
        P(None, "tp"),
        P(None, "tp"),
        P(None, "tp", "sp"),
    )
    return jax.shard_map(
        shards, mesh=mesh, in_specs=placed, out_specs=P(("grp", "sp"), "tp"), check_vma=False
    )
```

```python
import functools

import jax
import jax.numpy as jnp
from jax import lax
from jax.experimental import pallas as pl
from jax.experimental.pallas import tpu as pltpu
from jax.sharding import PartitionSpec as P

epsilon = 1e-06
CHUNK = 128
F32, BF16 = jnp.float32, jnp.bfloat16


def cuts(Ds, layer):
    if Ds < 512:
        return (1, 1, 1)
    return (2, 2, 2) if layer == 0 else (2, 4, 4)


def kernel(
    S, T, h_ref, gain_ref, wv_ref, wg_ref, taps_ref, ng_ref, ns_ref, wo_ref, out_ref,
    WV, WG, WO, X, XG, ACC, GACC, EXT, CONV, MIX, PART, PRECV, SUMB, RECV, STAT, GSTAT, HB,
    own_sem, zr, zs, zo, yr, ys, xr, xs, xf, sr, ss, gr, gs, hr, hs, br, bs,
    pr, ps, rr, rs,
):
    L = wv_ref.shape[0]
    Ds, Cn = wv_ref.shape[1], wv_ref.shape[2]
    rows, Dt = h_ref.shape
    taps = taps_ref.shape[0]
    features, channels = Dt * T, Cn * T
    chips = T // 2
    Q, Dq = WO.shape[2], WO.shape[4]
    halo = EXT.shape[1] - 2 * rows
    g, me, t = lax.axis_index("grp"), lax.axis_index("sp"), lax.axis_index("tp")
    core = lax.rem(t, 2)
    chip = lax.div(t, 2)
    partner = t + 1 - 2 * core
    MESH = pl.DeviceIdType.MESH
    both, either, no = jnp.logical_and, jnp.logical_or, jnp.logical_not
    first, last = me == 0, me == S - 1
    low, high = me == 1, me == S - 2
    edge, near = either(first, last), either(low, high)
    inward = jnp.where(first, 1, -1)
    outward = jnp.where(low, -1, 1)
    own_base = jnp.where(low, rows, 0)
    guest_base = jnp.where(low, 0, rows)

    def is_edge(plane):
        return either(plane == 0, plane == S - 1)

    table = []
    groups = []
    for layer in range(L):
        of_layer = []
        for which in range(3):
            ids = []
            for piece in range(cuts(Ds, layer)[which]):
                ids.append(len(table))
                table.append((layer, which, piece, cuts(Ds, layer)[which]))
            of_layer.append(ids)
        groups.append(of_layer)
    items = len(table)

    def fore(ids):
        return ids[: (len(ids) + 1) // 2]

    def aft(ids):
        return ids[(len(ids) + 1) // 2 :]

    def direct(item):
        _, which, piece, pieces = table[item]
        return which != 1 or 2 * piece < pieces

    def folded(item):
        layer, which, _, _ = table[item]
        return layer == 0 and which < 2

    def inside(item, plane):
        low_end, high_end = (1, S - 2) if folded(item) else (0, S - 1)
        return both(plane >= low_end, plane <= high_end)

    def skips_y(item, owner):
        if not direct(item):
            return jnp.bool_(False)
        return either(both(owner == 0, low), both(owner == S - 1, high))

    sources = [(wv_ref, WV), (wg_ref, WG), (wo_ref, WO)]

    def own(layer, which):
        source, slots = sources[which]
        if which < 2:
            return [pltpu.make_async_copy(source.at[layer], slots.at[layer, me], own_sem.at[layer, which])]
        return [
            pltpu.make_async_copy(
                source.at[layer, :, pl.ds(q * Dq, Dq)], slots.at[layer, me, q], own_sem.at[layer, 2]
            )
            for q in range(Q)
        ]

    def own_start(layer, which):
        for copy in own(layer, which):
            copy.start()

    own_start(0, 0)
    own_start(0, 1)

    def own_wait(layer, which):
        slot = sources[which][1].at[layer, me]
        pltpu.make_async_copy(slot, slot, own_sem.at[layer, which]).wait()

    def each_chunk(body, start=0, count=rows):
        def step(index, _):
            body(pl.ds(pl.multiple_of(index * CHUNK, CHUNK), CHUNK))
            return 0

        lax.fori_loop(start // CHUNK, (start + count) // CHUNK, step, 0)

    def parts_of(layer):
        return [(0, rows)]

    def put_stat(slot, where, left, right):
        lane = lax.broadcasted_iota(jnp.int32, (left.shape[0], 128), 1)
        wide = jnp.where(lane == 0, left, right)
        STAT[slot, t, :, where] = wide.T[:8]

    def stat_ref(slot, source, part):
        if slot % 2 == 0:
            return STAT.at[slot, source]
        start, count = parts_of(slot // 2)[part]
        return STAT.at[slot, source, :, pl.ds(start, count)]

    def stat_sem(slot, part):
        return 2 * L + slot // 2 if part else slot

    def stat_copy(slot, peer, part):
        at = stat_sem(slot, part)
        return pltpu.make_async_remote_copy(
            stat_ref(slot, t, part), stat_ref(slot, t, part), ss.at[at], sr.at[at, t],
            device_id={"tp": peer}, device_id_type=MESH,
        )

    def stat_arrival(slot, peer, part):
        at = stat_sem(slot, part)
        return pltpu.make_async_remote_copy(
            stat_ref(slot, peer, part), stat_ref(slot, peer, part), ss.at[at], sr.at[at, peer],
            device_id={"tp": peer}, device_id_type=MESH,
        )

    def send_stat(slot, part=0):
        for shift in range(1, T):
            stat_copy(slot, lax.rem(t + shift, T), part).start()

    def wait_stat(slot, part=0):
        for shift in range(1, T):
            stat_arrival(slot, lax.rem(t + shift, T), part).wait_recv()

    def total_stat(stat, where):
        total = stat[0, :, where]
        for peer in range(1, T):
            total = total + stat[peer, :, where]
        return jnp.concatenate([total] * 16, axis=0).T

    def part_ref(item, owner, half):
        layer, which, piece, pieces = table[item]
        slots = sources[which][1]
        if which == 2:
            split = 2 * pieces // Q
            size = Cn // split
            return slots.at[layer, owner, half * (Q // 2) + piece // split, pl.ds(piece % split * size, size)]
        size = slots.shape[2] // (2 * pieces)
        start = pl.multiple_of(half * (size * pieces) + piece * size, size)
        return slots.at[layer, owner, pl.ds(start, size)]

    def zcopy(item, owner, way):
        ref = part_ref(item, owner, g)
        layer, which, _, _ = table[item]
        return pltpu.make_async_remote_copy(
            ref, ref, zs.at[layer, which, owner], zr.at[item, owner],
            device_id={"sp": me + way}, device_id_type=MESH,
        )

    def zown(item, way):
        ref = part_ref(item, me, g)
        layer, which, _, _ = table[item]
        return pltpu.make_async_remote_copy(
            ref, ref, zo.at[layer, which, (way + 1) // 2], zr.at[item, me],
            device_id={"sp": me + way}, device_id_type=MESH,
        )

    def dcopy(item, owner):
        ref = part_ref(item, owner, 1 - g)
        layer, which, _, _ = table[item]
        return pltpu.make_async_remote_copy(
            ref, ref, ys.at[layer, which, owner], yr.at[item, owner],
            device_id={"sp": me + inward}, device_id_type=MESH,
        )

    def ycopy(item, owner):
        ref = part_ref(item, owner, g)
        return pltpu.make_async_remote_copy(
            ref, ref, ys.at[table[item][0], table[item][1], owner], yr.at[item, owner],
            device_id={"grp": 1 - g}, device_id_type=MESH,
        )

    def yarrival(item, owner):
        ref = part_ref(item, owner, 1 - g)
        return pltpu.make_async_remote_copy(
            ref, ref, ys.at[table[item][0], table[item][1], owner], yr.at[item, owner],
            device_id={"grp": 1 - g}, device_id_type=MESH,
        )

    def outgoing(way):
        return low if way < 0 else high

    def send_out(ids):
        for item in ids:
            for way in (1, -1):

                @pl.when(outgoing(way))
                def _(item=item, way=way):
                    zown(item, way).start()

    def send_own(ids):
        for item in ids:
            for way in (1, -1):
                allowed = inside(item, me + way)
                if not folded(item):
                    allowed = both(allowed, no(outgoing(way)))

                @pl.when(allowed)
                def _(item=item, way=way):
                    zown(item, way).start()

    def send_direct(ids):
        for item in ids:
            if direct(item):
                dcopy(item, me).start()

    def take(ids, k, select=None):
        for item in ids:
            for way in (1, -1):
                owner = me - way * k
                ok = both(both(owner >= 0, owner < S), inside(item, me))
                if select is not None:
                    ok = both(ok, select(owner))

                @pl.when(ok)
                def _(item=item, way=way, owner=owner):
                    zcopy(item, owner, way).wait_recv()

                    @pl.when(inside(item, me + way))
                    def _():
                        zcopy(item, owner, way).start()

                    @pl.when(no(skips_y(item, owner)))
                    def _():
                        ycopy(item, owner).start()

    def arrive(ids, owner):
        for item in ids:
            yarrival(item, owner).wait_recv()

    def x_ref(slot, source):
        return XG.at[source] if slot == L else X.at[slot, source]

    def xcopy(slot, source, peer, sem):
        return pltpu.make_async_remote_copy(
            x_ref(slot, source), x_ref(slot, source), sem, xr.at[slot, source],
            device_id={"tp": peer}, device_id_type=MESH,
        )

    def make_x(layer):
        source = h_ref if layer == 0 else HB

        def body(where):
            wide = source[where, :].astype(F32)
            X[layer, t, where, :] = (wide * gain_ref[layer : layer + 1, :]).astype(BF16)
            squares = jnp.sum(wide * wide, axis=1, keepdims=True)
            put_stat(2 * layer, where, squares, squares)

        each_chunk(body)

    def send_x(slot):
        for shift in range(1, chips):
            peer = lax.rem(chip + shift, chips) * 2 + core
            xcopy(slot, t, peer, xs.at[slot, shift]).start()
        xcopy(slot, t, partner, xs.at[slot, 0]).start()

    def relay_x(slot):
        for shift in range(1, chips):
            source = lax.rem(chip + shift, chips) * 2 + core
            xcopy(slot, source, partner, xf.at[slot, shift]).wait_recv()
            xcopy(slot, source, partner, xf.at[slot, shift]).start()

    def wait_x(slot):
        for shift in range(chips):
            source = lax.rem(chip + shift, chips) * 2 + 1 - core
            xcopy(slot, source, partner, xf.at[slot, 0]).wait_recv()

    def guest_x_copy():
        return pltpu.make_async_remote_copy(
            X.at[0, t], XG.at[t], xs.at[L, 0], xr.at[L, t],
            device_id={"sp": me + inward}, device_id_type=MESH,
        )

    def guest_stat_copy():
        return pltpu.make_async_remote_copy(
            STAT.at[0, t], GSTAT.at[t], gs.at[0], gr.at[t],
            device_id={"sp": me + inward}, device_id_type=MESH,
        )

    def guest_stat_pass(source, peer):
        return pltpu.make_async_remote_copy(
            GSTAT.at[source], GSTAT.at[source], gs.at[0], gr.at[source],
            device_id={"tp": peer}, device_id_type=MESH,
        )

    def guest_back(index):
        start = pl.multiple_of(index * CHUNK + halo, 16)
        return pltpu.make_async_remote_copy(
            EXT.at[0, pl.ds(pl.multiple_of(guest_base + start, 16), CHUNK)],
            EXT.at[0, pl.ds(start, CHUNK)],
            bs.at[index], br.at[index],
            device_id={"sp": me + outward}, device_id_type=MESH,
        )

    def at_distance(k, body, select=None):
        if k == 0:
            if select is None:
                body(me)
            else:
                pl.when(select(me))(lambda: body(me))
            return

        def step(index, _):
            owner = me + k - 2 * k * index
            ok = both(owner >= 0, owner < S)
            if select is not None:
                ok = both(ok, select(owner))

            @pl.when(ok)
            def _():
                body(owner)

            return 0

        lax.fori_loop(0, 2, step, 0)

    def multiply(total, x, layer, owner, start):
        at = lax.div(owner * Ds, Dt)
        columns = pl.ds(pl.multiple_of(lax.rem(owner * Ds, Dt), 128), Ds)
        xs_block = x[at, :, columns]
        for which, slots in ((0, WV), (1, WG)):
            part = jnp.dot(xs_block, slots[layer, owner], preferred_element_type=F32)
            if start:
                total[which] = part
            else:
                total[which] += part

    def project(layer, k, select=None):
        def block(owner):
            if k > 0:
                arrive(groups[layer][0] + groups[layer][1], owner)
            multiply(ACC, X.at[layer], layer, owner, k == 0)

        at_distance(k, block, select)

    def halo_copy(layer):
        end = halo + rows + (own_base if layer == 0 else 0)
        return pltpu.make_async_remote_copy(
            EXT.at[layer, pl.ds(pl.multiple_of(end - halo, 16), halo)],
            EXT.at[layer, pl.ds(0, halo)],
            hs.at[layer], hr.at[layer],
            device_id={"sp": me + 1}, device_id_type=MESH,
        )

    def sends_halo(layer):
        return both(no(last), no(first)) if layer == 0 else no(last)

    def takes_halo(layer):
        return both(no(first), no(low)) if layer == 0 else no(first)

    def gate_rows(layer, total, stat, base, where):
        mean = total_stat(stat, where)[:, :1] / features
        inv = lax.rsqrt(mean + epsilon)
        value, gating = total[0, where, :] * inv, total[1, where, :] * inv
        gated = (value / (1.0 + jnp.exp(-gating))).astype(BF16)
        EXT[layer, pl.ds(pl.multiple_of(base + where.start + halo, 16), where.size), :] = gated

    def gate(layer):
        base = own_base if layer == 0 else 0
        each_chunk(functools.partial(gate_rows, layer, ACC, STAT.at[2 * layer], base))

        @pl.when(sends_halo(layer))
        def _():
            halo_copy(layer).start()

    def convolve(layer, part):
        start, count = parts_of(layer)[part]
        if start == 0:

            @pl.when(first)
            def _():
                EXT[layer, pl.ds(0, halo), :] = jnp.zeros((halo, Cn), BF16)

            @pl.when(takes_halo(layer))
            def _():
                halo_copy(layer).wait_recv()

        tall = CHUNK + halo + 8
        offset = halo - (taps - 1)
        base = own_base if layer == 0 else 0

        def body(where):
            if layer == 0:

                @pl.when(edge)
                def _():
                    guest_back(lax.div(where.start, CHUNK)).wait_recv()

            for column in range(0, Cn, 128):
                at = pl.ds(column, 128)
                window = EXT[layer, pl.ds(pl.multiple_of(base + where.start, 16), CHUNK + halo), at]
                tile = jnp.concatenate([window.astype(F32), jnp.zeros((8, 128), F32)], axis=0)
                total = jnp.zeros((CHUNK, 128), F32)
                for residue in range(8):
                    ks = [k for k in range(taps) if (k + offset) % 8 == residue]
                    if not ks:
                        continue
                    turned = pltpu.roll(tile, tall - residue, 0) if residue else tile
                    for k in ks:
                        low_row = k + offset - residue
                        total = total + taps_ref[k, layer : layer + 1, at] * turned[low_row : low_row + CHUNK]
                CONV[where, at] = total
            conved = CONV[where, :]
            put_stat(
                2 * layer + 1, where,
                jnp.sum(conved, axis=1, keepdims=True),
                jnp.sum(conved * conved, axis=1, keepdims=True),
            )

        each_chunk(body, start, count)
        send_stat(2 * layer + 1, part)

    def mix(layer, part):
        start, count = parts_of(layer)[part]
        wait_stat(2 * layer + 1, part)

        def body(where):
            stat = total_stat(STAT.at[2 * layer + 1], where)
            mean = stat[:, 0:1] / channels
            spread = stat[:, 1:2] / channels - mean * mean
            normed = (CONV[where, :] - mean) * lax.rsqrt(spread + epsilon) * ng_ref[
                layer : layer + 1, :
            ] + ns_ref[layer : layer + 1, :]
            MIX[where, :] = (normed / (1.0 + jnp.exp(-normed))).astype(BF16)

        each_chunk(body, start, count)

    fine = Q if S == T else 1
    width = Dt // fine

    def cut(layer, ref, q, part):
        start, count = parts_of(layer)[part]
        return ref.at[pl.ds(start, count), columns_of(q)]

    def columns_of(q):
        return pl.ds(0, width) if fine == 1 else pl.ds(pl.multiple_of(q * width, 128), width)

    def pair_copy(layer, at, q, part):
        return pltpu.make_async_remote_copy(
            cut(layer, PART.at[layer, 2 * at + 1 - core], q, part), cut(layer, PRECV.at[layer, at], q, part),
            ps.at[layer, at], pr.at[layer, at, part, q],
            device_id={"tp": partner}, device_id_type=MESH,
        )

    def sum_copy(layer, at, q, part):
        return pltpu.make_async_remote_copy(
            cut(layer, SUMB.at[layer, at], q, part), cut(layer, RECV.at[layer, chip], q, part),
            rs.at[layer, at], rr.at[layer, chip, part, q],
            device_id={"tp": at * 2 + core}, device_id_type=MESH,
        )

    def sum_arrival(layer, at, q, part):
        return pltpu.make_async_remote_copy(
            cut(layer, SUMB.at[layer, at], q, part), cut(layer, RECV.at[layer, at], q, part),
            rs.at[layer, at], rr.at[layer, at, part, q],
            device_id={"tp": at * 2 + core}, device_id_type=MESH,
        )

    def sum_pair(layer, at, q, part):
        pair_copy(layer, at, q, part).wait_recv()
        columns = columns_of(q)

        def body(where):
            SUMB[layer, at, where, columns] = (
                PART[layer, at * 2 + core, where, columns].astype(F32)
                + PRECV[layer, at, where, columns].astype(F32)
            ).astype(BF16)

        each_chunk(body, *parts_of(layer)[part])
        sum_copy(layer, at, q, part).start()

    def turn_order():
        count = Q // 2
        return [(False, g * count + piece, piece) for piece in range(count)] + [
            (True, (1 - g) * count + piece, piece) for piece in range(count)
        ]

    def branch(layer, k, parts, early=True, late=True, wait=True, only=None, select=None, together=False):
        def block(owner):
            target = lax.div(owner * Ds, Dt)
            base = lax.rem(owner * Ds, Dt)
            at = lax.div(target, 2)

            def product(q, part):
                start, count = parts_of(layer)[part]
                columns = pl.ds(pl.multiple_of(base + q * Dq, 128), Dq)
                PART[layer, target, pl.ds(start, count), columns] = jnp.dot(
                    MIX[pl.ds(start, count), :], WO[layer, owner, q], preferred_element_type=F32
                ).astype(BF16)
                if S == T:

                    @pl.when(lax.rem(target, 2) != core)
                    def _():
                        pair_copy(layer, at, q, part).start()

            def total(q, part):
                if S == T:

                    @pl.when(both(lax.rem(target, 2) == core, at != chip))
                    def _():
                        sum_pair(layer, at, q, part)

            order = [o for o in turn_order() if only is None or o[2] in only]
            group = order if k == 0 or together else [o for o in order if not o[0]]
            if together and k > 0:
                arrive(groups[layer][2], owner)
            if early:
                for part in parts:
                    for _, q, _ in group:
                        product(q, part)
                    for _, q, _ in group:
                        total(q, part)
            if k > 0 and late:
                for _, q, piece in order[len(group) :]:
                    if wait:
                        ids = groups[layer][2]
                        split = 2 * len(ids) // Q
                        arrive(ids[piece * split : (piece + 1) * split], owner)
                    for part in parts:
                        product(q, part)
                    for part in parts:
                        total(q, part)

        at_distance(k, block, select)

    def stays(owner):
        return lax.div(owner * Ds, 2 * Dt) == chip

    def leaves(owner):
        return no(stays(owner))

    def share(layer):
        if S != T:
            for part in range(len(parts_of(layer))):
                for shift in list(range(1, chips)) + [0]:
                    pair_copy(layer, lax.rem(chip + shift, chips), 0, part).start()
                for shift in range(1, chips):
                    sum_pair(layer, lax.rem(chip + shift, chips), 0, part)

    def finish(layer):
        share(layer)
        source = h_ref if layer == 0 else HB
        target = out_ref if layer == L - 1 else HB
        for part, (start, count) in enumerate(parts_of(layer)):
            for q in [q for _, q, _ in turn_order()] if fine > 1 else [0]:
                pair_copy(layer, chip, q, part).wait_recv()
                for shift in range(1, chips):
                    sum_arrival(layer, lax.rem(chip + shift, chips), q, part).wait_recv()
                columns = columns_of(q)

                def body(where, columns=columns):
                    total = PART[layer, t, where, columns].astype(F32) + PRECV[
                        layer, chip, where, columns
                    ].astype(F32)
                    for shift in range(1, chips):
                        total = total + RECV[layer, lax.rem(chip + shift, chips), where, columns].astype(F32)
                    target[where, columns] = (source[where, columns].astype(F32) + total).astype(BF16)

                each_chunk(body, start, count)

    def sent(ref, sem):
        pltpu.make_async_remote_copy(
            ref, ref, sem, zr.at[0, 0], device_id={"tp": partner}, device_id_type=MESH
        ).wait_send()

    def half_ref(layer, which, owner, half):
        slots = sources[which][1]
        size = slots.shape[2] // 2
        return slots.at[layer, owner, pl.ds(pl.multiple_of(half * size, size), size)]

    def some_ref(layer, which, owner, half, begin, count, pieces):
        if count == pieces:
            return half_ref(layer, which, owner, half)
        slots = sources[which][1]
        size = slots.shape[2] // (2 * pieces)
        start = pl.multiple_of(half * (size * pieces) + begin * size, size)
        return slots.at[layer, owner, pl.ds(start, size * count)]

    def drain(layer, which):
        ids = groups[layer][which]
        whole = [item for item in ids if direct(item)]
        for way in (1, -1):

            @pl.when(inside(ids[0], me + way))
            def _(way=way):
                sent(half_ref(layer, which, me, g), zo.at[layer, which, (way + 1) // 2])

        @pl.when(edge)
        def _():
            sent(some_ref(layer, which, me, 1 - g, 0, len(whole), len(ids)), ys.at[layer, which, me])

        def settle(owner, _):
            @pl.when(both(owner != me, inside(ids[0], me)))
            def _():
                @pl.when(inside(ids[0], jnp.where(owner < me, me + 1, me - 1)))
                def _():
                    sent(half_ref(layer, which, owner, g), zs.at[layer, which, owner])

                skip = skips_y(whole[0], owner)

                @pl.when(no(skip))
                def _():
                    sent(half_ref(layer, which, owner, g), ys.at[layer, which, owner])

                if len(whole) < len(ids):

                    @pl.when(skip)
                    def _():
                        sent(
                            some_ref(layer, which, owner, g, len(whole), len(ids) - len(whole), len(ids)),
                            ys.at[layer, which, owner],
                        )

            return 0

        lax.fori_loop(0, S, settle, 0)

    def drain_x(slot):
        for shift in range(chips):
            xcopy(slot, t, partner, xs.at[slot, shift]).wait_send()
        for shift in range(1, chips):
            xcopy(slot, t, partner, xf.at[slot, shift]).wait_send()

    def drain_stat(slot):
        if slot % 2 == 0:
            sent(STAT.at[slot, pl.ds(0, T - 1)], ss.at[slot])
            return
        for part, (start, count) in enumerate(parts_of(slot // 2)):
            sent(STAT.at[slot, pl.ds(0, T - 1), :, pl.ds(start, count)], ss.at[stat_sem(slot, part)])

    def drain_start():
        @pl.when(edge)
        def _():
            guest_x_copy().wait_send()
            guest_stat_copy().wait_send()

        @pl.when(no(edge))
        def _():
            drain_x(0)
            drain_stat(0)

        @pl.when(near)
        def _():
            drain_x(L)
            sent(GSTAT.at[pl.ds(0, T - 1)], gs.at[0])
            for index in range(rows // CHUNK):
                guest_back(index).wait_send()

    def drain_sums(layer):
        for shift in range(chips):
            at = lax.rem(chip + shift, chips)
            sent(PRECV.at[layer, at], ps.at[layer, at])
        for shift in range(1, chips):
            at = lax.rem(chip + shift, chips)
            sent(SUMB.at[layer, at], rs.at[layer, at])

    def drain_halo(layer):
        @pl.when(sends_halo(layer))
        def _():
            halo_copy(layer).wait_send()

    barrier = pltpu.get_barrier_semaphore()
    for shift in range(1, T):
        pl.semaphore_signal(barrier, inc=1, device_id={"tp": lax.rem(t + shift, T)}, device_id_type=MESH)
    pl.semaphore_signal(barrier, inc=1, device_id={"grp": 1 - g}, device_id_type=MESH)

    @pl.when(no(first))
    def _():
        pl.semaphore_signal(barrier, inc=1, device_id={"sp": me - 1}, device_id_type=MESH)

    @pl.when(no(last))
    def _():
        pl.semaphore_signal(barrier, inc=1, device_id={"sp": me + 1}, device_id_type=MESH)

    inner = jnp.where(first, 0, 1) + jnp.where(last, 0, 1)
    pl.semaphore_wait(barrier, T + inner)

    value0, gating0, out0 = groups[0]
    for which in range(2):
        own_wait(0, which)
        send_own(groups[0][which])
    rest = [(0, 2)] + [(layer, which) for layer in range(1, L) for which in range(3)]
    for layer, which in rest:
        own_start(layer, which)
    for layer, which in rest:
        own_wait(layer, which)
        send_out(groups[layer][which])
    make_x(0)

    def owned_inside(owner):
        return no(is_edge(owner))

    def inner_take(ids, k, select=None):
        @pl.when(no(edge))
        def _():
            take(ids, k, select)

    def edge_take(ids, k):
        @pl.when(edge)
        def _():
            take(ids, k)

    def far_take(ids):
        for k in range(3, S):
            take(ids, k)

    @pl.when(edge)
    def _():
        guest_x_copy().start()
        guest_stat_copy().start()
        send_direct(value0 + gating0)
        send_own(out0)
        send_direct(out0)
        for layer in range(1, L):
            send_own(groups[layer][0] + groups[layer][1])
            send_direct(groups[layer][0] + groups[layer][1])
            send_own(groups[layer][2])
            send_direct(groups[layer][2])
        take(out0, 1)
        for layer in range(1, L):
            for which in range(3):
                take(groups[layer][which], 1)
        take(out0, 2)
        if L > 1:
            take(fore(groups[1][0]), 2)

    @pl.when(no(edge))
    def _():
        send_x(0)
        send_stat(0)
        take(value0 + gating0, 1)
        send_own(out0)
        relay_x(0)
        wait_x(0)
        project(0, 0)
        for k in range(2, S - 1):
            take(value0, k)
            if k == 2:

                @pl.when(near)
                def _():
                    xcopy(L, t, partner, xf.at[L, 0]).wait_recv()
                    guest_stat_pass(t, partner).wait_recv()
                    send_x(L)
                    for shift in range(1, T):
                        guest_stat_pass(t, lax.rem(t + shift, T)).start()

            take(gating0, k)
            if k == 2 and L > 1:
                send_own(groups[1][0])
            project(0, k - 1, lambda owner: no(skips_y(value0[0], owner)))
        take(out0, 1, owned_inside)

        @pl.when(near)
        def _():
            relay_x(L)
            wait_x(L)
            for shift in range(1, T):
                guest_stat_pass(lax.rem(t + shift, T), partner).wait_recv()

        if L > 1:
            take(fore(groups[1][0]), 1, owned_inside)
        take(fore(out0), 1, is_edge)
        project(0, S - 2)
        wait_stat(0)

        @pl.when(near)
        def _():
            corner = jnp.where(low, 0, S - 1)
            arrive(value0 + gating0, corner)
            multiply(ACC, X.at[0], 0, corner, False)
            multiply(GACC, XG, 0, me, True)

            def add(index, _):
                owner = lax.rem(me + index, S)
                multiply(GACC, XG, 0, owner, False)
                return 0

            lax.fori_loop(1, S, add, 0)

            def back(where):
                gate_rows(0, GACC, GSTAT, guest_base, where)
                guest_back(lax.div(where.start, CHUNK)).start()

            each_chunk(back)

        gate(0)
        take(aft(out0), 1, is_edge)
        if L > 1:
            send_own(groups[1][1])
            take(aft(groups[1][0]), 1, owned_inside)

    for layer in range(L):
        out = groups[layer][2]
        ahead = groups[layer + 1] if layer + 1 < L else None
        every = list(range(len(parts_of(layer))))
        columns = list(range(Q // 2))
        head_columns, tail_columns = columns[: Q // 4], columns[Q // 4 :]
        if ahead and layer > 0:
            inner_take(ahead[0], 1, owned_inside)
            edge_take(fore(ahead[0]), 2)
        if layer == 0:
            convolve(0, 0)
            inner_take(fore(out), 2)
            mix(0, 0)
            inner_take(aft(out), 2)
        else:
            inner_take(aft(out), 2)
            convolve(layer, 0)
            far_take(fore(out))
            mix(layer, 0)
            for k in range(3):
                branch(layer, k, every, select=leaves, together=True)
            far_take(aft(out)[:1])
            for k in range(3, S):
                branch(layer, k, every, late=False, only=head_columns, select=leaves)
            far_take(aft(out)[1:])
            for k in range(3):
                branch(layer, k, every, select=stays, together=True)
            for k in range(3, S):
                branch(layer, k, every, late=False, only=head_columns, select=stays)
        if ahead:
            edge_take(aft(ahead[0]), 2)
        if layer == 0:
            branch(layer, 0, [0])
            branch(layer, 1, [0])
            far_take(fore(out))
            if ahead:
                inner_take(fore(ahead[1]), 1, owned_inside)
                inner_take(fore(ahead[0]), 1, is_edge)
            branch(layer, 2, [0], late=False)
            if ahead:
                inner_take(aft(ahead[0]), 1, is_edge)
                inner_take(aft(ahead[1]), 1, owned_inside)
            branch(layer, 2, [0], early=False)
        else:
            for k in range(3, S):
                branch(layer, k, every, early=False, only=head_columns)
                branch(layer, k, every, late=False, only=tail_columns)
            if ahead:
                inner_take(fore(ahead[1]), 1, owned_inside)
                inner_take(ahead[0], 1, is_edge)
                inner_take(aft(ahead[1]), 1, owned_inside)
        if ahead is None:
            drain_stat(2 * layer + 1)
            drain_halo(layer)
            if layer > 0:
                drain_x(layer)
                drain_stat(2 * layer)
                drain(layer, 0)
                drain(layer, 1)
        if layer == 0:
            far_take(aft(out))
        for k in range(3, S) if layer == 0 else []:
            branch(layer, k, every, late=False)
        if ahead:
            edge_take(fore(ahead[1]), 2)
            for k in range(3, S):
                branch(layer, k, every, early=False, only=head_columns)
            edge_take(aft(ahead[1])[:1], 2)
            for k in range(3, S):
                branch(layer, k, every, early=False, only=tail_columns)
        else:
            for k in range(3, S):
                branch(layer, k, every, early=False, only=tail_columns)
        if ahead:
            inner_take(fore(ahead[1]), 1, is_edge)
            inner_take(fore(ahead[0]), 2)
            inner_take(aft(ahead[1]), 1, is_edge)
        last_share = lax.div(jnp.where(first, S - 1, 0) * Ds, Dt)
        afar = both(edge, last_share == t)
        if ahead:

            @pl.when(afar)
            def _(ahead=ahead):
                take(aft(ahead[1])[1:], 2)
                far_take(fore(ahead[0]))

        finish(layer)
        if ahead:
            after = layer + 1
            make_x(after)
            send_x(after)
            send_stat(2 * after)
            inner_take(aft(ahead[0]), 2)

            @pl.when(no(edge))
            def _(ahead=ahead):
                send_own(ahead[2])


            @pl.when(no(afar))
            def _(ahead=ahead):
                edge_take(aft(ahead[1])[1:], 2)
                far_take(fore(ahead[0]))

            far_take(aft(ahead[0]))
            inner_take(ahead[1], 2)
            if layer == 0:
                drain_start()
                drain(0, 0)
                drain(0, 1)
            far_take(ahead[1])
            relay_x(after)
            drain_stat(2 * layer + 1)
            drain_halo(layer)
            drain_sums(layer)
            wait_x(after)
            project(after, 0)
            project(after, 1)
            inner_take(fore(ahead[2]), 1, owned_inside)
            drain(layer, 2)
            if layer > 0:
                drain_x(layer)
                drain_stat(2 * layer)
                drain(layer, 0)
                drain(layer, 1)
            inner_take(aft(ahead[2]), 1, owned_inside)
            inner_take(ahead[2], 1, is_edge)
            project(after, 2)
            edge_take(fore(ahead[2]), 2)
            edge_take(aft(ahead[2])[:1], 2)
            for k in range(3, S):
                project(after, k)
            wait_stat(2 * after)
            gate(after)
            edge_take(aft(ahead[2])[1:], 2)
            if after + 1 < L:

                @pl.when(no(edge))
                def _(after=after):
                    send_own(groups[after + 1][0] + groups[after + 1][1])

            inner_take(fore(ahead[2]), 2)

    drain(L - 1, 2)
    drain_sums(L - 1)


def shards(hidden_in, in_gain, w_value, w_gate, conv_taps, norm_gain, norm_shift, w_out):
    S, T = lax.axis_size("sp"), lax.axis_size("tp")
    L, Ds, Cn = w_value.shape
    rows, Dt = hidden_in.shape
    chips = T // 2
    halo = (conv_taps.shape[1] - 1 + 15) // 16 * 16
    items = sum(sum(cuts(Ds, layer)) for layer in range(L))
    Q = 2 * cuts(Ds, 0)[2]
    fine = Q if S == T else 1
    vmem = pl.BlockSpec(memory_space=pltpu.VMEM)
    hbm = pl.BlockSpec(memory_space=pl.ANY)
    dma = pltpu.SemaphoreType.DMA
    return pl.pallas_call(
        functools.partial(kernel, S, T),
        out_shape=jax.ShapeDtypeStruct((rows, Dt), BF16),
        in_specs=[vmem, vmem, hbm, hbm, vmem, vmem, vmem, hbm],
        out_specs=vmem,
        scratch_shapes=[
            pltpu.VMEM((L, S, Ds, Cn), BF16),
            pltpu.VMEM((L, S, Ds, Cn), BF16),
            pltpu.VMEM((L, S, Q, Cn, Ds // Q), BF16),
            pltpu.VMEM((L, T, rows, Dt), BF16),
            pltpu.VMEM((T, rows, Dt), BF16),
            pltpu.VMEM((2, rows, Cn), F32),
            pltpu.VMEM((2, rows, Cn), F32),
            pltpu.VMEM((L, halo + 2 * rows, Cn), BF16),
            pltpu.VMEM((rows, Cn), F32),
            pltpu.VMEM((rows, Cn), BF16),
            pltpu.VMEM((L, T, rows, Dt), BF16),
            pltpu.VMEM((L, chips, rows, Dt), BF16),
            pltpu.VMEM((L, chips, rows, Dt), BF16),
            pltpu.VMEM((L, chips, rows, Dt), BF16),
            pltpu.VMEM((2 * L, T, 8, rows), F32),
            pltpu.VMEM((T, 8, rows), F32),
            pltpu.VMEM((rows, Dt), BF16),
            dma((L, 3)),
            dma((items, S)), dma((L, 3, S)), dma((L, 3, 2)), dma((items, S)), dma((L, 3, S)),
            dma((L + 1, T)), dma((L + 1, chips)), dma((L + 1, chips)),
            dma((2 * L, T)), dma((2 * L,)),
            dma((T,)), dma((1,)),
            dma((L,)), dma((L,)),
            dma((rows // CHUNK,)), dma((rows // CHUNK,)),
            dma((L, chips, 1, fine)), dma((L, chips)),
            dma((L, chips, 1, fine)), dma((L, chips)),
        ],
        compiler_params=pltpu.CompilerParams(
            collective_id=0, has_side_effects=True, vmem_limit_bytes=64_000_000
        ),
    )(hidden_in, in_gain, w_value, w_gate, jnp.swapaxes(conv_taps, 0, 1), norm_gain, norm_shift, w_out)


def solution(mesh):
    placed = (
        P(("grp", "sp"), "tp"),
        P(None, "tp"),
        P(None, "sp", "tp"),
        P(None, "sp", "tp"),
        P(None, None, "tp"),
        P(None, "tp"),
        P(None, "tp"),
        P(None, "tp", "sp"),
    )
    return jax.shard_map(
        shards, mesh=mesh, in_specs=placed, out_specs=P(("grp", "sp"), "tp"), check_vma=False
    )
```

```python
import functools

import jax
import jax.numpy as jnp
from jax import lax
from jax.experimental import pallas as pl
from jax.experimental.pallas import tpu as pltpu
from jax.sharding import PartitionSpec as P

epsilon = 1e-06
CHUNK = 128
F32, BF16 = jnp.float32, jnp.bfloat16


def cuts(Ds, layer):
    if Ds < 512:
        return (1, 1, 1)
    return (2, 2, 2) if layer == 0 else (2, 4, 4)


def kernel(
    S, T, h_ref, gain_ref, wv_ref, wg_ref, taps_ref, ng_ref, ns_ref, wo_ref, out_ref,
    WV, WG, WO, X, XG, ACC, GACC, EXT, CONV, MIX, PART, PRECV, SUMB, RECV, STAT, GSTAT, HB,
    own_sem, zr, zs, zo, yr, ys, xr, xs, xf, sr, ss, gr, gs, hr, hs, br, bs,
    pr, ps, rr, rs,
):
    L = wv_ref.shape[0]
    Ds, Cn = wv_ref.shape[1], wv_ref.shape[2]
    rows, Dt = h_ref.shape
    taps = taps_ref.shape[0]
    features, channels = Dt * T, Cn * T
    chips = T // 2
    Q, Dq = WO.shape[2], WO.shape[4]
    halo = EXT.shape[1] - 2 * rows
    g, me, t = lax.axis_index("grp"), lax.axis_index("sp"), lax.axis_index("tp")
    core = lax.rem(t, 2)
    chip = lax.div(t, 2)
    partner = t + 1 - 2 * core
    MESH = pl.DeviceIdType.MESH
    both, either, no = jnp.logical_and, jnp.logical_or, jnp.logical_not
    first, last = me == 0, me == S - 1
    low, high = me == 1, me == S - 2
    edge, near = either(first, last), either(low, high)
    inward = jnp.where(first, 1, -1)
    outward = jnp.where(low, -1, 1)
    own_base = jnp.where(low, rows, 0)
    guest_base = jnp.where(low, 0, rows)

    def is_edge(plane):
        return either(plane == 0, plane == S - 1)

    table = []
    groups = []
    for layer in range(L):
        of_layer = []
        for which in range(3):
            ids = []
            for piece in range(cuts(Ds, layer)[which]):
                ids.append(len(table))
                table.append((layer, which, piece, cuts(Ds, layer)[which]))
            of_layer.append(ids)
        groups.append(of_layer)
    items = len(table)

    def fore(ids):
        return ids[: (len(ids) + 1) // 2]

    def aft(ids):
        return ids[(len(ids) + 1) // 2 :]

    def direct(item):
        _, which, piece, pieces = table[item]
        return which != 1 or 2 * piece < pieces

    def folded(item):
        layer, which, _, _ = table[item]
        return layer == 0 and which < 2

    def inside(item, plane):
        low_end, high_end = (1, S - 2) if folded(item) else (0, S - 1)
        return both(plane >= low_end, plane <= high_end)

    def skips_y(item, owner):
        if not direct(item):
            return jnp.bool_(False)
        return either(both(owner == 0, low), both(owner == S - 1, high))

    sources = [(wv_ref, WV), (wg_ref, WG), (wo_ref, WO)]

    def own(layer, which):
        source, slots = sources[which]
        if which < 2:
            return [pltpu.make_async_copy(source.at[layer], slots.at[layer, me], own_sem.at[layer, which])]
        return [
            pltpu.make_async_copy(
                source.at[layer, :, pl.ds(q * Dq, Dq)], slots.at[layer, me, q], own_sem.at[layer, 2]
            )
            for q in range(Q)
        ]

    def own_start(layer, which):
        for copy in own(layer, which):
            copy.start()

    own_start(0, 0)
    own_start(0, 1)

    def own_wait(layer, which):
        slot = sources[which][1].at[layer, me]
        pltpu.make_async_copy(slot, slot, own_sem.at[layer, which]).wait()

    def each_chunk(body, start=0, count=rows):
        def step(index, _):
            body(pl.ds(pl.multiple_of(index * CHUNK, CHUNK), CHUNK))
            return 0

        lax.fori_loop(start // CHUNK, (start + count) // CHUNK, step, 0)

    def parts_of(layer):
        return [(0, rows)]

    def put_stat(slot, where, left, right):
        lane = lax.broadcasted_iota(jnp.int32, (left.shape[0], 128), 1)
        wide = jnp.where(lane == 0, left, right)
        STAT[slot, t, :, where] = wide.T[:8]

    def stat_ref(slot, source, part):
        if slot % 2 == 0:
            return STAT.at[slot, source]
        start, count = parts_of(slot // 2)[part]
        return STAT.at[slot, source, :, pl.ds(start, count)]

    def stat_sem(slot, part):
        return 2 * L + slot // 2 if part else slot

    def stat_copy(slot, peer, part):
        at = stat_sem(slot, part)
        return pltpu.make_async_remote_copy(
            stat_ref(slot, t, part), stat_ref(slot, t, part), ss.at[at], sr.at[at, t],
            device_id={"tp": peer}, device_id_type=MESH,
        )

    def stat_arrival(slot, peer, part):
        at = stat_sem(slot, part)
        return pltpu.make_async_remote_copy(
            stat_ref(slot, peer, part), stat_ref(slot, peer, part), ss.at[at], sr.at[at, peer],
            device_id={"tp": peer}, device_id_type=MESH,
        )

    def send_stat(slot, part=0):
        for shift in range(1, T):
            stat_copy(slot, lax.rem(t + shift, T), part).start()

    def wait_stat(slot, part=0):
        for shift in range(1, T):
            stat_arrival(slot, lax.rem(t + shift, T), part).wait_recv()

    def total_stat(stat, where):
        total = stat[0, :, where]
        for peer in range(1, T):
            total = total + stat[peer, :, where]
        return jnp.concatenate([total] * 16, axis=0).T

    def part_ref(item, owner, half):
        layer, which, piece, pieces = table[item]
        slots = sources[which][1]
        if which == 2:
            split = 2 * pieces // Q
            size = Cn // split
            return slots.at[layer, owner, half * (Q // 2) + piece // split, pl.ds(piece % split * size, size)]
        size = slots.shape[2] // (2 * pieces)
        start = pl.multiple_of(half * (size * pieces) + piece * size, size)
        return slots.at[layer, owner, pl.ds(start, size)]

    def zcopy(item, owner, way):
        ref = part_ref(item, owner, g)
        layer, which, _, _ = table[item]
        return pltpu.make_async_remote_copy(
            ref, ref, zs.at[layer, which, owner], zr.at[item, owner],
            device_id={"sp": me + way}, device_id_type=MESH,
        )

    def zown(item, way):
        ref = part_ref(item, me, g)
        layer, which, _, _ = table[item]
        return pltpu.make_async_remote_copy(
            ref, ref, zo.at[layer, which, (way + 1) // 2], zr.at[item, me],
            device_id={"sp": me + way}, device_id_type=MESH,
        )

    def dcopy(item, owner):
        ref = part_ref(item, owner, 1 - g)
        layer, which, _, _ = table[item]
        return pltpu.make_async_remote_copy(
            ref, ref, ys.at[layer, which, owner], yr.at[item, owner],
            device_id={"sp": me + inward}, device_id_type=MESH,
        )

    def ycopy(item, owner):
        ref = part_ref(item, owner, g)
        return pltpu.make_async_remote_copy(
            ref, ref, ys.at[table[item][0], table[item][1], owner], yr.at[item, owner],
            device_id={"grp": 1 - g}, device_id_type=MESH,
        )

    def yarrival(item, owner):
        ref = part_ref(item, owner, 1 - g)
        return pltpu.make_async_remote_copy(
            ref, ref, ys.at[table[item][0], table[item][1], owner], yr.at[item, owner],
            device_id={"grp": 1 - g}, device_id_type=MESH,
        )

    def outgoing(way):
        return low if way < 0 else high

    def send_out(ids):
        for item in ids:
            for way in (1, -1):

                @pl.when(outgoing(way))
                def _(item=item, way=way):
                    zown(item, way).start()

    def send_own(ids):
        for item in ids:
            for way in (1, -1):
                allowed = inside(item, me + way)
                if not folded(item):
                    allowed = both(allowed, no(outgoing(way)))

                @pl.when(allowed)
                def _(item=item, way=way):
                    zown(item, way).start()

    def send_direct(ids):
        for item in ids:
            if direct(item):
                dcopy(item, me).start()

    def take(ids, k, select=None):
        for item in ids:
            for way in (1, -1):
                owner = me - way * k
                ok = both(both(owner >= 0, owner < S), inside(item, me))
                if select is not None:
                    ok = both(ok, select(owner))

                @pl.when(ok)
                def _(item=item, way=way, owner=owner):
                    zcopy(item, owner, way).wait_recv()

                    @pl.when(inside(item, me + way))
                    def _():
                        zcopy(item, owner, way).start()

                    @pl.when(no(skips_y(item, owner)))
                    def _():
                        ycopy(item, owner).start()

    def arrive(ids, owner):
        for item in ids:
            yarrival(item, owner).wait_recv()

    def x_ref(slot, source):
        return XG.at[source] if slot == L else X.at[slot, source]

    def xcopy(slot, source, peer, sem):
        return pltpu.make_async_remote_copy(
            x_ref(slot, source), x_ref(slot, source), sem, xr.at[slot, source],
            device_id={"tp": peer}, device_id_type=MESH,
        )

    def make_x(layer):
        source = h_ref if layer == 0 else HB

        def body(where):
            wide = source[where, :].astype(F32)
            X[layer, t, where, :] = (wide * gain_ref[layer : layer + 1, :]).astype(BF16)
            squares = jnp.sum(wide * wide, axis=1, keepdims=True)
            put_stat(2 * layer, where, squares, squares)

        each_chunk(body)

    def send_x(slot):
        for shift in range(1, chips):
            peer = lax.rem(chip + shift, chips) * 2 + core
            xcopy(slot, t, peer, xs.at[slot, shift]).start()
        xcopy(slot, t, partner, xs.at[slot, 0]).start()

    def relay_x(slot):
        for shift in range(1, chips):
            source = lax.rem(chip + shift, chips) * 2 + core
            xcopy(slot, source, partner, xf.at[slot, shift]).wait_recv()
            xcopy(slot, source, partner, xf.at[slot, shift]).start()

    def wait_x(slot):
        for shift in range(chips):
            source = lax.rem(chip + shift, chips) * 2 + 1 - core
            xcopy(slot, source, partner, xf.at[slot, 0]).wait_recv()

    def guest_x_copy():
        return pltpu.make_async_remote_copy(
            X.at[0, t], XG.at[t], xs.at[L, 0], xr.at[L, t],
            device_id={"sp": me + inward}, device_id_type=MESH,
        )

    def guest_stat_copy():
        return pltpu.make_async_remote_copy(
            STAT.at[0, t], GSTAT.at[t], gs.at[0], gr.at[t],
            device_id={"sp": me + inward}, device_id_type=MESH,
        )

    def guest_stat_pass(source, peer):
        return pltpu.make_async_remote_copy(
            GSTAT.at[source], GSTAT.at[source], gs.at[0], gr.at[source],
            device_id={"tp": peer}, device_id_type=MESH,
        )

    def guest_back(index):
        start = pl.multiple_of(index * CHUNK + halo, 16)
        return pltpu.make_async_remote_copy(
            EXT.at[0, pl.ds(pl.multiple_of(guest_base + start, 16), CHUNK)],
            EXT.at[0, pl.ds(start, CHUNK)],
            bs.at[index], br.at[index],
            device_id={"sp": me + outward}, device_id_type=MESH,
        )

    def at_distance(k, body, select=None):
        if k == 0:
            if select is None:
                body(me)
            else:
                pl.when(select(me))(lambda: body(me))
            return

        def step(index, _):
            owner = me + k - 2 * k * index
            ok = both(owner >= 0, owner < S)
            if select is not None:
                ok = both(ok, select(owner))

            @pl.when(ok)
            def _():
                body(owner)

            return 0

        lax.fori_loop(0, 2, step, 0)

    def multiply(total, x, layer, owner, start):
        at = lax.div(owner * Ds, Dt)
        columns = pl.ds(pl.multiple_of(lax.rem(owner * Ds, Dt), 128), Ds)
        xs_block = x[at, :, columns]
        for which, slots in ((0, WV), (1, WG)):
            part = jnp.dot(xs_block, slots[layer, owner], preferred_element_type=F32)
            if start:
                total[which] = part
            else:
                total[which] += part

    def project(layer, k, select=None):
        def block(owner):
            if k > 0:
                arrive(groups[layer][0] + groups[layer][1], owner)
            multiply(ACC, X.at[layer], layer, owner, k == 0)

        at_distance(k, block, select)

    def halo_copy(layer):
        end = halo + rows + (own_base if layer == 0 else 0)
        return pltpu.make_async_remote_copy(
            EXT.at[layer, pl.ds(pl.multiple_of(end - halo, 16), halo)],
            EXT.at[layer, pl.ds(0, halo)],
            hs.at[layer], hr.at[layer],
            device_id={"sp": me + 1}, device_id_type=MESH,
        )

    def sends_halo(layer):
        return both(no(last), no(first)) if layer == 0 else no(last)

    def takes_halo(layer):
        return both(no(first), no(low)) if layer == 0 else no(first)

    def gate_rows(layer, total, stat, base, where):
        mean = total_stat(stat, where)[:, :1] / features
        inv = lax.rsqrt(mean + epsilon)
        value, gating = total[0, where, :] * inv, total[1, where, :] * inv
        gated = (value / (1.0 + jnp.exp(-gating))).astype(BF16)
        EXT[layer, pl.ds(pl.multiple_of(base + where.start + halo, 16), where.size), :] = gated

    def gate(layer):
        base = own_base if layer == 0 else 0
        each_chunk(functools.partial(gate_rows, layer, ACC, STAT.at[2 * layer], base))

        @pl.when(sends_halo(layer))
        def _():
            halo_copy(layer).start()

    def convolve(layer, part):
        def wait_halo():
            @pl.when(first)
            def _():
                EXT[layer, pl.ds(0, halo), :] = jnp.zeros((halo, Cn), BF16)

            @pl.when(takes_halo(layer))
            def _():
                halo_copy(layer).wait_recv()

        tall = CHUNK + halo + 8
        offset = halo - (taps - 1)
        base = own_base if layer == 0 else 0

        def body(where):
            if layer == 0:

                @pl.when(edge)
                def _():
                    guest_back(lax.div(where.start, CHUNK)).wait_recv()

            for column in range(0, Cn, 128):
                at = pl.ds(column, 128)
                window = EXT[layer, pl.ds(pl.multiple_of(base + where.start, 16), CHUNK + halo), at]
                tile = jnp.concatenate([window.astype(F32), jnp.zeros((8, 128), F32)], axis=0)
                total = jnp.zeros((CHUNK, 128), F32)
                for residue in range(8):
                    ks = [k for k in range(taps) if (k + offset) % 8 == residue]
                    if not ks:
                        continue
                    turned = pltpu.roll(tile, tall - residue, 0) if residue else tile
                    for k in ks:
                        low_row = k + offset - residue
                        total = total + taps_ref[k, layer : layer + 1, at] * turned[low_row : low_row + CHUNK]
                CONV[where, at] = total
            conved = CONV[where, :]
            put_stat(
                2 * layer + 1, where,
                jnp.sum(conved, axis=1, keepdims=True),
                jnp.sum(conved * conved, axis=1, keepdims=True),
            )

        if layer == 0:
            wait_halo()
            each_chunk(body)
        else:
            each_chunk(body, CHUNK, rows - CHUNK)
            wait_halo()
            each_chunk(body, 0, CHUNK)
        send_stat(2 * layer + 1, part)

    def mix(layer, part):
        start, count = parts_of(layer)[part]
        wait_stat(2 * layer + 1, part)

        def body(where):
            stat = total_stat(STAT.at[2 * layer + 1], where)
            mean = stat[:, 0:1] / channels
            spread = stat[:, 1:2] / channels - mean * mean
            normed = (CONV[where, :] - mean) * lax.rsqrt(spread + epsilon) * ng_ref[
                layer : layer + 1, :
            ] + ns_ref[layer : layer + 1, :]
            MIX[where, :] = (normed / (1.0 + jnp.exp(-normed))).astype(BF16)

        each_chunk(body, start, count)

    fine = Q if S == T else 1
    width = Dt // fine

    def cut(layer, ref, q, part):
        start, count = parts_of(layer)[part]
        return ref.at[pl.ds(start, count), columns_of(q)]

    def columns_of(q):
        return pl.ds(0, width) if fine == 1 else pl.ds(pl.multiple_of(q * width, 128), width)

    def pair_copy(layer, at, q, part):
        return pltpu.make_async_remote_copy(
            cut(layer, PART.at[layer, 2 * at + 1 - core], q, part), cut(layer, PRECV.at[layer, at], q, part),
            ps.at[layer, at], pr.at[layer, at, part, q],
            device_id={"tp": partner}, device_id_type=MESH,
        )

    def sum_copy(layer, at, q, part):
        return pltpu.make_async_remote_copy(
            cut(layer, SUMB.at[layer, at], q, part), cut(layer, RECV.at[layer, chip], q, part),
            rs.at[layer, at], rr.at[layer, chip, part, q],
            device_id={"tp": at * 2 + core}, device_id_type=MESH,
        )

    def sum_arrival(layer, at, q, part):
        return pltpu.make_async_remote_copy(
            cut(layer, SUMB.at[layer, at], q, part), cut(layer, RECV.at[layer, at], q, part),
            rs.at[layer, at], rr.at[layer, at, part, q],
            device_id={"tp": at * 2 + core}, device_id_type=MESH,
        )

    def sum_pair(layer, at, q, part):
        pair_copy(layer, at, q, part).wait_recv()
        columns = columns_of(q)

        def body(where):
            SUMB[layer, at, where, columns] = (
                PART[layer, at * 2 + core, where, columns].astype(F32)
                + PRECV[layer, at, where, columns].astype(F32)
            ).astype(BF16)

        each_chunk(body, *parts_of(layer)[part])
        sum_copy(layer, at, q, part).start()

    def turn_order():
        count = Q // 2
        return [(False, g * count + piece, piece) for piece in range(count)] + [
            (True, (1 - g) * count + piece, piece) for piece in range(count)
        ]

    def branch(layer, k, parts, early=True, late=True, wait=True, only=None, select=None, together=False):
        def block(owner):
            target = lax.div(owner * Ds, Dt)
            base = lax.rem(owner * Ds, Dt)
            at = lax.div(target, 2)

            def product(q, part):
                start, count = parts_of(layer)[part]
                columns = pl.ds(pl.multiple_of(base + q * Dq, 128), Dq)
                PART[layer, target, pl.ds(start, count), columns] = jnp.dot(
                    MIX[pl.ds(start, count), :], WO[layer, owner, q], preferred_element_type=F32
                ).astype(BF16)
                if S == T:

                    @pl.when(lax.rem(target, 2) != core)
                    def _():
                        pair_copy(layer, at, q, part).start()

            def total(q, part):
                if S == T:

                    @pl.when(both(lax.rem(target, 2) == core, at != chip))
                    def _():
                        sum_pair(layer, at, q, part)

            order = [o for o in turn_order() if only is None or o[2] in only]
            group = order if k == 0 or together else [o for o in order if not o[0]]
            if together and k > 0:
                arrive(groups[layer][2], owner)
            if early:
                for part in parts:
                    for _, q, _ in group:
                        product(q, part)
                    for _, q, _ in group:
                        total(q, part)
            if k > 0 and late:
                for _, q, piece in order[len(group) :]:
                    if wait:
                        ids = groups[layer][2]
                        split = 2 * len(ids) // Q
                        arrive(ids[piece * split : (piece + 1) * split], owner)
                    for part in parts:
                        product(q, part)
                    for part in parts:
                        total(q, part)

        at_distance(k, block, select)

    def stays(owner):
        return lax.div(owner * Ds, 2 * Dt) == chip

    def leaves(owner):
        return no(stays(owner))

    def share(layer):
        if S != T:
            for part in range(len(parts_of(layer))):
                for shift in list(range(1, chips)) + [0]:
                    pair_copy(layer, lax.rem(chip + shift, chips), 0, part).start()
                for shift in range(1, chips):
                    sum_pair(layer, lax.rem(chip + shift, chips), 0, part)

    def finish(layer):
        share(layer)
        source = h_ref if layer == 0 else HB
        target = out_ref if layer == L - 1 else HB
        for part, (start, count) in enumerate(parts_of(layer)):
            for q in [q for _, q, _ in turn_order()] if fine > 1 else [0]:
                pair_copy(layer, chip, q, part).wait_recv()
                for shift in range(1, chips):
                    sum_arrival(layer, lax.rem(chip + shift, chips), q, part).wait_recv()
                columns = columns_of(q)

                def body(where, columns=columns):
                    total = PART[layer, t, where, columns].astype(F32) + PRECV[
                        layer, chip, where, columns
                    ].astype(F32)
                    for shift in range(1, chips):
                        total = total + RECV[layer, lax.rem(chip + shift, chips), where, columns].astype(F32)
                    target[where, columns] = (source[where, columns].astype(F32) + total).astype(BF16)

                each_chunk(body, start, count)

    def sent(ref, sem):
        pltpu.make_async_remote_copy(
            ref, ref, sem, zr.at[0, 0], device_id={"tp": partner}, device_id_type=MESH
        ).wait_send()

    def half_ref(layer, which, owner, half):
        slots = sources[which][1]
        size = slots.shape[2] // 2
        return slots.at[layer, owner, pl.ds(pl.multiple_of(half * size, size), size)]

    def some_ref(layer, which, owner, half, begin, count, pieces):
        if count == pieces:
            return half_ref(layer, which, owner, half)
        slots = sources[which][1]
        size = slots.shape[2] // (2 * pieces)
        start = pl.multiple_of(half * (size * pieces) + begin * size, size)
        return slots.at[layer, owner, pl.ds(start, size * count)]

    def drain(layer, which):
        ids = groups[layer][which]
        whole = [item for item in ids if direct(item)]
        for way in (1, -1):

            @pl.when(inside(ids[0], me + way))
            def _(way=way):
                sent(half_ref(layer, which, me, g), zo.at[layer, which, (way + 1) // 2])

        @pl.when(edge)
        def _():
            sent(some_ref(layer, which, me, 1 - g, 0, len(whole), len(ids)), ys.at[layer, which, me])

        def settle(owner, _):
            @pl.when(both(owner != me, inside(ids[0], me)))
            def _():
                @pl.when(inside(ids[0], jnp.where(owner < me, me + 1, me - 1)))
                def _():
                    sent(half_ref(layer, which, owner, g), zs.at[layer, which, owner])

                skip = skips_y(whole[0], owner)

                @pl.when(no(skip))
                def _():
                    sent(half_ref(layer, which, owner, g), ys.at[layer, which, owner])

                if len(whole) < len(ids):

                    @pl.when(skip)
                    def _():
                        sent(
                            some_ref(layer, which, owner, g, len(whole), len(ids) - len(whole), len(ids)),
                            ys.at[layer, which, owner],
                        )

            return 0

        lax.fori_loop(0, S, settle, 0)

    def drain_x(slot):
        for shift in range(chips):
            xcopy(slot, t, partner, xs.at[slot, shift]).wait_send()
        for shift in range(1, chips):
            xcopy(slot, t, partner, xf.at[slot, shift]).wait_send()

    def drain_stat(slot):
        if slot % 2 == 0:
            sent(STAT.at[slot, pl.ds(0, T - 1)], ss.at[slot])
            return
        for part, (start, count) in enumerate(parts_of(slot // 2)):
            sent(STAT.at[slot, pl.ds(0, T - 1), :, pl.ds(start, count)], ss.at[stat_sem(slot, part)])

    def drain_start():
        @pl.when(edge)
        def _():
            guest_x_copy().wait_send()
            guest_stat_copy().wait_send()

        @pl.when(no(edge))
        def _():
            drain_x(0)
            drain_stat(0)

        @pl.when(near)
        def _():
            drain_x(L)
            sent(GSTAT.at[pl.ds(0, T - 1)], gs.at[0])
            for index in range(rows // CHUNK):
                guest_back(index).wait_send()

    def drain_sums(layer):
        for shift in range(chips):
            at = lax.rem(chip + shift, chips)
            sent(PRECV.at[layer, at], ps.at[layer, at])
        for shift in range(1, chips):
            at = lax.rem(chip + shift, chips)
            sent(SUMB.at[layer, at], rs.at[layer, at])

    def drain_halo(layer):
        @pl.when(sends_halo(layer))
        def _():
            halo_copy(layer).wait_send()

    barrier = pltpu.get_barrier_semaphore()
    for shift in range(1, T):
        pl.semaphore_signal(barrier, inc=1, device_id={"tp": lax.rem(t + shift, T)}, device_id_type=MESH)
    pl.semaphore_signal(barrier, inc=1, device_id={"grp": 1 - g}, device_id_type=MESH)

    @pl.when(no(first))
    def _():
        pl.semaphore_signal(barrier, inc=1, device_id={"sp": me - 1}, device_id_type=MESH)

    @pl.when(no(last))
    def _():
        pl.semaphore_signal(barrier, inc=1, device_id={"sp": me + 1}, device_id_type=MESH)

    inner = jnp.where(first, 0, 1) + jnp.where(last, 0, 1)
    pl.semaphore_wait(barrier, T + inner)

    value0, gating0, out0 = groups[0]
    for which in range(2):
        own_wait(0, which)
        send_own(groups[0][which])
    rest = [(0, 2)] + [(layer, which) for layer in range(1, L) for which in range(3)]
    for layer, which in rest:
        own_start(layer, which)
    for layer, which in rest:
        own_wait(layer, which)
        send_out(groups[layer][which])
    make_x(0)

    def owned_inside(owner):
        return no(is_edge(owner))

    def inner_take(ids, k, select=None):
        @pl.when(no(edge))
        def _():
            take(ids, k, select)

    def edge_take(ids, k):
        @pl.when(edge)
        def _():
            take(ids, k)

    def far_take(ids):
        for k in range(3, S):
            take(ids, k)

    @pl.when(edge)
    def _():
        guest_x_copy().start()
        guest_stat_copy().start()
        send_direct(value0 + gating0)
        send_own(out0)
        send_direct(out0)
        for layer in range(1, L):
            send_own(groups[layer][0] + groups[layer][1])
            send_direct(groups[layer][0] + groups[layer][1])
            send_own(groups[layer][2])
            send_direct(groups[layer][2])
        take(out0, 1)
        for layer in range(1, L):
            for which in range(3):
                take(groups[layer][which], 1)
        take(out0, 2)
        if L > 1:
            take(fore(groups[1][0]), 2)

    @pl.when(no(edge))
    def _():
        send_x(0)
        send_stat(0)
        take(value0 + gating0, 1)
        send_own(out0)
        relay_x(0)
        wait_x(0)
        project(0, 0)
        for k in range(2, S - 1):
            take(value0, k)
            if k == 2:

                @pl.when(near)
                def _():
                    xcopy(L, t, partner, xf.at[L, 0]).wait_recv()
                    guest_stat_pass(t, partner).wait_recv()
                    send_x(L)
                    for shift in range(1, T):
                        guest_stat_pass(t, lax.rem(t + shift, T)).start()

            take(gating0, k)
            if k == 2 and L > 1:
                send_own(groups[1][0])
            project(0, k - 1, lambda owner: no(skips_y(value0[0], owner)))
        take(out0, 1, owned_inside)

        @pl.when(near)
        def _():
            relay_x(L)
            wait_x(L)
            for shift in range(1, T):
                guest_stat_pass(lax.rem(t + shift, T), partner).wait_recv()

        if L > 1:
            take(fore(groups[1][0]), 1, owned_inside)
        take(fore(out0), 1, is_edge)
        project(0, S - 2)
        wait_stat(0)

        @pl.when(near)
        def _():
            corner = jnp.where(low, 0, S - 1)
            arrive(value0 + gating0, corner)
            multiply(ACC, X.at[0], 0, corner, False)
            multiply(GACC, XG, 0, me, True)

            def add(index, _):
                owner = lax.rem(me + index, S)
                multiply(GACC, XG, 0, owner, False)
                return 0

            lax.fori_loop(1, S, add, 0)

            def back(where):
                gate_rows(0, GACC, GSTAT, guest_base, where)
                guest_back(lax.div(where.start, CHUNK)).start()

            each_chunk(back)

        gate(0)
        take(aft(out0), 1, is_edge)
        if L > 1:
            send_own(groups[1][1])
            take(aft(groups[1][0]), 1, owned_inside)

    for layer in range(L):
        out = groups[layer][2]
        ahead = groups[layer + 1] if layer + 1 < L else None
        every = list(range(len(parts_of(layer))))
        columns = list(range(Q // 2))
        head_columns, tail_columns = columns[: Q // 4], columns[Q // 4 :]
        if ahead and layer > 0:
            inner_take(ahead[0], 1, owned_inside)
            edge_take(fore(ahead[0]), 2)
        if layer == 0:
            convolve(0, 0)
            inner_take(fore(out), 2)
            mix(0, 0)
            inner_take(aft(out), 2)
        else:
            inner_take(aft(out), 2)
            convolve(layer, 0)
            far_take(fore(out))
            mix(layer, 0)
            for k in range(3):
                branch(layer, k, every, late=False, select=leaves)
            for k in range(3, S):
                branch(layer, k, every, late=False, only=head_columns, select=leaves)
            far_take(aft(out)[:1])
            for k in range(1, 3):
                branch(layer, k, every, early=False, select=leaves)
            far_take(aft(out)[1:])
            for k in range(3):
                branch(layer, k, every, select=stays, together=True)
            for k in range(3, S):
                branch(layer, k, every, late=False, only=head_columns, select=stays)
        if ahead:
            edge_take(aft(ahead[0]), 2)
        if layer == 0:
            branch(layer, 0, [0])
            branch(layer, 1, [0])
            far_take(fore(out))
            if ahead:
                inner_take(fore(ahead[1]), 1, owned_inside)
                inner_take(fore(ahead[0]), 1, is_edge)
            branch(layer, 2, [0], late=False)
            if ahead:
                inner_take(aft(ahead[0]), 1, is_edge)
                inner_take(aft(ahead[1]), 1, owned_inside)
            branch(layer, 2, [0], early=False)
        else:
            for k in range(3, S):
                branch(layer, k, every, early=False, only=head_columns)
                branch(layer, k, every, late=False, only=tail_columns)
            if ahead:
                inner_take(fore(ahead[1]), 1, owned_inside)
                inner_take(ahead[0], 1, is_edge)
                inner_take(aft(ahead[1]), 1, owned_inside)
        if ahead is None:
            drain_stat(2 * layer + 1)
            drain_halo(layer)
            if layer > 0:
                drain_x(layer)
                drain_stat(2 * layer)
                drain(layer, 0)
                drain(layer, 1)
        if layer == 0:
            far_take(aft(out))
        for k in range(3, S) if layer == 0 else []:
            branch(layer, k, every, late=False)
        if ahead:
            edge_take(fore(ahead[1]), 2)
            for k in range(3, S):
                branch(layer, k, every, early=False, only=head_columns)
            edge_take(aft(ahead[1])[:1], 2)
            for k in range(3, S):
                branch(layer, k, every, early=False, only=tail_columns)
        else:
            for k in range(3, S):
                branch(layer, k, every, early=False, only=tail_columns)
        if ahead:
            inner_take(fore(ahead[1]), 1, is_edge)
            inner_take(fore(ahead[0]), 2)
            inner_take(aft(ahead[1]), 1, is_edge)
        last_share = lax.div(jnp.where(first, S - 1, 0) * Ds, Dt)
        afar = both(edge, last_share == t)
        if ahead:

            @pl.when(afar)
            def _(ahead=ahead):
                take(aft(ahead[1])[1:], 2)
                far_take(fore(ahead[0]))

        finish(layer)
        if ahead:
            after = layer + 1
            make_x(after)
            send_x(after)
            send_stat(2 * after)
            inner_take(aft(ahead[0]), 2)

            @pl.when(no(edge))
            def _(ahead=ahead):
                send_own(ahead[2])


            @pl.when(no(afar))
            def _(ahead=ahead):
                edge_take(aft(ahead[1])[1:], 2)
                far_take(fore(ahead[0]))

            far_take(aft(ahead[0]))
            inner_take(ahead[1], 2)
            if layer == 0:
                drain_start()
                drain(0, 0)
                drain(0, 1)
            far_take(ahead[1])
            relay_x(after)
            drain_stat(2 * layer + 1)
            drain_halo(layer)
            drain_sums(layer)
            wait_x(after)
            project(after, 0)
            project(after, 1)
            inner_take(fore(ahead[2]), 1, owned_inside)
            drain(layer, 2)
            if layer > 0:
                drain_x(layer)
                drain_stat(2 * layer)
                drain(layer, 0)
                drain(layer, 1)
            inner_take(aft(ahead[2]), 1, owned_inside)
            inner_take(ahead[2], 1, is_edge)
            project(after, 2)
            edge_take(fore(ahead[2]), 2)
            edge_take(aft(ahead[2])[:1], 2)
            for k in range(3, S):
                project(after, k)
            wait_stat(2 * after)
            gate(after)
            edge_take(aft(ahead[2])[1:], 2)
            if after + 1 < L:

                @pl.when(no(edge))
                def _(after=after):
                    send_own(groups[after + 1][0] + groups[after + 1][1])

            inner_take(fore(ahead[2]), 2)

    drain(L - 1, 2)
    drain_sums(L - 1)


def shards(hidden_in, in_gain, w_value, w_gate, conv_taps, norm_gain, norm_shift, w_out):
    S, T = lax.axis_size("sp"), lax.axis_size("tp")
    L, Ds, Cn = w_value.shape
    rows, Dt = hidden_in.shape
    chips = T // 2
    halo = (conv_taps.shape[1] - 1 + 15) // 16 * 16
    items = sum(sum(cuts(Ds, layer)) for layer in range(L))
    Q = 2 * cuts(Ds, 0)[2]
    fine = Q if S == T else 1
    vmem = pl.BlockSpec(memory_space=pltpu.VMEM)
    hbm = pl.BlockSpec(memory_space=pl.ANY)
    dma = pltpu.SemaphoreType.DMA
    return pl.pallas_call(
        functools.partial(kernel, S, T),
        out_shape=jax.ShapeDtypeStruct((rows, Dt), BF16),
        in_specs=[vmem, vmem, hbm, hbm, vmem, vmem, vmem, hbm],
        out_specs=vmem,
        scratch_shapes=[
            pltpu.VMEM((L, S, Ds, Cn), BF16),
            pltpu.VMEM((L, S, Ds, Cn), BF16),
            pltpu.VMEM((L, S, Q, Cn, Ds // Q), BF16),
            pltpu.VMEM((L, T, rows, Dt), BF16),
            pltpu.VMEM((T, rows, Dt), BF16),
            pltpu.VMEM((2, rows, Cn), F32),
            pltpu.VMEM((2, rows, Cn), F32),
            pltpu.VMEM((L, halo + 2 * rows, Cn), BF16),
            pltpu.VMEM((rows, Cn), F32),
            pltpu.VMEM((rows, Cn), BF16),
            pltpu.VMEM((L, T, rows, Dt), BF16),
            pltpu.VMEM((L, chips, rows, Dt), BF16),
            pltpu.VMEM((L, chips, rows, Dt), BF16),
            pltpu.VMEM((L, chips, rows, Dt), BF16),
            pltpu.VMEM((2 * L, T, 8, rows), F32),
            pltpu.VMEM((T, 8, rows), F32),
            pltpu.VMEM((rows, Dt), BF16),
            dma((L, 3)),
            dma((items, S)), dma((L, 3, S)), dma((L, 3, 2)), dma((items, S)), dma((L, 3, S)),
            dma((L + 1, T)), dma((L + 1, chips)), dma((L + 1, chips)),
            dma((2 * L, T)), dma((2 * L,)),
            dma((T,)), dma((1,)),
            dma((L,)), dma((L,)),
            dma((rows // CHUNK,)), dma((rows // CHUNK,)),
            dma((L, chips, 1, fine)), dma((L, chips)),
            dma((L, chips, 1, fine)), dma((L, chips)),
        ],
        compiler_params=pltpu.CompilerParams(
            collective_id=0, has_side_effects=True, vmem_limit_bytes=64_000_000
        ),
    )(hidden_in, in_gain, w_value, w_gate, jnp.swapaxes(conv_taps, 0, 1), norm_gain, norm_shift, w_out)


def solution(mesh):
    placed = (
        P(("grp", "sp"), "tp"),
        P(None, "tp"),
        P(None, "sp", "tp"),
        P(None, "sp", "tp"),
        P(None, None, "tp"),
        P(None, "tp"),
        P(None, "tp"),
        P(None, "tp", "sp"),
    )
    return jax.shard_map(
        shards, mesh=mesh, in_specs=placed, out_specs=P(("grp", "sp"), "tp"), check_vma=False
    )
```

```python
import functools

import jax
import jax.numpy as jnp
from jax import lax
from jax.experimental import pallas as pl
from jax.experimental.pallas import tpu as pltpu
from jax.sharding import PartitionSpec as P

epsilon = 1e-06
CHUNK = 128
F32, BF16 = jnp.float32, jnp.bfloat16


def cuts(Ds, layer):
    if Ds < 512:
        return (1, 1, 1)
    return (2, 2, 4) if layer == 0 else (4, 4, 4)


def kernel(
    S, T, h_ref, gain_ref, wv_ref, wg_ref, taps_ref, ng_ref, ns_ref, wo_ref, out_ref,
    WV, WG, WO, X, XG, ACC, GACC, EXT, CONV, MIX, PART, PRECV, SUMB, RECV, STAT, GSTAT, HB,
    own_sem, zr, zs, zo, yr, ys, xr, xs, xf, sr, ss, gr, gs, hr, hs, br, bs,
    pr, ps, rr, rs,
):
    L = wv_ref.shape[0]
    Ds, Cn = wv_ref.shape[1], wv_ref.shape[2]
    rows, Dt = h_ref.shape
    taps = taps_ref.shape[0]
    features, channels = Dt * T, Cn * T
    chips = T // 2
    Q, Dq = WO.shape[2], WO.shape[4]
    halo = EXT.shape[1] - 2 * rows
    g, me, t = lax.axis_index("grp"), lax.axis_index("sp"), lax.axis_index("tp")
    core = lax.rem(t, 2)
    chip = lax.div(t, 2)
    partner = t + 1 - 2 * core
    MESH = pl.DeviceIdType.MESH
    both, either, no = jnp.logical_and, jnp.logical_or, jnp.logical_not
    first, last = me == 0, me == S - 1
    low, high = me == 1, me == S - 2
    edge, near = either(first, last), either(low, high)
    inward = jnp.where(first, 1, -1)
    outward = jnp.where(low, -1, 1)
    own_base = jnp.where(low, rows, 0)
    guest_base = jnp.where(low, 0, rows)

    def is_edge(plane):
        return either(plane == 0, plane == S - 1)

    table = []
    groups = []
    for layer in range(L):
        of_layer = []
        for which in range(3):
            ids = []
            for piece in range(cuts(Ds, layer)[which]):
                ids.append(len(table))
                table.append((layer, which, piece, cuts(Ds, layer)[which]))
            of_layer.append(ids)
        groups.append(of_layer)
    items = len(table)

    def fore(ids):
        return ids[: (len(ids) + 1) // 2]

    def aft(ids):
        return ids[(len(ids) + 1) // 2 :]

    def direct(item):
        _, which, piece, pieces = table[item]
        return which != 1 or 2 * piece < pieces

    def folded(item):
        layer, which, _, _ = table[item]
        return layer == 0 and which < 2

    def inside(item, plane):
        low_end, high_end = (1, S - 2) if folded(item) else (0, S - 1)
        return both(plane >= low_end, plane <= high_end)

    def skips_y(item, owner):
        if not direct(item):
            return jnp.bool_(False)
        return either(both(owner == 0, low), both(owner == S - 1, high))

    sources = [(wv_ref, WV), (wg_ref, WG), (wo_ref, WO)]

    def own(layer, which):
        source, slots = sources[which]
        if which < 2:
            return [pltpu.make_async_copy(source.at[layer], slots.at[layer, me], own_sem.at[layer, which])]
        return [
            pltpu.make_async_copy(
                source.at[layer, :, pl.ds(q * Dq, Dq)], slots.at[layer, me, q], own_sem.at[layer, 2]
            )
            for q in range(Q)
        ]

    def own_start(layer, which):
        for copy in own(layer, which):
            copy.start()

    own_start(0, 0)
    own_start(0, 1)

    def own_wait(layer, which):
        slot = sources[which][1].at[layer, me]
        pltpu.make_async_copy(slot, slot, own_sem.at[layer, which]).wait()

    def each_chunk(body, start=0, count=rows):
        def step(index, _):
            body(pl.ds(pl.multiple_of(index * CHUNK, CHUNK), CHUNK))
            return 0

        lax.fori_loop(start // CHUNK, (start + count) // CHUNK, step, 0)

    def parts_of(layer):
        return [(0, rows)]

    def put_stat(slot, where, left, right):
        lane = lax.broadcasted_iota(jnp.int32, (left.shape[0], 128), 1)
        wide = jnp.where(lane == 0, left, right)
        STAT[slot, t, :, where] = wide.T[:8]

    def stat_ref(slot, source, part):
        if slot % 2 == 0:
            return STAT.at[slot, source]
        start, count = parts_of(slot // 2)[part]
        return STAT.at[slot, source, :, pl.ds(start, count)]

    def stat_sem(slot, part):
        return 2 * L + slot // 2 if part else slot

    def stat_copy(slot, peer, part):
        at = stat_sem(slot, part)
        return pltpu.make_async_remote_copy(
            stat_ref(slot, t, part), stat_ref(slot, t, part), ss.at[at], sr.at[at, t],
            device_id={"tp": peer}, device_id_type=MESH,
        )

    def stat_arrival(slot, peer, part):
        at = stat_sem(slot, part)
        return pltpu.make_async_remote_copy(
            stat_ref(slot, peer, part), stat_ref(slot, peer, part), ss.at[at], sr.at[at, peer],
            device_id={"tp": peer}, device_id_type=MESH,
        )

    def send_stat(slot, part=0):
        for shift in range(1, T):
            stat_copy(slot, lax.rem(t + shift, T), part).start()

    def wait_stat(slot, part=0):
        for shift in range(1, T):
            stat_arrival(slot, lax.rem(t + shift, T), part).wait_recv()

    def total_stat(stat, where):
        total = stat[0, :, where]
        for peer in range(1, T):
            total = total + stat[peer, :, where]
        return jnp.concatenate([total] * 16, axis=0).T

    def part_ref(item, owner, half):
        layer, which, piece, pieces = table[item]
        slots = sources[which][1]
        if which == 2:
            split = 2 * pieces // Q
            size = Cn // split
            return slots.at[layer, owner, half * (Q // 2) + piece // split, pl.ds(piece % split * size, size)]
        size = slots.shape[2] // (2 * pieces)
        start = pl.multiple_of(half * (size * pieces) + piece * size, size)
        return slots.at[layer, owner, pl.ds(start, size)]

    def zcopy(item, owner, way):
        ref = part_ref(item, owner, g)
        layer, which, _, _ = table[item]
        return pltpu.make_async_remote_copy(
            ref, ref, zs.at[layer, which, owner], zr.at[item, owner],
            device_id={"sp": me + way}, device_id_type=MESH,
        )

    def zown(item, way):
        ref = part_ref(item, me, g)
        layer, which, _, _ = table[item]
        return pltpu.make_async_remote_copy(
            ref, ref, zo.at[layer, which, (way + 1) // 2], zr.at[item, me],
            device_id={"sp": me + way}, device_id_type=MESH,
        )

    def dcopy(item, owner):
        ref = part_ref(item, owner, 1 - g)
        layer, which, _, _ = table[item]
        return pltpu.make_async_remote_copy(
            ref, ref, ys.at[layer, which, owner], yr.at[item, owner],
            device_id={"sp": me + inward}, device_id_type=MESH,
        )

    def ycopy(item, owner):
        ref = part_ref(item, owner, g)
        return pltpu.make_async_remote_copy(
            ref, ref, ys.at[table[item][0], table[item][1], owner], yr.at[item, owner],
            device_id={"grp": 1 - g}, device_id_type=MESH,
        )

    def yarrival(item, owner):
        ref = part_ref(item, owner, 1 - g)
        return pltpu.make_async_remote_copy(
            ref, ref, ys.at[table[item][0], table[item][1], owner], yr.at[item, owner],
            device_id={"grp": 1 - g}, device_id_type=MESH,
        )

    def outgoing(way):
        return low if way < 0 else high

    def send_out(ids):
        for item in ids:
            for way in (1, -1):

                @pl.when(outgoing(way))
                def _(item=item, way=way):
                    zown(item, way).start()

    def send_own(ids):
        for item in ids:
            for way in (1, -1):
                allowed = inside(item, me + way)
                if not folded(item):
                    allowed = both(allowed, no(outgoing(way)))

                @pl.when(allowed)
                def _(item=item, way=way):
                    zown(item, way).start()

    def send_direct(ids):
        for item in ids:
            if direct(item):
                dcopy(item, me).start()

    def take(ids, k, select=None):
        for item in ids:
            for way in (1, -1):
                owner = me - way * k
                ok = both(both(owner >= 0, owner < S), inside(item, me))
                if select is not None:
                    ok = both(ok, select(owner))

                @pl.when(ok)
                def _(item=item, way=way, owner=owner):
                    zcopy(item, owner, way).wait_recv()

                    @pl.when(inside(item, me + way))
                    def _():
                        zcopy(item, owner, way).start()

                    @pl.when(no(skips_y(item, owner)))
                    def _():
                        ycopy(item, owner).start()

    def arrive(ids, owner):
        for item in ids:
            yarrival(item, owner).wait_recv()

    def x_ref(slot, source):
        return XG.at[source] if slot == L else X.at[slot, source]

    def xcopy(slot, source, peer, sem):
        return pltpu.make_async_remote_copy(
            x_ref(slot, source), x_ref(slot, source), sem, xr.at[slot, source],
            device_id={"tp": peer}, device_id_type=MESH,
        )

    def make_x(layer):
        source = h_ref if layer == 0 else HB

        def body(where):
            wide = source[where, :].astype(F32)
            X[layer, t, where, :] = (wide * gain_ref[layer : layer + 1, :]).astype(BF16)
            squares = jnp.sum(wide * wide, axis=1, keepdims=True)
            put_stat(2 * layer, where, squares, squares)

        each_chunk(body)

    def send_x(slot):
        for shift in range(1, chips):
            peer = lax.rem(chip + shift, chips) * 2 + core
            xcopy(slot, t, peer, xs.at[slot, shift]).start()
        xcopy(slot, t, partner, xs.at[slot, 0]).start()

    def relay_x(slot):
        for shift in range(1, chips):
            source = lax.rem(chip + shift, chips) * 2 + core
            xcopy(slot, source, partner, xf.at[slot, shift]).wait_recv()
            xcopy(slot, source, partner, xf.at[slot, shift]).start()

    def wait_x(slot):
        for shift in range(chips):
            source = lax.rem(chip + shift, chips) * 2 + 1 - core
            xcopy(slot, source, partner, xf.at[slot, 0]).wait_recv()

    def guest_x_copy():
        return pltpu.make_async_remote_copy(
            X.at[0, t], XG.at[t], xs.at[L, 0], xr.at[L, t],
            device_id={"sp": me + inward}, device_id_type=MESH,
        )

    def guest_stat_copy():
        return pltpu.make_async_remote_copy(
            STAT.at[0, t], GSTAT.at[t], gs.at[0], gr.at[t],
            device_id={"sp": me + inward}, device_id_type=MESH,
        )

    def guest_stat_pass(source, peer):
        return pltpu.make_async_remote_copy(
            GSTAT.at[source], GSTAT.at[source], gs.at[0], gr.at[source],
            device_id={"tp": peer}, device_id_type=MESH,
        )

    def guest_back(index):
        start = pl.multiple_of(index * CHUNK + halo, 16)
        return pltpu.make_async_remote_copy(
            EXT.at[0, pl.ds(pl.multiple_of(guest_base + start, 16), CHUNK)],
            EXT.at[0, pl.ds(start, CHUNK)],
            bs.at[index], br.at[index],
            device_id={"sp": me + outward}, device_id_type=MESH,
        )

    def at_distance(k, body, select=None):
        if k == 0:
            if select is None:
                body(me)
            else:
                pl.when(select(me))(lambda: body(me))
            return

        def step(index, _):
            owner = me + k - 2 * k * index
            ok = both(owner >= 0, owner < S)
            if select is not None:
                ok = both(ok, select(owner))

            @pl.when(ok)
            def _():
                body(owner)

            return 0

        lax.fori_loop(0, 2, step, 0)

    def multiply(total, x, layer, owner, start):
        at = lax.div(owner * Ds, Dt)
        columns = pl.ds(pl.multiple_of(lax.rem(owner * Ds, Dt), 128), Ds)
        xs_block = x[at, :, columns]
        for which, slots in ((0, WV), (1, WG)):
            part = jnp.dot(xs_block, slots[layer, owner], preferred_element_type=F32)
            if start:
                total[which] = part
            else:
                total[which] += part

    def project(layer, k, select=None):
        def block(owner):
            if k > 0:
                arrive(groups[layer][0] + groups[layer][1], owner)
            multiply(ACC, X.at[layer], layer, owner, k == 0)

        at_distance(k, block, select)

    def halo_copy(layer):
        end = halo + rows + (own_base if layer == 0 else 0)
        return pltpu.make_async_remote_copy(
            EXT.at[layer, pl.ds(pl.multiple_of(end - halo, 16), halo)],
            EXT.at[layer, pl.ds(0, halo)],
            hs.at[layer], hr.at[layer],
            device_id={"sp": me + 1}, device_id_type=MESH,
        )

    def sends_halo(layer):
        return both(no(last), no(first)) if layer == 0 else no(last)

    def takes_halo(layer):
        return both(no(first), no(low)) if layer == 0 else no(first)

    def gate_rows(layer, total, stat, base, where):
        mean = total_stat(stat, where)[:, :1] / features
        inv = lax.rsqrt(mean + epsilon)
        value, gating = total[0, where, :] * inv, total[1, where, :] * inv
        gated = (value / (1.0 + jnp.exp(-gating))).astype(BF16)
        EXT[layer, pl.ds(pl.multiple_of(base + where.start + halo, 16), where.size), :] = gated

    def gate(layer):
        base = own_base if layer == 0 else 0
        each_chunk(functools.partial(gate_rows, layer, ACC, STAT.at[2 * layer], base))

        @pl.when(sends_halo(layer))
        def _():
            halo_copy(layer).start()

    def convolve(layer, part):
        def wait_halo():
            @pl.when(first)
            def _():
                EXT[layer, pl.ds(0, halo), :] = jnp.zeros((halo, Cn), BF16)

            @pl.when(takes_halo(layer))
            def _():
                halo_copy(layer).wait_recv()

        tall = CHUNK + halo + 8
        offset = halo - (taps - 1)
        base = own_base if layer == 0 else 0

        def body(where):
            if layer == 0:

                @pl.when(edge)
                def _():
                    guest_back(lax.div(where.start, CHUNK)).wait_recv()

            for column in range(0, Cn, 128):
                at = pl.ds(column, 128)
                window = EXT[layer, pl.ds(pl.multiple_of(base + where.start, 16), CHUNK + halo), at]
                tile = jnp.concatenate([window.astype(F32), jnp.zeros((8, 128), F32)], axis=0)
                total = jnp.zeros((CHUNK, 128), F32)
                for residue in range(8):
                    ks = [k for k in range(taps) if (k + offset) % 8 == residue]
                    if not ks:
                        continue
                    turned = pltpu.roll(tile, tall - residue, 0) if residue else tile
                    for k in ks:
                        low_row = k + offset - residue
                        total = total + taps_ref[k, layer : layer + 1, at] * turned[low_row : low_row + CHUNK]
                CONV[where, at] = total
            conved = CONV[where, :]
            put_stat(
                2 * layer + 1, where,
                jnp.sum(conved, axis=1, keepdims=True),
                jnp.sum(conved * conved, axis=1, keepdims=True),
            )

        if layer == 0:
            wait_halo()
            each_chunk(body)
        else:
            each_chunk(body, CHUNK, rows - CHUNK)
            wait_halo()
            each_chunk(body, 0, CHUNK)
        send_stat(2 * layer + 1, part)

    def mix(layer, part):
        start, count = parts_of(layer)[part]
        wait_stat(2 * layer + 1, part)

        def body(where):
            stat = total_stat(STAT.at[2 * layer + 1], where)
            mean = stat[:, 0:1] / channels
            spread = stat[:, 1:2] / channels - mean * mean
            normed = (CONV[where, :] - mean) * lax.rsqrt(spread + epsilon) * ng_ref[
                layer : layer + 1, :
            ] + ns_ref[layer : layer + 1, :]
            MIX[where, :] = (normed / (1.0 + jnp.exp(-normed))).astype(BF16)

        each_chunk(body, start, count)

    fine = Q if S == T else 1
    width = Dt // fine

    def cut(layer, ref, q, part):
        start, count = parts_of(layer)[part]
        return ref.at[pl.ds(start, count), columns_of(q)]

    def columns_of(q):
        return pl.ds(0, width) if fine == 1 else pl.ds(pl.multiple_of(q * width, 128), width)

    def pair_copy(layer, at, q, part):
        return pltpu.make_async_remote_copy(
            cut(layer, PART.at[layer, 2 * at + 1 - core], q, part), cut(layer, PRECV.at[layer, at], q, part),
            ps.at[layer, at], pr.at[layer, at, part, q],
            device_id={"tp": partner}, device_id_type=MESH,
        )

    def sum_copy(layer, at, q, part):
        return pltpu.make_async_remote_copy(
            cut(layer, SUMB.at[layer, at], q, part), cut(layer, RECV.at[layer, chip], q, part),
            rs.at[layer, at], rr.at[layer, chip, part, q],
            device_id={"tp": at * 2 + core}, device_id_type=MESH,
        )

    def sum_arrival(layer, at, q, part):
        return pltpu.make_async_remote_copy(
            cut(layer, SUMB.at[layer, at], q, part), cut(layer, RECV.at[layer, at], q, part),
            rs.at[layer, at], rr.at[layer, at, part, q],
            device_id={"tp": at * 2 + core}, device_id_type=MESH,
        )

    def sum_pair(layer, at, q, part):
        pair_copy(layer, at, q, part).wait_recv()
        columns = columns_of(q)

        def body(where):
            SUMB[layer, at, where, columns] = (
                PART[layer, at * 2 + core, where, columns].astype(F32)
                + PRECV[layer, at, where, columns].astype(F32)
            ).astype(BF16)

        each_chunk(body, *parts_of(layer)[part])
        sum_copy(layer, at, q, part).start()

    def turn_order():
        count = Q // 2
        return [(False, g * count + piece, piece) for piece in range(count)] + [
            (True, (1 - g) * count + piece, piece) for piece in range(count)
        ]

    def branch(layer, k, parts, early=True, late=True, wait=True, only=None, select=None, together=False):
        def block(owner):
            target = lax.div(owner * Ds, Dt)
            base = lax.rem(owner * Ds, Dt)
            at = lax.div(target, 2)

            def product(q, part):
                start, count = parts_of(layer)[part]
                columns = pl.ds(pl.multiple_of(base + q * Dq, 128), Dq)
                PART[layer, target, pl.ds(start, count), columns] = jnp.dot(
                    MIX[pl.ds(start, count), :], WO[layer, owner, q], preferred_element_type=F32
                ).astype(BF16)
                if S == T:

                    @pl.when(lax.rem(target, 2) != core)
                    def _():
                        pair_copy(layer, at, q, part).start()

            def total(q, part):
                if S == T:

                    @pl.when(both(lax.rem(target, 2) == core, at != chip))
                    def _():
                        sum_pair(layer, at, q, part)

            order = [o for o in turn_order() if only is None or o[2] in only]
            group = order if k == 0 or together else [o for o in order if not o[0]]
            if together and k > 0:
                arrive(groups[layer][2], owner)
            if early:
                for part in parts:
                    for _, q, _ in group:
                        product(q, part)
                    for _, q, _ in group:
                        total(q, part)
            if k > 0 and late:
                for _, q, piece in order[len(group) :]:
                    if wait:
                        ids = groups[layer][2]
                        split = 2 * len(ids) // Q
                        arrive(ids[piece * split : (piece + 1) * split], owner)
                    for part in parts:
                        product(q, part)
                    for part in parts:
                        total(q, part)

        at_distance(k, block, select)

    def stays(owner):
        return lax.div(owner * Ds, 2 * Dt) == chip

    def leaves(owner):
        return no(stays(owner))

    def share(layer):
        if S != T:
            for part in range(len(parts_of(layer))):
                for shift in list(range(1, chips)) + [0]:
                    pair_copy(layer, lax.rem(chip + shift, chips), 0, part).start()
                for shift in range(1, chips):
                    sum_pair(layer, lax.rem(chip + shift, chips), 0, part)

    def finish(layer):
        share(layer)
        source = h_ref if layer == 0 else HB
        target = out_ref if layer == L - 1 else HB
        for part, (start, count) in enumerate(parts_of(layer)):
            for q in [q for _, q, _ in turn_order()] if fine > 1 else [0]:
                pair_copy(layer, chip, q, part).wait_recv()
                for shift in range(1, chips):
                    sum_arrival(layer, lax.rem(chip + shift, chips), q, part).wait_recv()
                columns = columns_of(q)

                def body(where, columns=columns):
                    total = PART[layer, t, where, columns].astype(F32) + PRECV[
                        layer, chip, where, columns
                    ].astype(F32)
                    for shift in range(1, chips):
                        total = total + RECV[layer, lax.rem(chip + shift, chips), where, columns].astype(F32)
                    target[where, columns] = (source[where, columns].astype(F32) + total).astype(BF16)

                each_chunk(body, start, count)

    def sent(ref, sem):
        pltpu.make_async_remote_copy(
            ref, ref, sem, zr.at[0, 0], device_id={"tp": partner}, device_id_type=MESH
        ).wait_send()

    def half_ref(layer, which, owner, half):
        slots = sources[which][1]
        size = slots.shape[2] // 2
        return slots.at[layer, owner, pl.ds(pl.multiple_of(half * size, size), size)]

    def some_ref(layer, which, owner, half, begin, count, pieces):
        if count == pieces:
            return half_ref(layer, which, owner, half)
        slots = sources[which][1]
        size = slots.shape[2] // (2 * pieces)
        start = pl.multiple_of(half * (size * pieces) + begin * size, size)
        return slots.at[layer, owner, pl.ds(start, size * count)]

    def drain(layer, which):
        ids = groups[layer][which]
        whole = [item for item in ids if direct(item)]
        for way in (1, -1):

            @pl.when(inside(ids[0], me + way))
            def _(way=way):
                sent(half_ref(layer, which, me, g), zo.at[layer, which, (way + 1) // 2])

        @pl.when(edge)
        def _():
            sent(some_ref(layer, which, me, 1 - g, 0, len(whole), len(ids)), ys.at[layer, which, me])

        def settle(owner, _):
            @pl.when(both(owner != me, inside(ids[0], me)))
            def _():
                @pl.when(inside(ids[0], jnp.where(owner < me, me + 1, me - 1)))
                def _():
                    sent(half_ref(layer, which, owner, g), zs.at[layer, which, owner])

                skip = skips_y(whole[0], owner)

                @pl.when(no(skip))
                def _():
                    sent(half_ref(layer, which, owner, g), ys.at[layer, which, owner])

                if len(whole) < len(ids):

                    @pl.when(skip)
                    def _():
                        sent(
                            some_ref(layer, which, owner, g, len(whole), len(ids) - len(whole), len(ids)),
                            ys.at[layer, which, owner],
                        )

            return 0

        lax.fori_loop(0, S, settle, 0)

    def drain_x(slot):
        for shift in range(chips):
            xcopy(slot, t, partner, xs.at[slot, shift]).wait_send()
        for shift in range(1, chips):
            xcopy(slot, t, partner, xf.at[slot, shift]).wait_send()

    def drain_stat(slot):
        if slot % 2 == 0:
            sent(STAT.at[slot, pl.ds(0, T - 1)], ss.at[slot])
            return
        for part, (start, count) in enumerate(parts_of(slot // 2)):
            sent(STAT.at[slot, pl.ds(0, T - 1), :, pl.ds(start, count)], ss.at[stat_sem(slot, part)])

    def drain_start():
        @pl.when(edge)
        def _():
            guest_x_copy().wait_send()
            guest_stat_copy().wait_send()

        @pl.when(no(edge))
        def _():
            drain_x(0)
            drain_stat(0)

        @pl.when(near)
        def _():
            drain_x(L)
            sent(GSTAT.at[pl.ds(0, T - 1)], gs.at[0])
            for index in range(rows // CHUNK):
                guest_back(index).wait_send()

    def drain_sums(layer):
        for shift in range(chips):
            at = lax.rem(chip + shift, chips)
            sent(PRECV.at[layer, at], ps.at[layer, at])
        for shift in range(1, chips):
            at = lax.rem(chip + shift, chips)
            sent(SUMB.at[layer, at], rs.at[layer, at])

    def drain_halo(layer):
        @pl.when(sends_halo(layer))
        def _():
            halo_copy(layer).wait_send()

    barrier = pltpu.get_barrier_semaphore()
    for shift in range(1, T):
        pl.semaphore_signal(barrier, inc=1, device_id={"tp": lax.rem(t + shift, T)}, device_id_type=MESH)
    pl.semaphore_signal(barrier, inc=1, device_id={"grp": 1 - g}, device_id_type=MESH)

    @pl.when(no(first))
    def _():
        pl.semaphore_signal(barrier, inc=1, device_id={"sp": me - 1}, device_id_type=MESH)

    @pl.when(no(last))
    def _():
        pl.semaphore_signal(barrier, inc=1, device_id={"sp": me + 1}, device_id_type=MESH)

    inner = jnp.where(first, 0, 1) + jnp.where(last, 0, 1)
    pl.semaphore_wait(barrier, T + inner)

    value0, gating0, out0 = groups[0]
    for which in range(2):
        own_wait(0, which)
        send_own(groups[0][which])
    rest = [(0, 2)] + [(layer, which) for layer in range(1, L) for which in range(3)]
    for layer, which in rest:
        own_start(layer, which)
    for layer, which in rest:
        own_wait(layer, which)
        send_out(groups[layer][which])
    make_x(0)

    def owned_inside(owner):
        return no(is_edge(owner))

    def inner_take(ids, k, select=None):
        @pl.when(no(edge))
        def _():
            take(ids, k, select)

    def edge_take(ids, k):
        @pl.when(edge)
        def _():
            take(ids, k)

    def far_take(ids):
        for k in range(3, S):
            take(ids, k)

    @pl.when(edge)
    def _():
        guest_x_copy().start()
        guest_stat_copy().start()
        send_direct(value0 + gating0)
        send_own(out0)
        send_direct(out0)
        for layer in range(1, L):
            send_own(groups[layer][0] + groups[layer][1])
            send_direct(groups[layer][0] + groups[layer][1])
            send_own(groups[layer][2])
            send_direct(groups[layer][2])
        take(out0, 1)
        for layer in range(1, L):
            for which in range(3):
                take(groups[layer][which], 1)
        take(out0, 2)
        if L > 1:
            take(fore(groups[1][0]), 2)

    @pl.when(no(edge))
    def _():
        send_x(0)
        send_stat(0)
        take(value0 + gating0, 1)
        send_own(out0)
        relay_x(0)
        wait_x(0)
        project(0, 0)
        for k in range(2, S - 1):
            take(value0, k)
            if k == 2:

                @pl.when(near)
                def _():
                    xcopy(L, t, partner, xf.at[L, 0]).wait_recv()
                    guest_stat_pass(t, partner).wait_recv()
                    send_x(L)
                    for shift in range(1, T):
                        guest_stat_pass(t, lax.rem(t + shift, T)).start()

            take(gating0, k)
            if k == 2 and L > 1:
                send_own(groups[1][0])
            project(0, k - 1, lambda owner: no(skips_y(value0[0], owner)))
        take(out0, 1, owned_inside)

        @pl.when(near)
        def _():
            relay_x(L)
            wait_x(L)
            for shift in range(1, T):
                guest_stat_pass(lax.rem(t + shift, T), partner).wait_recv()

        if L > 1:
            take(fore(groups[1][0]), 1, owned_inside)
        take(fore(out0), 1, is_edge)
        project(0, S - 2)
        wait_stat(0)

        @pl.when(near)
        def _():
            corner = jnp.where(low, 0, S - 1)
            arrive(value0 + gating0, corner)
            multiply(ACC, X.at[0], 0, corner, False)
            multiply(GACC, XG, 0, me, True)

            def add(index, _):
                owner = lax.rem(me + index, S)
                multiply(GACC, XG, 0, owner, False)
                return 0

            lax.fori_loop(1, S, add, 0)

            def back(where):
                gate_rows(0, GACC, GSTAT, guest_base, where)
                guest_back(lax.div(where.start, CHUNK)).start()

            each_chunk(back)

        gate(0)
        take(aft(out0), 1, is_edge)
        if L > 1:
            send_own(groups[1][1])
            take(aft(groups[1][0]), 1, owned_inside)

    for layer in range(L):
        out = groups[layer][2]
        ahead = groups[layer + 1] if layer + 1 < L else None
        every = list(range(len(parts_of(layer))))
        columns = list(range(Q // 2))
        head_columns, tail_columns = columns[: Q // 4], columns[Q // 4 :]
        if ahead and layer > 0:
            inner_take(ahead[0], 1, owned_inside)
            edge_take(fore(ahead[0]), 2)
        if layer == 0:
            convolve(0, 0)
            inner_take(fore(out), 2)
            mix(0, 0)
            inner_take(aft(out), 2)
        else:
            inner_take(aft(out), 2)
            convolve(layer, 0)
            far_take(fore(out))
            mix(layer, 0)
            for k in range(3):
                branch(layer, k, every, late=False, select=leaves)
            for k in range(3, S):
                branch(layer, k, every, late=False, only=head_columns, select=leaves)
            far_take(aft(out)[:1])
            for k in range(1, 3):
                branch(layer, k, every, early=False, select=leaves)
            far_take(aft(out)[1:])
            for k in range(3):
                branch(layer, k, every, select=stays, together=True)
            for k in range(3, S):
                branch(layer, k, every, late=False, only=head_columns, select=stays)
        if ahead:
            edge_take(aft(ahead[0]), 2)
        if layer == 0:
            branch(layer, 0, [0])
            branch(layer, 1, [0])
            far_take(fore(out))
            if ahead:
                inner_take(fore(ahead[1]), 1, owned_inside)
                inner_take(fore(ahead[0]), 1, is_edge)
            branch(layer, 2, [0], late=False)
            if ahead:
                inner_take(aft(ahead[0]), 1, is_edge)
                inner_take(aft(ahead[1]), 1, owned_inside)
            branch(layer, 2, [0], early=False)
        else:
            for k in range(3, S):
                branch(layer, k, every, early=False, only=head_columns)
                branch(layer, k, every, late=False, only=tail_columns)
            if ahead:
                inner_take(fore(ahead[1]), 1, owned_inside)
                inner_take(ahead[0], 1, is_edge)
                inner_take(aft(ahead[1]), 1, owned_inside)
        if ahead is None:
            drain_stat(2 * layer + 1)
            drain_halo(layer)
            if layer > 0:
                drain_x(layer)
                drain_stat(2 * layer)
                drain(layer, 0)
                drain(layer, 1)
        if layer == 0:
            far_take(aft(out))
        for k in range(3, S) if layer == 0 else []:
            branch(layer, k, every, late=False)
        if ahead:
            edge_take(fore(ahead[1]), 2)
            for k in range(3, S):
                branch(layer, k, every, early=False, only=head_columns)
            edge_take(aft(ahead[1])[:1], 2)
            for k in range(3, S):
                branch(layer, k, every, early=False, only=tail_columns)
        else:
            for k in range(3, S):
                branch(layer, k, every, early=False, only=tail_columns)
        if ahead:
            inner_take(fore(ahead[1]), 1, is_edge)
            inner_take(fore(ahead[0]), 2)
            inner_take(aft(ahead[1]), 1, is_edge)
        last_share = lax.div(jnp.where(first, S - 1, 0) * Ds, Dt)
        afar = both(edge, last_share == t)
        if ahead:

            @pl.when(afar)
            def _(ahead=ahead):
                take(aft(ahead[1])[1:], 2)
                far_take(fore(ahead[0]))

        finish(layer)
        if ahead:
            after = layer + 1
            make_x(after)
            send_x(after)
            send_stat(2 * after)
            inner_take(aft(ahead[0]), 2)

            @pl.when(no(edge))
            def _(ahead=ahead):
                send_own(ahead[2])


            @pl.when(no(afar))
            def _(ahead=ahead):
                edge_take(aft(ahead[1])[1:], 2)
                far_take(fore(ahead[0]))

            far_take(aft(ahead[0]))
            inner_take(ahead[1], 2)
            if layer == 0:
                drain_start()
                drain(0, 0)
                drain(0, 1)
            far_take(ahead[1])
            relay_x(after)
            drain_stat(2 * layer + 1)
            drain_halo(layer)
            drain_sums(layer)
            wait_x(after)
            project(after, 0)
            project(after, 1)
            inner_take(fore(ahead[2]), 1, owned_inside)
            drain(layer, 2)
            if layer > 0:
                drain_x(layer)
                drain_stat(2 * layer)
                drain(layer, 0)
                drain(layer, 1)
            inner_take(aft(ahead[2]), 1, owned_inside)
            inner_take(ahead[2], 1, is_edge)
            project(after, 2)
            edge_take(fore(ahead[2]), 2)
            edge_take(aft(ahead[2])[:1], 2)
            for k in range(3, S):
                project(after, k)
            wait_stat(2 * after)
            gate(after)
            edge_take(aft(ahead[2])[1:], 2)
            if after + 1 < L:

                @pl.when(no(edge))
                def _(after=after):
                    send_own(groups[after + 1][0] + groups[after + 1][1])

            inner_take(fore(ahead[2]), 2)

    drain(L - 1, 2)
    drain_sums(L - 1)


def shards(hidden_in, in_gain, w_value, w_gate, conv_taps, norm_gain, norm_shift, w_out):
    S, T = lax.axis_size("sp"), lax.axis_size("tp")
    L, Ds, Cn = w_value.shape
    rows, Dt = hidden_in.shape
    chips = T // 2
    halo = (conv_taps.shape[1] - 1 + 15) // 16 * 16
    items = sum(sum(cuts(Ds, layer)) for layer in range(L))
    Q = max(2, cuts(Ds, 0)[2])
    fine = Q if S == T else 1
    vmem = pl.BlockSpec(memory_space=pltpu.VMEM)
    hbm = pl.BlockSpec(memory_space=pl.ANY)
    dma = pltpu.SemaphoreType.DMA
    return pl.pallas_call(
        functools.partial(kernel, S, T),
        out_shape=jax.ShapeDtypeStruct((rows, Dt), BF16),
        in_specs=[vmem, vmem, hbm, hbm, vmem, vmem, vmem, hbm],
        out_specs=vmem,
        scratch_shapes=[
            pltpu.VMEM((L, S, Ds, Cn), BF16),
            pltpu.VMEM((L, S, Ds, Cn), BF16),
            pltpu.VMEM((L, S, Q, Cn, Ds // Q), BF16),
            pltpu.VMEM((L, T, rows, Dt), BF16),
            pltpu.VMEM((T, rows, Dt), BF16),
            pltpu.VMEM((2, rows, Cn), F32),
            pltpu.VMEM((2, rows, Cn), F32),
            pltpu.VMEM((L, halo + 2 * rows, Cn), BF16),
            pltpu.VMEM((rows, Cn), F32),
            pltpu.VMEM((rows, Cn), BF16),
            pltpu.VMEM((L, T, rows, Dt), BF16),
            pltpu.VMEM((L, chips, rows, Dt), BF16),
            pltpu.VMEM((L, chips, rows, Dt), BF16),
            pltpu.VMEM((L, chips, rows, Dt), BF16),
            pltpu.VMEM((2 * L, T, 8, rows), F32),
            pltpu.VMEM((T, 8, rows), F32),
            pltpu.VMEM((rows, Dt), BF16),
            dma((L, 3)),
            dma((items, S)), dma((L, 3, S)), dma((L, 3, 2)), dma((items, S)), dma((L, 3, S)),
            dma((L + 1, T)), dma((L + 1, chips)), dma((L + 1, chips)),
            dma((2 * L, T)), dma((2 * L,)),
            dma((T,)), dma((1,)),
            dma((L,)), dma((L,)),
            dma((rows // CHUNK,)), dma((rows // CHUNK,)),
            dma((L, chips, 1, fine)), dma((L, chips)),
            dma((L, chips, 1, fine)), dma((L, chips)),
        ],
        compiler_params=pltpu.CompilerParams(
            collective_id=0, has_side_effects=True, vmem_limit_bytes=64_000_000
        ),
    )(hidden_in, in_gain, w_value, w_gate, jnp.swapaxes(conv_taps, 0, 1), norm_gain, norm_shift, w_out)


def solution(mesh):
    placed = (
        P(("grp", "sp"), "tp"),
        P(None, "tp"),
        P(None, "sp", "tp"),
        P(None, "sp", "tp"),
        P(None, None, "tp"),
        P(None, "tp"),
        P(None, "tp"),
        P(None, "tp", "sp"),
    )
    return jax.shard_map(
        shards, mesh=mesh, in_specs=placed, out_specs=P(("grp", "sp"), "tp"), check_vma=False
    )
```
